32 devices in a mesh: fs: 8 (over z, y), tp: 4 (over x, core).
Axes of the slice: x: 2, y: 2, z: 4, core: 2. Of those that a mesh axis runs over, the one named last changes fastest.
Arguments:
- normed_input: bfloat16 [6144, 2048], P(('fs', 'tp')), may hold values from -6 to 6
- pre_act: bfloat16 [6144, 8192], P('fs', 'tp'), may hold values from -6 to 6
- out_grad: bfloat16 [6144, 2048], P(('fs', 'tp')), may hold values from -6 to 6
- up_weight: bfloat16 [2048, 8192], P('fs', 'tp'), may hold values from -0.125 to 0.125
- down_weight: bfloat16 [8192, 2048], P('tp', 'fs'), may hold values from -0.0625 to 0.0625
Outputs:
- input_grad: bfloat16 [6144, 2048], P(('fs', 'tp'))
- up_grad: float32 [2048, 8192], P('fs', 'tp')
- down_grad: float32 [8192, 2048], P('tp', 'fs')
The draws below stay inside these ranges and needn't reach their ends.
All inputs are finite; a program needn't handle non-finite values.
Results may differ from the reference program's by a relative error of at most 0.014.
Values may be sent and summed in bfloat16 or wider, within the bound.
A program may use at most 128 MiB of HBM per device.

```python
import jax
import jax.numpy as jnp
from jax import lax

D = 2048
FF = 8192
TOKENS = 6144
N_TP = 4


def raised(values, stream_key, source, target, blocks, factor):
    owner, partner = [(jnp.arange(values.shape[dim]) // (values.shape[dim] // blocks)).reshape([-1 if axis == dim else 1 for axis in range(values.ndim)]) for dim in (source, target)]
    chosen = jax.random.permutation(stream_key, blocks)[partner]
    strong = (owner == chosen) | (owner == (partner + blocks // 2) % blocks)
    return jnp.where(strong, factor * values, values)


def shard_levels(stream_key, extent, split, smallest, high):
    gain, own = 1.0, jax.random.fold_in(stream_key, 6)
    for position, shards_of in split:
        steps = jnp.exp(jax.random.uniform(jax.random.fold_in(own, position), (shards_of,), jnp.float32, smallest / len(split), high / len(split)))
        gain = gain * jnp.repeat(steps, extent[position] // shards_of).reshape([-1 if axis == position else 1 for axis in range(len(extent))])
    return gain


def centred(key, shape, scale, limit, cuts=(), dtype=jnp.bfloat16):
    drawn = jax.random.normal(key, shape, jnp.float32) * scale
    if len(cuts) > 0:
        drawn = shard_levels(key, shape, cuts, -0.22, 0.18) * drawn
    return jnp.clip(drawn, min=-limit, max=limit).astype(dtype)


def heavy_noise(stream_key, dims, spread, most, cuts, heavy, kind=jnp.bfloat16):
    result = spread * jax.random.normal(stream_key, dims, jnp.float32)
    if cuts:
        result = result * shard_levels(stream_key, dims, cuts, -0.22, 0.18)
    return jnp.clip(raised(result, jax.random.fold_in(stream_key, 3), *heavy), -most, most).astype(kind)


def setup_inputs(seed: int = 0) -> dict:
    streams_of = jax.random.split(jax.random.key(seed), 6)
    normed_input = centred(streams_of[0], (TOKENS, D), 1.0, 6.0, ((0, 32),))
    pre_act = centred(streams_of[1], (TOKENS, FF), 1.0, 6.0, ((0, 8), (1, 4)))
    out_grad = heavy_noise(streams_of[2], (TOKENS, D), 1.0, 6.0, ((0, 32),), (0, 1, 32, 2.75))
    up_weight = centred(streams_of[3], (D, FF), D ** -0.5, 0.125, ((0, 8), (1, 4)))
    down_weight = centred(streams_of[4], (FF, D), FF ** -0.5, 0.0625, ((0, 4), (1, 8)))
    return {"normed_input": normed_input, "pre_act": pre_act, "out_grad": out_grad, "up_weight": up_weight, "down_weight": down_weight}


def reference(normed_input, pre_act, out_grad, up_weight, down_weight):
    active = jnp.maximum(pre_act.astype(jnp.float32), 0.0)
    hidden = (active * active).astype(jnp.bfloat16)
    width = FF // N_TP
    up_blocks = up_weight.reshape(D, N_TP, width).transpose(1, 0, 2)
    down_blocks = down_weight.reshape(N_TP, width, D)
    act_blocks = active.reshape(TOKENS, N_TP, width).transpose(1, 0, 2)
    hid_blocks = hidden.reshape(TOKENS, N_TP, width).transpose(1, 0, 2)

    def one_block(items):
        up_part, down_part, act_part, hid_part = items
        grad_hidden = jnp.dot(out_grad, down_part.T, preferred_element_type=jnp.float32)
        pre_grad = (2.0 * act_part * grad_hidden).astype(jnp.bfloat16)
        part = jnp.dot(pre_grad, up_part.T, preferred_element_type=jnp.float32).astype(jnp.bfloat16)
        up_part_grad = jnp.dot(normed_input.T, pre_grad, preferred_element_type=jnp.float32)
        down_part_grad = jnp.dot(hid_part.T, out_grad, preferred_element_type=jnp.float32)
        return part, up_part_grad, down_part_grad

    parts, up_grads, down_grads = lax.map(one_block, (up_blocks, down_blocks, act_blocks, hid_blocks))
    input_grad = jnp.sum(parts.astype(jnp.float32), axis=0).astype(jnp.bfloat16)
    up_grad = up_grads.transpose(1, 0, 2).reshape(D, FF)
    down_grad = down_grads.reshape(FF, D)
    return input_grad, up_grad, down_grad
```

```python
import functools

import jax
import jax.numpy as jnp
from jax import lax
from jax.experimental import pallas as pl
from jax.experimental.pallas import tpu as pltpu
from jax.sharding import PartitionSpec as P

MESH = pl.DeviceIdType.MESH
BF16, F32 = jnp.bfloat16, jnp.float32
CHUNKS = 4
ACT_PARTS = 2
DN, UP = 0, 1
RIGHT, LEFT = 0, 1


def aligned(value, unit):
    return pl.multiple_of(value, unit)


class Dims:
    def __init__(self, fs, tp, tokens, d, hidden):
        self.fs, self.tp = fs, tp
        self.ny, self.nc = 2, 2
        self.nz, self.nx = fs // 2, tp // 2
        self.t, self.d, self.h = tokens, d, hidden
        self.rows = tokens * tp
        self.all_rows = self.rows * self.ny
        self.hh = hidden // self.ny
        self.df = d // fs
        self.dz = self.df * self.ny
        self.half = tokens // 2
        self.hc = self.hh // CHUNKS
        self.ha = self.hh // ACT_PARTS


def kernel(
    m, inp, act, og, upw, dnw, ig_out, ug_out, dg_out,
    og_all, in_all, acts, hid, dn_all, up_all,
    part_dn, part_up, slot_dn, slot_up, crecv, xr1, yr1, yr2, xr2,
    loc, ag_s, ag_r, wy_s, wy_r, tok_s, tok_r, act_s, act_r,
    rs_s, rs_r, fin_s, fin_r, fin_l, igc_s, igc_r, igx_s, igx_r,
):
    f, tt = lax.axis_index("fs"), lax.axis_index("tp")
    ny, nx, nz = m.ny, m.nx, m.nz
    z, y = f // ny, f % ny
    x, c = tt // 2, tt % 2
    yo, co = 1 - y, 1 - c
    sends = []

    def at(zz, yy, xx, cc):
        return (zz * ny + yy, xx * 2 + cc)

    y_dev, c_dev = at(z, yo, x, c), at(z, y, x, co)
    z_dev = (at(z + 1, y, x, c), at(z - 1, y, x, c))
    has_z = (z < nz - 1, z > 0)

    def x_at(k):
        return lax.rem(x + k, nx)

    def remote(src, dst, ss, rs, dev):
        return pltpu.make_async_remote_copy(
            src_ref=src, dst_ref=dst, send_sem=ss, recv_sem=rs,
            device_id=dev, device_id_type=MESH,
        )

    def go(copy, cond=None):
        if cond is None:
            copy.start()
        else:
            pl.when(cond)(copy.start)
        sends.append((cond, copy))

    def drain():
        for cond, copy in sends:
            if cond is None:
                copy.wait_send()
            else:
                pl.when(cond)(copy.wait_send)
        sends.clear()

    barrier = pltpu.get_barrier_semaphore()
    peers = [(None, y_dev), (None, c_dev)]
    peers += [(None, at(z, y, x_at(k), c)) for k in range(1, nx)]
    peers += [(has_z[RIGHT], z_dev[RIGHT]), (has_z[LEFT], z_dev[LEFT])]
    for cond, dev in peers:
        def hello(dev=dev):
            pl.semaphore_signal(barrier, inc=1, device_id=dev, device_id_type=MESH)
        hello() if cond is None else pl.when(cond)(hello)
    lines = jnp.where(z > 0, 1, 0) + jnp.where(z < nz - 1, 1, 0)
    pl.semaphore_wait(barrier, 1 + nx + lines)

    def slot(buf, yy, xx, cc):
        start = aligned(((yy * nx + xx) * 2 + cc) * m.t, m.t)
        return buf.at[pl.ds(start, m.t), :]

    def weight_view(w, ff):
        start = aligned(ff * m.df, m.df)
        if w == DN:
            return dn_all.at[:, pl.ds(start, m.df)]
        return up_all.at[pl.ds(start, m.df), :]

    def weight_own(w, yy):
        start = aligned(yy * m.hh, m.hh)
        if w == DN:
            return dnw.at[pl.ds(start, m.hh), :]
        return upw.at[:, pl.ds(start, m.hh)]

    def ag(w, u, side, k, receive=False):
        back = k + 1 if receive else k
        origin = jnp.clip(z - back if side == RIGHT else z + back, 0, nz - 1)
        view = weight_view(w, origin * ny + (y if u == 0 else yo))
        src = weight_own(w, y) if (u == 0 and k == 0) else view
        dev = z_dev[side]
        return remote(src, view, ag_s.at[w, u, side, k], ag_r.at[w, u, side, k], dev)

    def ag_sends(side, k):
        if side == RIGHT:
            return jnp.logical_and(z >= k, z < nz - 1)
        return jnp.logical_and(z <= nz - 1 - k, z > 0)

    def ag_step(w, u, k):
        for side in (RIGHT, LEFT):
            cond = ag_sends(side, k)
            if k > 0:
                pl.when(cond)(ag(w, u, side, k - 1, True).wait_recv)
            go(ag(w, u, side, k), cond)

    def ag_finish(w, u):
        for k in range(nz - 1):
            pl.when(jnp.logical_and(z == nz - 1, z >= k + 1))(
                ag(w, u, RIGHT, k, True).wait_recv)
            pl.when(jnp.logical_and(z == 0, z <= nz - 2 - k))(
                ag(w, u, LEFT, k, True).wait_recv)

    def weight_y(w, receive=False):
        ff = z * ny + (yo if receive else y)
        return remote(weight_own(w, yo), weight_view(w, ff), wy_s.at[w], wy_r.at[w], y_dev)

    class Rows:
        def __init__(self, a, src, buf):
            self.a, self.src, self.buf = a, src, buf

        def copy(self, index, src, where, dev):
            return remote(src, slot(self.buf, *where), tok_s.at[self.a, index],
                          tok_r.at[self.a, index], dev)

        def over_y(self, receive=False):
            return self.copy(0, self.src, (yo if receive else y, x, c), y_dev)

        def over_x(self, j, k, receive=False):
            yy = y if j == 0 else yo
            xx = x_at(nx - k) if receive else x
            src = self.src if j == 0 else slot(self.buf, yy, x, c)
            return self.copy(j * (nx - 1) + k, src, (yy, xx, c), at(z, y, x_at(k), c))

        def over_c(self, j, k, receive=False):
            yy = y if j == 0 else yo
            xx = x_at(nx - k) if k else x
            src = self.src if j == 0 and k == 0 else slot(self.buf, yy, xx, c)
            index = 1 + 2 * (nx - 1) + j * nx + k
            return self.copy(index, src, (yy, xx, co if receive else c), c_dev)

        def start_y(self):
            go(self.over_y())

        def start_x(self):
            for k in range(1, nx):
                go(self.over_x(0, k))
            go(self.over_c(0, 0))

        def relay_y(self):
            self.over_y(True).wait_recv()
            for k in range(1, nx):
                go(self.over_x(1, k))
            go(self.over_c(1, 0))

        def relay_x(self, j):
            for k in range(1, nx):
                self.over_x(j, k, True).wait_recv()
                go(self.over_c(j, k))

        def finish(self):
            for j in range(ny):
                for k in range(nx):
                    self.over_c(j, k, True).wait_recv()

    og_rows = Rows(0, og, og_all)
    in_rows = Rows(1, inp, in_all)

    def act_copy(part, receive=False):
        col = part * m.ha
        src = act.at[:, pl.ds(aligned(yo * m.hh + col, m.ha), m.ha)]
        row = aligned((yo if receive else y) * m.rows, m.rows)
        dst = acts.at[pl.ds(row, m.rows), pl.ds(col, m.ha)]
        return remote(src, dst, act_s.at[part], act_r.at[part], y_dev)

    local = [
        pltpu.make_async_copy(weight_own(DN, y), weight_view(DN, f), loc.at[0]),
        pltpu.make_async_copy(weight_own(UP, y), weight_view(UP, f), loc.at[1]),
        pltpu.make_async_copy(og, slot(og_all, y, x, c), loc.at[2]),
        pltpu.make_async_copy(inp, slot(in_all, y, x, c), loc.at[3]),
        pltpu.make_async_copy(
            act.at[:, pl.ds(aligned(y * m.hh, m.hh), m.hh)],
            acts.at[pl.ds(aligned(y * m.rows, m.rows), m.rows), :], loc.at[4]),
    ]

    parts, slots = (part_dn, part_up), (slot_dn, slot_up)

    def rs(w, side, target, ch, own):
        src = (parts if own else slots)[w].at[target, ch]
        if side == RIGHT:
            place = target
        else:
            place = jnp.where(target == z - 1, nz, target)
        return remote(src, slots[w].at[place, ch], rs_s.at[w, side, target, ch],
                      rs_r.at[w, side, target, ch], z_dev[side])

    def rs_waits(w, side, target, ch, place):
        return remote(parts[w].at[0, ch], slots[w].at[place, ch],
                      rs_s.at[w, side, target, ch], rs_r.at[w, side, target, ch],
                      z_dev[side])

    def by_rows(count, step, body):
        @pl.loop(0, count // step)
        def _(i):
            body(pl.ds(aligned(i * step, step), step))

    def rs_edge(w, target, ch):
        @pl.when(jnp.logical_and(z == 0, target > 0))
        def _():
            rs(w, RIGHT, target, ch, True).start()

        @pl.when(jnp.logical_and(z == nz - 1, target < nz - 1))
        def _():
            rs(w, LEFT, target, ch, True).start()

    def rs_relay(w, step):
        for side in (RIGHT, LEFT):
            target = nz - 1 - step if side == RIGHT else step
            if side == RIGHT:
                cond = jnp.logical_and(z > 0, z < target)
            else:
                cond = jnp.logical_and(z < nz - 1, z > target)

            @pl.when(cond)
            def _():
                @pl.loop(0, CHUNKS)
                def _(ch):
                    rs_waits(w, side, target, ch, target).wait_recv()
                    buf, own = slots[w].at[target, ch], parts[w].at[target, ch]

                    def add(rows):
                        buf[rows, :] = (buf[rows, :].astype(F32)
                                        + own[rows, :].astype(F32)).astype(BF16)
                    by_rows(buf.shape[0], 64, add)
                    rs(w, side, target, ch, False).start()

    def rs_drain(w):
        for target in range(nz):
            @pl.loop(0, CHUNKS)
            def _(ch):
                pl.when(z < target)(rs(w, RIGHT, target, ch, False).wait_send)
                pl.when(z > target)(rs(w, LEFT, target, ch, False).wait_send)

    def fin_copy(w, ch, yy, receive=False):
        src = parts[w].at[z, ch]
        if w == DN:
            src = src.at[:, pl.ds(aligned(yy * m.df, m.df), m.df)]
            row = aligned((yo if receive else y) * m.hh + ch * m.hc, m.hc)
            return src, dg_out.at[pl.ds(row, m.hc), :]
        src = src.at[pl.ds(aligned(yy * m.df, m.df), m.df), :]
        col = aligned((yo if receive else y) * m.hh + ch * m.hc, m.hc)
        return src, ug_out.at[:, pl.ds(col, m.hc)]

    def fin_remote(w, ch, receive=False):
        src, dst = fin_copy(w, ch, yo, receive)
        return remote(src, dst, fin_s.at[w, ch], fin_r.at[w, ch], y_dev)

    def fin_local(w, ch):
        src, dst = fin_copy(w, ch, y)
        return pltpu.make_async_copy(src, dst, fin_l.at[w, ch])

    def rs_finish(w):
        @pl.loop(0, CHUNKS)
        def _(ch):
            own = parts[w].at[z, ch]
            right, left = slots[w].at[z, ch], slots[w].at[nz, ch]
            pl.when(z > 0)(rs_waits(w, RIGHT, z, ch, z).wait_recv)
            pl.when(z < nz - 1)(rs_waits(w, LEFT, z, ch, nz).wait_recv)

            def total(*others):
                def add(rows):
                    value = own[rows, :].astype(F32)
                    for other in others:
                        value = value + other[rows, :].astype(F32)
                    own[rows, :] = value.astype(BF16)
                by_rows(own.shape[0], 64, add)

            pl.when(z == 0)(lambda: total(left))
            pl.when(z == nz - 1)(lambda: total(right))
            pl.when(jnp.logical_and(z > 0, z < nz - 1))(lambda: total(right, left))
            fin_remote(w, ch).start()
            fin_local(w, ch).start()

    def fin_wait(w):
        @pl.loop(0, CHUNKS)
        def _(ch):
            fin_remote(w, ch).wait_send()
            fin_remote(w, ch, True).wait_recv()
            fin_local(w, ch).wait()

    def targets(i):
        turn = i // 2
        return jnp.where(i % 2 == 0, nz - 1 - turn, turn)

    def squares():
        def body(rows):
            active = jnp.maximum(acts[rows, :].astype(F32), 0.0)
            hid[rows, :] = (active * active).astype(BF16)
        by_rows(m.all_rows, 64, body)

    def dot_rows(a, b):
        return lax.dot_general(a, b, (((0,), (0,)), ((), ())), preferred_element_type=F32)

    def dot_cols(a, b):
        return lax.dot_general(a, b, (((1,), (1,)), ((), ())), preferred_element_type=F32)

    def dot_dn():
        @pl.loop(0, nz * CHUNKS)
        def _(i):
            target, ch = targets(i // CHUNKS), i % CHUNKS
            a = hid[:, pl.ds(aligned(ch * m.hc, m.hc), m.hc)]
            b = og_all[:, pl.ds(aligned(target * m.dz, m.dz), m.dz)]
            part_dn[target, ch] = dot_rows(a, b).astype(BF16)
            rs_edge(DN, target, ch)

    def dot_hg():
        @pl.loop(0, m.all_rows // 256)
        def _(i):
            rows = pl.ds(aligned(i * 256, 256), 256)
            active = jnp.maximum(acts[rows, :].astype(F32), 0.0)
            grad = dot_cols(og_all[rows, :], dn_all[...])
            hid[rows, :] = (2.0 * active * grad).astype(BF16)

    def dot_up():
        @pl.loop(0, nz * CHUNKS)
        def _(i):
            target, ch = targets(i // CHUNKS), i % CHUNKS
            a = in_all[:, pl.ds(aligned(target * m.dz, m.dz), m.dz)]
            b = hid[:, pl.ds(aligned(ch * m.hc, m.hc), m.hc)]
            part_up[target, ch] = dot_rows(a, b).astype(BF16)
            rs_edge(UP, target, ch)

    part = og_all

    def ig_c(j, receive=False):
        yy, xx = j // nx, j % nx
        return remote(slot(part, yy, xx, co), crecv.at[yy, xx], igc_s.at[j], igc_r.at[j], c_dev)

    def dot_in():
        @pl.loop(0, 2 * ny * nx)
        def _(i):
            j = i % (ny * nx)
            cc = jnp.where(i < ny * nx, co, c)
            rows = pl.ds(aligned((j * 2 + cc) * m.t, m.t), m.t)
            part[rows, :] = dot_cols(hid[rows, :], up_all[...]).astype(BF16)
            pl.when(i < ny * nx)(ig_c(j).start)

    def ig_sum():
        @pl.loop(0, ny * nx)
        def _(j):
            ig_c(j).wait_recv()
            buf, own = crecv.at[j // nx, j % nx], slot(part, j // nx, j % nx, c)

            def add(rows):
                buf[rows, :] = (buf[rows, :].astype(F32) + own[rows, :].astype(F32)).astype(BF16)
            by_rows(m.t, 32, add)

    low, high = pl.ds(0, m.half), pl.ds(m.half, m.half)

    def accumulate(dst, others):
        def add(rows):
            value = dst[rows, :].astype(F32)
            for other in others:
                value = value + other[rows, :].astype(F32)
            dst[rows, :] = value.astype(BF16)
        by_rows(m.half, 32, add)

    def ig_x1(k):
        return remote(crecv.at[:, x_at(k), low, :], xr1.at[k - 1],
                      igx_s.at[0, k], igx_r.at[0, k], at(z, y, x_at(k), c))

    def ig_y1():
        return remote(crecv.at[yo, x, low, :], yr1, igx_s.at[1, 0], igx_r.at[1, 0], y_dev)

    def ig_y2():
        return remote(crecv.at[yo, :, high, :], yr2, igx_s.at[2, 0], igx_r.at[2, 0], y_dev)

    def ig_x2(k):
        return remote(crecv.at[y, x_at(k), high, :], xr2.at[k - 1],
                      igx_s.at[3, k], igx_r.at[3, k], at(z, y, x_at(k), c))

    def ig_first():
        for k in range(1, nx):
            go(ig_x1(k))
        go(ig_y2())

    def ig_second():
        for k in range(1, nx):
            ig_x1(k).wait_recv()
        for yy in range(ny):
            accumulate(crecv.at[yy, x, low, :], [xr1.at[k, yy] for k in range(nx - 1)])
        go(ig_y1())
        ig_y2().wait_recv()
        for xx in range(nx):
            accumulate(crecv.at[y, xx, high, :], [yr2.at[xx]])
        for k in range(1, nx):
            go(ig_x2(k))

    ig_local = pltpu.make_async_copy(crecv.at[y, x], ig_out, loc.at[5])

    def ig_last():
        ig_y1().wait_recv()
        accumulate(crecv.at[y, x, low, :], [yr1])
        for k in range(1, nx):
            ig_x2(k).wait_recv()
        accumulate(crecv.at[y, x, high, :], [xr2.at[k] for k in range(nx - 1)])
        ig_local.start()

    ag_step(DN, 0, 0)
    og_rows.start_y()
    og_rows.start_x()
    go(weight_y(DN))
    for part_index in range(ACT_PARTS):
        go(act_copy(part_index))
    for copy in local:
        copy.start()
    for copy in local:
        copy.wait()
    ag_step(DN, 0, 1)
    og_rows.relay_y()
    og_rows.relay_x(0)
    for k in range(2, nz - 1):
        ag_step(DN, 0, k)
    weight_y(DN, True).wait_recv()
    ag_step(DN, 1, 0)
    ag_step(UP, 0, 0)
    og_rows.relay_x(1)
    in_rows.start_y()
    in_rows.start_x()
    go(weight_y(UP))
    ag_step(DN, 1, 1)
    og_rows.finish()
    for part_index in range(ACT_PARTS):
        act_copy(part_index, True).wait_recv()
    for k in range(2, nz - 1):
        ag_step(DN, 1, k)
    squares()
    dot_dn()
    ag_step(UP, 0, 1)
    in_rows.relay_y()
    in_rows.relay_x(0)
    rs_relay(DN, 0)
    for k in range(2, nz - 1):
        ag_step(UP, 0, k)
    weight_y(UP, True).wait_recv()
    ag_step(UP, 1, 0)
    in_rows.relay_x(1)
    ag_finish(DN, 0)
    ag_finish(DN, 1)
    dot_hg()
    in_rows.finish()
    dot_up()
    ag_step(UP, 1, 1)
    for step in range(1, nz - 1):
        rs_relay(DN, step)
    for k in range(2, nz - 1):
        ag_step(UP, 1, k)
    rs_relay(UP, 0)
    rs_finish(DN)
    ag_finish(UP, 0)
    ag_finish(UP, 1)
    drain()
    dot_in()
    for step in range(1, nz - 1):
        rs_relay(UP, step)
    ig_sum()
    ig_first()
    ig_second()
    ig_last()
    rs_finish(UP)
    drain()

    @pl.loop(0, ny * nx)
    def _(j):
        ig_c(j).wait_send()

    rs_drain(DN)
    rs_drain(UP)
    ig_local.wait()
    fin_wait(DN)
    fin_wait(UP)


def local_step(fs, tp, inp, act, og, upw, dnw):
    m = Dims(fs, tp, og.shape[0], og.shape[1], act.shape[1])
    dma = pltpu.SemaphoreType.DMA
    vm = pltpu.VMEM
    any_space = pl.BlockSpec(memory_space=pl.ANY)
    rows_events = 1 + 2 * (m.nx - 1) + m.ny * m.nx
    flops = 8 * m.all_rows * m.hh * m.d
    ig, ug, dg = pl.pallas_call(
        functools.partial(kernel, m),
        name="ffn_backward",
        out_shape=(
            jax.ShapeDtypeStruct((m.t, m.d), BF16),
            jax.ShapeDtypeStruct((m.df, m.h), BF16),
            jax.ShapeDtypeStruct((m.h, m.df), BF16),
        ),
        in_specs=[any_space] * 5,
        out_specs=(any_space,) * 3,
        scratch_shapes=[
            vm((m.all_rows, m.d), BF16),
            vm((m.all_rows, m.d), BF16),
            vm((m.all_rows, m.hh), BF16),
            vm((m.all_rows, m.hh), BF16),
            vm((m.hh, m.d), BF16),
            vm((m.d, m.hh), BF16),
            vm((m.nz, CHUNKS, m.hc, m.dz), BF16),
            vm((m.nz, CHUNKS, m.dz, m.hc), BF16),
            vm((m.nz + 1, CHUNKS, m.hc, m.dz), BF16),
            vm((m.nz + 1, CHUNKS, m.dz, m.hc), BF16),
            vm((m.ny, m.nx, m.t, m.d), BF16),
            vm((m.nx - 1, m.ny, m.half, m.d), BF16),
            vm((m.half, m.d), BF16),
            vm((m.nx, m.half, m.d), BF16),
            vm((m.nx - 1, m.half, m.d), BF16),
            dma((6,)),
            dma((2, m.ny, 2, m.nz - 1)),
            dma((2, m.ny, 2, m.nz - 1)),
            dma((2,)),
            dma((2,)),
            dma((2, rows_events)),
            dma((2, rows_events)),
            dma((ACT_PARTS,)),
            dma((ACT_PARTS,)),
            dma((2, 2, m.nz, CHUNKS)),
            dma((2, 2, m.nz, CHUNKS)),
            dma((2, CHUNKS)),
            dma((2, CHUNKS)),
            dma((2, CHUNKS)),
            dma((m.ny * m.nx,)),
            dma((m.ny * m.nx,)),
            dma((4, m.nx)),
            dma((4, m.nx)),
        ],
        cost_estimate=pl.CostEstimate(flops=flops, bytes_accessed=2**25, transcendentals=0),
        compiler_params=pltpu.CompilerParams(
            collective_id=0, has_side_effects=True, vmem_limit_bytes=67043328
        ),
    )(inp, act, og, upw, dnw)
    return ig, ug.astype(F32), dg.astype(F32)


def solution(mesh):
    placed = (
        P(("fs", "tp"), None),
        P("fs", "tp"),
        P(("fs", "tp"), None),
        P("fs", "tp"),
        P("tp", "fs"),
    )
    return jax.shard_map(
        functools.partial(local_step, mesh.shape["fs"], mesh.shape["tp"]),
        mesh=mesh,
        in_specs=placed,
        out_specs=(P(("fs", "tp"), None), P("fs", "tp"), P("tp", "fs")),
        check_vma=False,
    )
```

```python
import functools

import jax
import jax.numpy as jnp
from jax import lax
from jax.experimental import pallas as pl
from jax.experimental.pallas import tpu as pltpu
from jax.sharding import PartitionSpec as P

MESH = pl.DeviceIdType.MESH
BF16, F32 = jnp.bfloat16, jnp.float32
CHUNKS = 4
ACT_PARTS = 4
DN, UP = 0, 1
RIGHT, LEFT = 0, 1


def aligned(value, unit):
    return pl.multiple_of(value, unit)


class Dims:
    def __init__(self, fs, tp, tokens, d, hidden):
        self.fs, self.tp = fs, tp
        self.ny, self.nc = 2, 2
        self.nz, self.nx = fs // 2, tp // 2
        self.t, self.d, self.h = tokens, d, hidden
        self.rows = tokens * tp
        self.all_rows = self.rows * self.ny
        self.hh = hidden // self.ny
        self.df = d // fs
        self.dz = self.df * self.ny
        self.half = tokens // 2
        self.hc = self.hh // CHUNKS
        self.ha = self.hh // ACT_PARTS


def kernel(
    m, inp, act, og, upw, dnw, ig_out, ug_out, dg_out,
    og_all, in_all, acts, hid, dn_all, up_all,
    part_dn, part_up, slot_dn, slot_up, crecv, xr1, yr1, yr2, xr2,
    loc, ag_s, ag_r, wy_s, wy_r, tok_s, tok_r, act_s, act_r,
    rs_s, rs_r, fin_s, fin_r, fin_l, igc_s, igc_r, igx_s, igx_r,
):
    f, tt = lax.axis_index("fs"), lax.axis_index("tp")
    ny, nx, nz = m.ny, m.nx, m.nz
    z, y = f // ny, f % ny
    x, c = tt // 2, tt % 2
    yo, co = 1 - y, 1 - c
    sends = []

    def at(zz, yy, xx, cc):
        return (zz * ny + yy, xx * 2 + cc)

    y_dev, c_dev = at(z, yo, x, c), at(z, y, x, co)
    z_dev = (at(z + 1, y, x, c), at(z - 1, y, x, c))
    has_z = (z < nz - 1, z > 0)

    def x_at(k):
        return lax.rem(x + k, nx)

    def remote(src, dst, ss, rs, dev):
        return pltpu.make_async_remote_copy(
            src_ref=src, dst_ref=dst, send_sem=ss, recv_sem=rs,
            device_id=dev, device_id_type=MESH,
        )

    def go(copy, cond=None, group=sends):
        if cond is None:
            copy.start()
        else:
            pl.when(cond)(copy.start)
        group.append((cond, copy))

    def drain(group):
        for cond, copy in group:
            if cond is None:
                copy.wait_send()
            else:
                pl.when(cond)(copy.wait_send)
        group.clear()

    barrier = pltpu.get_barrier_semaphore()
    peers = [(None, y_dev), (None, c_dev)]
    peers += [(None, at(z, y, x_at(k), c)) for k in range(1, nx)]
    peers += [(has_z[RIGHT], z_dev[RIGHT]), (has_z[LEFT], z_dev[LEFT])]
    for cond, dev in peers:
        def hello(dev=dev):
            pl.semaphore_signal(barrier, inc=1, device_id=dev, device_id_type=MESH)
        hello() if cond is None else pl.when(cond)(hello)
    lines = jnp.where(z > 0, 1, 0) + jnp.where(z < nz - 1, 1, 0)
    pl.semaphore_wait(barrier, 1 + nx + lines)

    def slot(buf, yy, xx, cc):
        start = aligned(((yy * nx + xx) * 2 + cc) * m.t, m.t)
        return buf.at[pl.ds(start, m.t), :]

    def weight_view(w, ff):
        start = aligned(ff * m.df, m.df)
        if w == DN:
            return dn_all.at[:, pl.ds(start, m.df)]
        return up_all.at[pl.ds(start, m.df), :]

    def weight_own(w, yy):
        start = aligned(yy * m.hh, m.hh)
        if w == DN:
            return dnw.at[pl.ds(start, m.hh), :]
        return upw.at[:, pl.ds(start, m.hh)]

    def ag(w, u, side, k, receive=False):
        back = k + 1 if receive else k
        origin = jnp.clip(z - back if side == RIGHT else z + back, 0, nz - 1)
        view = weight_view(w, origin * ny + (y if u == 0 else yo))
        src = weight_own(w, y) if (u == 0 and k == 0) else view
        dev = z_dev[side]
        return remote(src, view, ag_s.at[w, u, side, k], ag_r.at[w, u, side, k], dev)

    def ag_sends(side, k):
        if side == RIGHT:
            return jnp.logical_and(z >= k, z < nz - 1)
        return jnp.logical_and(z <= nz - 1 - k, z > 0)

    def ag_step(w, u, k, where="all"):
        outer = (z == 0, z == nz - 1)
        inner = jnp.logical_and(z > 0, z < nz - 1)
        for side in (RIGHT, LEFT):
            cond = ag_sends(side, k)
            if where == "edge":
                cond = outer[side]
            if where == "inner":
                cond = inner
            if k > 0:
                pl.when(cond)(ag(w, u, side, k - 1, True).wait_recv)
            go(ag(w, u, side, k), cond)

    def ag_finish(w, u):
        for k in range(nz - 1):
            pl.when(jnp.logical_and(z == nz - 1, z >= k + 1))(
                ag(w, u, RIGHT, k, True).wait_recv)
            pl.when(jnp.logical_and(z == 0, z <= nz - 2 - k))(
                ag(w, u, LEFT, k, True).wait_recv)

    def weight_y(w, receive=False):
        ff = z * ny + (yo if receive else y)
        return remote(weight_own(w, yo), weight_view(w, ff), wy_s.at[w], wy_r.at[w], y_dev)

    class Rows:
        def __init__(self, a, src, buf):
            self.a, self.src, self.buf, self.sends = a, src, buf, []

        def go(self, copy):
            go(copy, None, self.sends)

        def drain(self):
            drain(self.sends)

        def copy(self, index, src, where, dev):
            return remote(src, slot(self.buf, *where), tok_s.at[self.a, index],
                          tok_r.at[self.a, index], dev)

        def over_y(self, receive=False):
            return self.copy(0, self.src, (yo if receive else y, x, c), y_dev)

        def over_x(self, j, k, receive=False):
            yy = y if j == 0 else yo
            xx = x_at(nx - k) if receive else x
            src = self.src if j == 0 else slot(self.buf, yy, x, c)
            return self.copy(j * (nx - 1) + k, src, (yy, xx, c), at(z, y, x_at(k), c))

        def over_c(self, j, k, receive=False):
            yy = y if j == 0 else yo
            xx = x_at(nx - k) if k else x
            src = self.src if j == 0 and k == 0 else slot(self.buf, yy, xx, c)
            index = 1 + 2 * (nx - 1) + j * nx + k
            return self.copy(index, src, (yy, xx, co if receive else c), c_dev)

        def start_y(self):
            self.go(self.over_y())

        def start_x(self):
            for k in range(1, nx):
                self.go(self.over_x(0, k))
            self.go(self.over_c(0, 0))

        def relay_y(self):
            self.over_y(True).wait_recv()
            for k in range(1, nx):
                self.go(self.over_x(1, k))
            self.go(self.over_c(1, 0))

        def relay_x(self, j):
            for k in range(1, nx):
                self.over_x(j, k, True).wait_recv()
                self.go(self.over_c(j, k))

        def finish(self):
            for j in range(ny):
                for k in range(nx):
                    self.over_c(j, k, True).wait_recv()

    og_rows = Rows(0, og, og_all)
    in_rows = Rows(1, inp, in_all)

    def act_copy(part, receive=False):
        col = part * m.ha
        src = act.at[:, pl.ds(aligned(yo * m.hh + col, m.ha), m.ha)]
        row = aligned((yo if receive else y) * m.rows, m.rows)
        dst = acts.at[pl.ds(row, m.rows), pl.ds(col, m.ha)]
        return remote(src, dst, act_s.at[part], act_r.at[part], y_dev)

    local = [
        pltpu.make_async_copy(weight_own(DN, y), weight_view(DN, f), loc.at[0]),
        pltpu.make_async_copy(weight_own(UP, y), weight_view(UP, f), loc.at[1]),
        pltpu.make_async_copy(og, slot(og_all, y, x, c), loc.at[2]),
        pltpu.make_async_copy(inp, slot(in_all, y, x, c), loc.at[3]),
        pltpu.make_async_copy(
            act.at[:, pl.ds(aligned(y * m.hh, m.hh), m.hh)],
            acts.at[pl.ds(aligned(y * m.rows, m.rows), m.rows), :], loc.at[4]),
    ]

    parts, slots = (part_dn, part_up), (slot_dn, slot_up)

    def rs(w, side, target, ch, own):
        src = (parts if own else slots)[w].at[target, ch]
        if side == RIGHT:
            place = target
        else:
            place = jnp.where(target == z - 1, nz, target)
        return remote(src, slots[w].at[place, ch], rs_s.at[w, side, target, ch],
                      rs_r.at[w, side, target, ch], z_dev[side])

    def rs_waits(w, side, target, ch, place):
        return remote(parts[w].at[0, ch], slots[w].at[place, ch],
                      rs_s.at[w, side, target, ch], rs_r.at[w, side, target, ch],
                      z_dev[side])

    def by_rows(count, step, body):
        @pl.loop(0, count // step)
        def _(i):
            body(pl.ds(aligned(i * step, step), step))

    def rs_edge(w, target, ch):
        @pl.when(jnp.logical_and(z == 0, target > 0))
        def _():
            rs(w, RIGHT, target, ch, True).start()

        @pl.when(jnp.logical_and(z == nz - 1, target < nz - 1))
        def _():
            rs(w, LEFT, target, ch, True).start()

    def rs_pass(w, side, step, ch):
        target = nz - 1 - step if side == RIGHT else step
        if side == RIGHT:
            cond = jnp.logical_and(z > 0, z < target)
        else:
            cond = jnp.logical_and(z < nz - 1, z > target)

        @pl.when(cond)
        def _():
            rs_waits(w, side, target, ch, target).wait_recv()
            buf, own = slots[w].at[target, ch], parts[w].at[target, ch]

            def add(rows):
                buf[rows, :] = (buf[rows, :].astype(F32)
                                + own[rows, :].astype(F32)).astype(BF16)
            by_rows(buf.shape[0], 64, add)
            rs(w, side, target, ch, False).start()

    def near(w, ch):
        @pl.when(z < nz // 2)
        def _():
            for step in range(nz - 2):
                rs_pass(w, RIGHT, step, ch)

        @pl.when(z >= nz // 2)
        def _():
            for step in range(nz - 2):
                rs_pass(w, LEFT, step, ch)

    def far(w, ch):
        @pl.when(z < nz // 2)
        def _():
            for step in range(nz - 2):
                rs_pass(w, LEFT, step, ch)

        @pl.when(z >= nz // 2)
        def _():
            for step in range(nz - 2):
                rs_pass(w, RIGHT, step, ch)

    def rs_drain(w):
        for target in range(nz):
            @pl.loop(0, CHUNKS)
            def _(ch):
                pl.when(z < target)(rs(w, RIGHT, target, ch, False).wait_send)
                pl.when(z > target)(rs(w, LEFT, target, ch, False).wait_send)

    def fin_copy(w, ch, yy, receive=False):
        src = parts[w].at[z, ch]
        if w == DN:
            src = src.at[:, pl.ds(aligned(yy * m.df, m.df), m.df)]
            row = aligned((yo if receive else y) * m.hh + ch * m.hc, m.hc)
            return src, dg_out.at[pl.ds(row, m.hc), :]
        src = src.at[pl.ds(aligned(yy * m.df, m.df), m.df), :]
        col = aligned((yo if receive else y) * m.hh + ch * m.hc, m.hc)
        return src, ug_out.at[:, pl.ds(col, m.hc)]

    def fin_remote(w, ch, receive=False):
        src, dst = fin_copy(w, ch, yo, receive)
        return remote(src, dst, fin_s.at[w, ch], fin_r.at[w, ch], y_dev)

    def fin_local(w, ch):
        src, dst = fin_copy(w, ch, y)
        return pltpu.make_async_copy(src, dst, fin_l.at[w, ch])

    def rs_finish(w, ch):
        own = parts[w].at[z, ch]
        right, left = slots[w].at[z, ch], slots[w].at[nz, ch]
        pl.when(z > 0)(rs_waits(w, RIGHT, z, ch, z).wait_recv)
        pl.when(z < nz - 1)(rs_waits(w, LEFT, z, ch, nz).wait_recv)

        def total(*others):
            def add(rows):
                value = own[rows, :].astype(F32)
                for other in others:
                    value = value + other[rows, :].astype(F32)
                own[rows, :] = value.astype(BF16)
            by_rows(own.shape[0], 64, add)

        pl.when(z == 0)(lambda: total(left))
        pl.when(z == nz - 1)(lambda: total(right))
        pl.when(jnp.logical_and(z > 0, z < nz - 1))(lambda: total(right, left))
        fin_remote(w, ch).start()
        fin_local(w, ch).start()

    def fin_wait(w):
        @pl.loop(0, CHUNKS)
        def _(ch):
            fin_remote(w, ch).wait_send()
            fin_remote(w, ch, True).wait_recv()
            fin_local(w, ch).wait()

    def targets(i):
        turn = i // 2
        return jnp.where(i % 2 == 0, nz - 1 - turn, turn)

    def squares(ch):
        cols = pl.ds(ch * m.hc, m.hc)

        def body(rows):
            active = jnp.maximum(acts[rows, cols].astype(F32), 0.0)
            hid[rows, cols] = (active * active).astype(BF16)
        by_rows(m.all_rows, 64, body)

    def dot_rows(a, b):
        return lax.dot_general(a, b, (((0,), (0,)), ((), ())), preferred_element_type=F32)

    def dot_cols(a, b):
        return lax.dot_general(a, b, (((1,), (1,)), ((), ())), preferred_element_type=F32)

    def dot_dn(ch):
        @pl.loop(0, nz)
        def _(i):
            target = targets(i)
            a = hid[:, pl.ds(ch * m.hc, m.hc)]
            b = og_all[:, pl.ds(aligned(target * m.dz, m.dz), m.dz)]
            part_dn[target, ch] = dot_rows(a, b).astype(BF16)
            rs_edge(DN, target, ch)

    def dot_hg():
        @pl.loop(0, m.all_rows // 256)
        def _(i):
            rows = pl.ds(aligned(i * 256, 256), 256)
            active = jnp.maximum(acts[rows, :].astype(F32), 0.0)
            grad = dot_cols(og_all[rows, :], dn_all[...])
            hid[rows, :] = (2.0 * active * grad).astype(BF16)

    def dot_up(ch):
        @pl.loop(0, nz)
        def _(i):
            target = targets(i)
            a = in_all[:, pl.ds(aligned(target * m.dz, m.dz), m.dz)]
            b = hid[:, pl.ds(ch * m.hc, m.hc)]
            part_up[target, ch] = dot_rows(a, b).astype(BF16)
            rs_edge(UP, target, ch)

    part = og_all

    def ig_c(j, receive=False):
        yy, xx = j // nx, j % nx
        return remote(slot(part, yy, xx, co), crecv.at[yy, xx], igc_s.at[j], igc_r.at[j], c_dev)

    def dot_in(remote_half):
        @pl.loop(0, ny * nx)
        def _(j):
            cc = co if remote_half else c
            rows = pl.ds(aligned((j * 2 + cc) * m.t, m.t), m.t)
            part[rows, :] = dot_cols(hid[rows, :], up_all[...]).astype(BF16)
            if remote_half:
                ig_c(j).start()

    def ig_sum():
        @pl.loop(0, ny * nx)
        def _(j):
            ig_c(j).wait_recv()
            buf, own = crecv.at[j // nx, j % nx], slot(part, j // nx, j % nx, c)

            def add(rows):
                buf[rows, :] = (buf[rows, :].astype(F32) + own[rows, :].astype(F32)).astype(BF16)
            by_rows(m.t, 32, add)

    low, high = pl.ds(0, m.half), pl.ds(m.half, m.half)

    def accumulate(dst, others):
        def add(rows):
            value = dst[rows, :].astype(F32)
            for other in others:
                value = value + other[rows, :].astype(F32)
            dst[rows, :] = value.astype(BF16)
        by_rows(m.half, 32, add)

    def ig_x1(k):
        return remote(crecv.at[:, x_at(k), low, :], xr1.at[k - 1],
                      igx_s.at[0, k], igx_r.at[0, k], at(z, y, x_at(k), c))

    def ig_y1():
        return remote(crecv.at[yo, x, low, :], yr1, igx_s.at[1, 0], igx_r.at[1, 0], y_dev)

    def ig_y2():
        return remote(crecv.at[yo, :, high, :], yr2, igx_s.at[2, 0], igx_r.at[2, 0], y_dev)

    def ig_x2(k):
        return remote(crecv.at[y, x_at(k), high, :], xr2.at[k - 1],
                      igx_s.at[3, k], igx_r.at[3, k], at(z, y, x_at(k), c))

    def ig_first():
        for k in range(1, nx):
            go(ig_x1(k))
        go(ig_y2())

    def ig_second():
        for k in range(1, nx):
            ig_x1(k).wait_recv()
        for yy in range(ny):
            accumulate(crecv.at[yy, x, low, :], [xr1.at[k, yy] for k in range(nx - 1)])
        go(ig_y1())
        ig_y2().wait_recv()
        for xx in range(nx):
            accumulate(crecv.at[y, xx, high, :], [yr2.at[xx]])
        for k in range(1, nx):
            go(ig_x2(k))

    ig_local = pltpu.make_async_copy(crecv.at[y, x], ig_out, loc.at[5])

    def ig_last():
        ig_y1().wait_recv()
        accumulate(crecv.at[y, x, low, :], [yr1])
        for k in range(1, nx):
            ig_x2(k).wait_recv()
        accumulate(crecv.at[y, x, high, :], [xr2.at[k] for k in range(nx - 1)])
        ig_local.start()

    def acts_in(index):
        act_copy(index, True).wait_recv()

    def start():
        ag_step(DN, 0, 0)
        og_rows.start_y()
        og_rows.start_x()
        go(weight_y(DN))
        go(act_copy(0))
        go(act_copy(1))
        go(weight_y(UP))
        go(act_copy(2))
        go(act_copy(3))
        in_rows.start_y()
        ag_step(UP, 0, 0, "edge")
        for copy in local:
            copy.start()

    def local_wait():
        for copy in local:
            copy.wait()

    def weight_in(w):
        weight_y(w, True).wait_recv()

    def ig_drain():
        @pl.loop(0, ny * nx)
        def _(j):
            ig_c(j).wait_send()
        ig_local.wait()

    def steps(function, *args, first=2):
        return [(function, *args, k) for k in range(first, nz - 1)]

    plan = [
        (start,),
        (ag_step, DN, 0, 1),
        (og_rows.relay_y,),
        (og_rows.relay_x, 0),
        (in_rows.start_x,),
        *steps(ag_step, DN, 0),
        (weight_in, DN),
        (ag_step, DN, 1, 0),
        (og_rows.relay_x, 1),
        (og_rows.finish,),
        (local_wait,),
        (acts_in, 0),
        (squares, 0),
        (dot_dn, 0),
        (ag_step, DN, 1, 1),
        (acts_in, 1),
        (squares, 1),
        (dot_dn, 1),
        (near, DN, 0),
        *steps(ag_step, DN, 1),
        (ag_step, UP, 0, 0, "inner"),
        (weight_in, UP),
        (far, DN, 0),
        (acts_in, 2),
        (squares, 2),
        (dot_dn, 2),
        (near, DN, 1),
        (ag_step, UP, 0, 1),
        (acts_in, 3),
        (squares, 3),
        (dot_dn, 3),
        (ag_finish, DN, 0),
        (ag_finish, DN, 1),
        (dot_hg,),
        (near, DN, 2),
        (far, DN, 1),
        *steps(ag_step, UP, 0),
        (ag_step, UP, 1, 0),
        (in_rows.relay_y,),
        (in_rows.relay_x, 0),
        (near, DN, 3),
        (far, DN, 2),
        (ag_step, UP, 1, 1),
        (in_rows.relay_x, 1),
        (in_rows.finish,),
        (dot_up, 0),
        (far, DN, 3),
        *steps(ag_step, UP, 1),
        (dot_up, 1),
        (dot_up, 2),
        (dot_up, 3),
        (near, UP, 0),
        (rs_finish, DN, 0),
        (rs_finish, DN, 1),
        (far, UP, 0),
        (near, UP, 1),
        (rs_finish, DN, 2),
        (rs_finish, DN, 3),
        (ag_finish, UP, 0),
        (ag_finish, UP, 1),
        (og_rows.drain,),
        (dot_in, True),
        (far, UP, 1),
        (near, UP, 2),
        (dot_in, False),
        (ig_sum,),
        (ig_first,),
        (rs_finish, UP, 0),
        (far, UP, 2),
        (near, UP, 3),
        (rs_finish, UP, 1),
        (far, UP, 3),
        (ig_second,),
        (rs_finish, UP, 2),
        (ig_last,),
        (rs_finish, UP, 3),
        (in_rows.drain,),
        (drain, sends),
        (ig_drain,),
        (rs_drain, DN),
        (rs_drain, UP),
        (fin_wait, DN),
        (fin_wait, UP),
    ]
    for index, (function, *args) in enumerate(plan):
        tags = [str(arg) for arg in args if not isinstance(arg, list)]
        label = "_".join([str(index), function.__name__, *tags])
        with jax.named_scope(label):
            function(*args)


def local_step(fs, tp, inp, act, og, upw, dnw):
    m = Dims(fs, tp, og.shape[0], og.shape[1], act.shape[1])
    dma = pltpu.SemaphoreType.DMA
    vm = pltpu.VMEM
    any_space = pl.BlockSpec(memory_space=pl.ANY)
    rows_events = 1 + 2 * (m.nx - 1) + m.ny * m.nx
    flops = 8 * m.all_rows * m.hh * m.d
    ig, ug, dg = pl.pallas_call(
        functools.partial(kernel, m),
        name="ffn_backward",
        out_shape=(
            jax.ShapeDtypeStruct((m.t, m.d), BF16),
            jax.ShapeDtypeStruct((m.df, m.h), BF16),
            jax.ShapeDtypeStruct((m.h, m.df), BF16),
        ),
        in_specs=[any_space] * 5,
        out_specs=(any_space,) * 3,
        scratch_shapes=[
            vm((m.all_rows, m.d), BF16),
            vm((m.all_rows, m.d), BF16),
            vm((m.all_rows, m.hh), BF16),
            vm((m.all_rows, m.hh), BF16),
            vm((m.hh, m.d), BF16),
            vm((m.d, m.hh), BF16),
            vm((m.nz, CHUNKS, m.hc, m.dz), BF16),
            vm((m.nz, CHUNKS, m.dz, m.hc), BF16),
            vm((m.nz + 1, CHUNKS, m.hc, m.dz), BF16),
            vm((m.nz + 1, CHUNKS, m.dz, m.hc), BF16),
            vm((m.ny, m.nx, m.t, m.d), BF16),
            vm((m.nx - 1, m.ny, m.half, m.d), BF16),
            vm((m.half, m.d), BF16),
            vm((m.nx, m.half, m.d), BF16),
            vm((m.nx - 1, m.half, m.d), BF16),
            dma((6,)),
            dma((2, m.ny, 2, m.nz - 1)),
            dma((2, m.ny, 2, m.nz - 1)),
            dma((2,)),
            dma((2,)),
            dma((2, rows_events)),
            dma((2, rows_events)),
            dma((ACT_PARTS,)),
            dma((ACT_PARTS,)),
            dma((2, 2, m.nz, CHUNKS)),
            dma((2, 2, m.nz, CHUNKS)),
            dma((2, CHUNKS)),
            dma((2, CHUNKS)),
            dma((2, CHUNKS)),
            dma((m.ny * m.nx,)),
            dma((m.ny * m.nx,)),
            dma((4, m.nx)),
            dma((4, m.nx)),
        ],
        cost_estimate=pl.CostEstimate(flops=flops, bytes_accessed=2**25, transcendentals=0),
        compiler_params=pltpu.CompilerParams(
            collective_id=0, has_side_effects=True, vmem_limit_bytes=67043328
        ),
    )(inp, act, og, upw, dnw)
    return ig, ug.astype(F32), dg.astype(F32)


def solution(mesh):
    placed = (
        P(("fs", "tp"), None),
        P("fs", "tp"),
        P(("fs", "tp"), None),
        P("fs", "tp"),
        P("tp", "fs"),
    )
    return jax.shard_map(
        functools.partial(local_step, mesh.shape["fs"], mesh.shape["tp"]),
        mesh=mesh,
        in_specs=placed,
        out_specs=(P(("fs", "tp"), None), P("fs", "tp"), P("tp", "fs")),
        check_vma=False,
    )
```

```python
import functools

import jax
import jax.numpy as jnp
from jax import lax
from jax.experimental import pallas as pl
from jax.experimental.pallas import tpu as pltpu
from jax.sharding import PartitionSpec as P

MESH = pl.DeviceIdType.MESH
BF16, F32 = jnp.bfloat16, jnp.float32
CHUNKS = 4
ACT_PARTS = 4
DN, UP = 0, 1
RIGHT, LEFT = 0, 1


def aligned(value, unit):
    return pl.multiple_of(value, unit)


class Dims:
    def __init__(self, fs, tp, tokens, d, hidden):
        self.fs, self.tp = fs, tp
        self.ny, self.nc = 2, 2
        self.nz, self.nx = fs // 2, tp // 2
        self.t, self.d, self.h = tokens, d, hidden
        self.rows = tokens * tp
        self.all_rows = self.rows * self.ny
        self.hh = hidden // self.ny
        self.df = d // fs
        self.dz = self.df * self.ny
        self.half = tokens // 2
        self.hc = self.hh // CHUNKS
        self.ha = self.hh // ACT_PARTS


def kernel(
    m, inp, act, og, upw, dnw, ig_out, ug_out, dg_out,
    og_all, in_all, acts, hid, pre, dn_all, up_all,
    part_dn, part_up, slot_dn, slot_up, crecv, xr1, yr1, yr2, xr2,
    loc, ag_s, ag_r, wy_s, wy_r, tok_s, tok_r, act_s, act_r,
    rs_s, rs_r, fin_s, fin_r, fin_l, igc_s, igc_r, igx_s, igx_r,
):
    f, tt = lax.axis_index("fs"), lax.axis_index("tp")
    ny, nx, nz = m.ny, m.nx, m.nz
    z, y = f // ny, f % ny
    x, c = tt // 2, tt % 2
    yo, co = 1 - y, 1 - c
    sends = []

    def at(zz, yy, xx, cc):
        return (zz * ny + yy, xx * 2 + cc)

    y_dev, c_dev = at(z, yo, x, c), at(z, y, x, co)
    z_dev = (at(z + 1, y, x, c), at(z - 1, y, x, c))
    has_z = (z < nz - 1, z > 0)

    def x_at(k):
        return lax.rem(x + k, nx)

    def remote(src, dst, ss, rs, dev):
        return pltpu.make_async_remote_copy(
            src_ref=src, dst_ref=dst, send_sem=ss, recv_sem=rs,
            device_id=dev, device_id_type=MESH,
        )

    def go(copy, cond=None, group=sends):
        if cond is None:
            copy.start()
        else:
            pl.when(cond)(copy.start)
        group.append((cond, copy))

    def drain(group):
        for cond, copy in group:
            if cond is None:
                copy.wait_send()
            else:
                pl.when(cond)(copy.wait_send)
        group.clear()

    barrier = pltpu.get_barrier_semaphore()
    peers = [(None, y_dev), (None, c_dev)]
    peers += [(None, at(z, y, x_at(k), c)) for k in range(1, nx)]
    peers += [(has_z[RIGHT], z_dev[RIGHT]), (has_z[LEFT], z_dev[LEFT])]
    for cond, dev in peers:
        def hello(dev=dev):
            pl.semaphore_signal(barrier, inc=1, device_id=dev, device_id_type=MESH)
        hello() if cond is None else pl.when(cond)(hello)
    lines = jnp.where(z > 0, 1, 0) + jnp.where(z < nz - 1, 1, 0)
    pl.semaphore_wait(barrier, 1 + nx + lines)

    def slot(buf, yy, xx, cc):
        start = aligned(((yy * nx + xx) * 2 + cc) * m.t, m.t)
        return buf.at[pl.ds(start, m.t), :]

    parts_of = (1, 2)

    def weight_view(w, ff, h=None):
        start, size = ff * m.df, m.df
        if w == DN:
            return dn_all.at[:, pl.ds(aligned(start, m.df), m.df)]
        if h is not None:
            size = m.df // parts_of[w]
            start = start + h * size
        return up_all.at[pl.ds(aligned(start, size), size), :]

    def weight_own(w, yy, h=None):
        start = aligned(yy * m.hh, m.hh)
        if w == DN:
            return dnw.at[pl.ds(start, m.hh), :]
        first, size = 0, m.df
        if h is not None:
            size = m.df // parts_of[w]
            first = h * size
        return upw.at[pl.ds(first, size), pl.ds(start, m.hh)]

    def ag(w, u, h, side, k, receive=False):
        back = k + 1 if receive else k
        origin = jnp.clip(z - back if side == RIGHT else z + back, 0, nz - 1)
        view = weight_view(w, origin * ny + (y if u == 0 else yo), h)
        src = weight_own(w, y, h) if (u == 0 and k == 0) else view
        return remote(src, view, ag_s.at[w, u, h, side, k], ag_r.at[w, u, h, side, k],
                      z_dev[side])

    def ag_sends(side, k):
        if side == RIGHT:
            return jnp.logical_and(z >= k, z < nz - 1)
        return jnp.logical_and(z <= nz - 1 - k, z > 0)

    def ag_step(w, u, h, k, where="all"):
        outer = (z == 0, z == nz - 1)
        inner = jnp.logical_and(z > 0, z < nz - 1)
        close = (z < nz // 2, z >= nz // 2)
        for side in (RIGHT, LEFT):
            cond = ag_sends(side, k)
            if where == "edge":
                cond = outer[side]
            if where == "inner":
                cond = inner
            if where == "near":
                cond = jnp.logical_and(cond, close[side])
            if where == "far":
                cond = jnp.logical_and(cond, close[1 - side])
            if k > 0:
                pl.when(cond)(ag(w, u, h, side, k - 1, True).wait_recv)
            go(ag(w, u, h, side, k), cond)

    def ag_finish(w, u, h):
        for k in range(nz - 1):
            pl.when(jnp.logical_and(z == nz - 1, z >= k + 1))(
                ag(w, u, h, RIGHT, k, True).wait_recv)
            pl.when(jnp.logical_and(z == 0, z <= nz - 2 - k))(
                ag(w, u, h, LEFT, k, True).wait_recv)

    def weight_y(w, receive=False):
        ff = z * ny + (yo if receive else y)
        return remote(weight_own(w, yo), weight_view(w, ff), wy_s.at[w], wy_r.at[w], y_dev)

    class Rows:
        def __init__(self, a, src, buf, pieces):
            self.a, self.buf, self.sends = a, buf, []
            self.pieces, self.width, self.source = pieces, m.d // pieces, src

        def go(self, copy):
            go(copy, None, self.sends)

        def drain(self):
            drain(self.sends)

        def src(self, p):
            return self.source.at[:, pl.ds(p * self.width, self.width)]

        def place(self, p, yy, xx, cc):
            start = aligned(((yy * nx + xx) * 2 + cc) * m.t, m.t)
            return self.buf.at[pl.ds(start, m.t), pl.ds(p * self.width, self.width)]

        def copy(self, p, index, src, where, dev):
            index = index * self.pieces + p
            return remote(src, self.place(p, *where), tok_s.at[self.a, index],
                          tok_r.at[self.a, index], dev)

        def over_y(self, p, receive=False):
            return self.copy(p, 0, self.src(p), (yo if receive else y, x, c), y_dev)

        def over_x(self, p, j, k, receive=False):
            yy = y if j == 0 else yo
            xx = x_at(nx - k) if receive else x
            src = self.src(p) if j == 0 else self.place(p, yy, x, c)
            index = 1 + j * (nx - 1) + k - 1
            return self.copy(p, index, src, (yy, xx, c), at(z, y, x_at(k), c))

        def over_c(self, p, j, k, receive=False):
            yy = y if j == 0 else yo
            xx = x_at(nx - k) if k else x
            src = self.src(p) if j == 0 and k == 0 else self.place(p, yy, xx, c)
            index = 1 + 2 * (nx - 1) + j * nx + k
            return self.copy(p, index, src, (yy, xx, co if receive else c), c_dev)

        def start_y(self, p):
            self.go(self.over_y(p))

        def start_x(self, p):
            for k in range(1, nx):
                self.go(self.over_x(p, 0, k))
            self.go(self.over_c(p, 0, 0))

        def relay_y(self, p):
            self.over_y(p, True).wait_recv()
            for k in range(1, nx):
                self.go(self.over_x(p, 1, k))
            self.go(self.over_c(p, 1, 0))

        def relay_x(self, p, j):
            for k in range(1, nx):
                self.over_x(p, j, k, True).wait_recv()
                self.go(self.over_c(p, j, k))

        def finish(self, p):
            for j in range(ny):
                for k in range(nx):
                    self.over_c(p, j, k, True).wait_recv()

    og_rows = Rows(0, og, og_all, nz)
    in_rows = Rows(1, inp, in_all, 1)

    def act_copy(part, receive=False):
        col = part * m.ha
        src = act.at[:, pl.ds(aligned(yo * m.hh + col, m.ha), m.ha)]
        row = aligned((yo if receive else y) * m.rows, m.rows)
        dst = acts.at[pl.ds(row, m.rows), pl.ds(col, m.ha)]
        return remote(src, dst, act_s.at[part], act_r.at[part], y_dev)

    local = [
        pltpu.make_async_copy(weight_own(DN, y), weight_view(DN, f), loc.at[0]),
        pltpu.make_async_copy(weight_own(UP, y), weight_view(UP, f), loc.at[1]),
        pltpu.make_async_copy(og, slot(og_all, y, x, c), loc.at[2]),
        pltpu.make_async_copy(inp, slot(in_all, y, x, c), loc.at[3]),
        pltpu.make_async_copy(
            act.at[:, pl.ds(aligned(y * m.hh, m.hh), m.hh)],
            acts.at[pl.ds(aligned(y * m.rows, m.rows), m.rows), :], loc.at[4]),
    ]

    parts, slots = (part_dn, part_up), (slot_dn, slot_up)

    def rs(w, side, target, ch, own):
        src = (parts if own else slots)[w].at[target, ch]
        if side == RIGHT:
            place = target
        else:
            place = jnp.where(target == z - 1, nz, target)
        return remote(src, slots[w].at[place, ch], rs_s.at[w, side, target, ch],
                      rs_r.at[w, side, target, ch], z_dev[side])

    def rs_waits(w, side, target, ch, place):
        return remote(parts[w].at[0, ch], slots[w].at[place, ch],
                      rs_s.at[w, side, target, ch], rs_r.at[w, side, target, ch],
                      z_dev[side])

    def by_rows(count, step, body):
        @pl.loop(0, count // step)
        def _(i):
            body(pl.ds(aligned(i * step, step), step))

    def rs_edge(w, target, ch):
        @pl.when(jnp.logical_and(z == 0, target > 0))
        def _():
            rs(w, RIGHT, target, ch, True).start()

        @pl.when(jnp.logical_and(z == nz - 1, target < nz - 1))
        def _():
            rs(w, LEFT, target, ch, True).start()

    def rs_pass(w, side, step, ch):
        target = nz - 1 - step if side == RIGHT else step
        if side == RIGHT:
            cond = jnp.logical_and(z > 0, z < target)
        else:
            cond = jnp.logical_and(z < nz - 1, z > target)

        @pl.when(cond)
        def _():
            rs_waits(w, side, target, ch, target).wait_recv()
            buf, own = slots[w].at[target, ch], parts[w].at[target, ch]

            def add(rows):
                buf[rows, :] = (buf[rows, :].astype(F32)
                                + own[rows, :].astype(F32)).astype(BF16)
            by_rows(buf.shape[0], 64, add)
            rs(w, side, target, ch, False).start()

    def near(w, ch, first=0, last=nz - 2):
        @pl.when(z < nz // 2)
        def _():
            for step in range(first, last):
                rs_pass(w, RIGHT, step, ch)

        @pl.when(z >= nz // 2)
        def _():
            for step in range(first, last):
                rs_pass(w, LEFT, step, ch)

    def far(w, ch):
        @pl.when(z < nz // 2)
        def _():
            for step in range(nz - 2):
                rs_pass(w, LEFT, step, ch)

        @pl.when(z >= nz // 2)
        def _():
            for step in range(nz - 2):
                rs_pass(w, RIGHT, step, ch)

    def rs_drain(w):
        for target in range(nz):
            @pl.loop(0, CHUNKS)
            def _(ch):
                pl.when(z < target)(rs(w, RIGHT, target, ch, False).wait_send)
                pl.when(z > target)(rs(w, LEFT, target, ch, False).wait_send)

    def fin_copy(w, ch, yy, receive=False):
        src = parts[w].at[z, ch]
        if w == DN:
            src = src.at[:, pl.ds(aligned(yy * m.df, m.df), m.df)]
            row = aligned((yo if receive else y) * m.hh + ch * m.hc, m.hc)
            return src, dg_out.at[pl.ds(row, m.hc), :]
        src = src.at[pl.ds(aligned(yy * m.df, m.df), m.df), :]
        col = aligned((yo if receive else y) * m.hh + ch * m.hc, m.hc)
        return src, ug_out.at[:, pl.ds(col, m.hc)]

    def fin_remote(w, ch, receive=False):
        src, dst = fin_copy(w, ch, yo, receive)
        return remote(src, dst, fin_s.at[w, ch], fin_r.at[w, ch], y_dev)

    def fin_local(w, ch):
        src, dst = fin_copy(w, ch, y)
        return pltpu.make_async_copy(src, dst, fin_l.at[w, ch])

    def rs_finish(w, ch):
        own = parts[w].at[z, ch]
        right, left = slots[w].at[z, ch], slots[w].at[nz, ch]
        pl.when(z > 0)(rs_waits(w, RIGHT, z, ch, z).wait_recv)
        pl.when(z < nz - 1)(rs_waits(w, LEFT, z, ch, nz).wait_recv)

        def total(*others):
            def add(rows):
                value = own[rows, :].astype(F32)
                for other in others:
                    value = value + other[rows, :].astype(F32)
                own[rows, :] = value.astype(BF16)
            by_rows(own.shape[0], 64, add)

        pl.when(z == 0)(lambda: total(left))
        pl.when(z == nz - 1)(lambda: total(right))
        pl.when(jnp.logical_and(z > 0, z < nz - 1))(lambda: total(right, left))
        fin_remote(w, ch).start()
        fin_local(w, ch).start()

    def fin_wait(w):
        @pl.loop(0, CHUNKS)
        def _(ch):
            fin_remote(w, ch).wait_send()
            fin_remote(w, ch, True).wait_recv()
            fin_local(w, ch).wait()

    def targets(i):
        turn = i // 2
        return jnp.where(i % 2 == 0, nz - 1 - turn, turn)

    order = [nz - 1 - i // 2 if i % 2 == 0 else i // 2 for i in range(nz)]

    def squares(ch):
        cols = pl.ds(ch * m.hc, m.hc)

        def body(rows):
            active = jnp.maximum(acts[rows, cols].astype(F32), 0.0)
            hid[rows, cols] = (active * active).astype(BF16)
        by_rows(m.all_rows, 64, body)

    def dot_rows(a, b):
        return lax.dot_general(a, b, (((0,), (0,)), ((), ())), preferred_element_type=F32)

    def dot_cols(a, b):
        return lax.dot_general(a, b, (((1,), (1,)), ((), ())), preferred_element_type=F32)

    def dot_dn(ch, first=0, last=nz):
        @pl.loop(first, last)
        def _(i):
            target = targets(i)
            a = hid[:, pl.ds(ch * m.hc, m.hc)]
            b = og_all[:, pl.ds(aligned(target * m.dz, m.dz), m.dz)]
            part_dn[target, ch] = dot_rows(a, b).astype(BF16)
            rs_edge(DN, target, ch)

    def dot_hg(ch):
        cols = pl.ds(ch * m.hc, m.hc)

        @pl.loop(0, m.all_rows // 512)
        def _(i):
            rows = pl.ds(aligned(i * 512, 512), 512)
            active = jnp.maximum(acts[rows, cols].astype(F32), 0.0)
            grad = dot_cols(og_all[rows, :], dn_all[cols, :])
            pre[rows, cols] = (2.0 * active * grad).astype(BF16)

    def dot_up(ch):
        @pl.loop(0, nz)
        def _(i):
            target = targets(i)
            a = in_all[:, pl.ds(aligned(target * m.dz, m.dz), m.dz)]
            b = pre[:, pl.ds(ch * m.hc, m.hc)]
            part_up[target, ch] = dot_rows(a, b).astype(BF16)
            rs_edge(UP, target, ch)

    part = og_all
    width = m.d // 2
    sets = [pl.ds(0, width), pl.ds(width, width)]

    def ig_c(g, j):
        yy, xx = j // nx, j % nx
        return remote(slot(part, yy, xx, co).at[:, sets[g]], crecv.at[yy, xx, :, sets[g]],
                      igc_s.at[g, j], igc_r.at[g, j], c_dev)

    def dot_in(g, remote_half):
        piece = m.df // 2
        group = 4
        tile = piece * group
        cc = co if remote_half else c
        count = m.fs // group

        @pl.loop(0, ny * count)
        def _(i):
            yy, n = i // count, i % count
            cols = pl.ds(aligned(g * width + n * tile, tile), tile)
            blocks = [pl.ds(aligned(((yy * nx + xx) * 2 + cc) * m.t, m.t), m.t)
                      for xx in range(nx)]
            rows_of = [pl.ds(aligned((n * group + q) * m.df + g * piece, piece), piece)
                       for q in range(group)]
            a = jnp.concatenate([pre[rows, :] for rows in blocks], 0)
            b = jnp.concatenate([up_all[rows, :] for rows in rows_of], 0)
            value = dot_cols(a, b).astype(BF16)
            for xx, rows in enumerate(blocks):
                part[rows, cols] = value[xx * m.t:(xx + 1) * m.t]
            if remote_half:
                @pl.when(n == count - 1)
                def _():
                    for xx in range(nx):
                        ig_c(g, yy * nx + xx).start()

    def ig_sum(g):
        @pl.loop(0, ny * nx)
        def _(j):
            ig_c(g, j).wait_recv()
            buf = crecv.at[j // nx, j % nx, :, sets[g]]
            own = slot(part, j // nx, j % nx, c).at[:, sets[g]]

            def add(rows):
                buf[rows, :] = (buf[rows, :].astype(F32) + own[rows, :].astype(F32)).astype(BF16)
            by_rows(m.t, 32, add)

    low, high = pl.ds(0, m.half), pl.ds(m.half, m.half)

    def accumulate(dst, others):
        def add(rows):
            value = dst[rows, :].astype(F32)
            for other in others:
                value = value + other[rows, :].astype(F32)
            dst[rows, :] = value.astype(BF16)
        by_rows(m.half, 32, add)

    def ig_x1(g, k):
        return remote(crecv.at[:, x_at(k), low, sets[g]], xr1.at[k - 1, :, :, sets[g]],
                      igx_s.at[g, 0, k], igx_r.at[g, 0, k], at(z, y, x_at(k), c))

    def ig_y1(g):
        return remote(crecv.at[yo, x, low, sets[g]], yr1.at[:, sets[g]],
                      igx_s.at[g, 1, 0], igx_r.at[g, 1, 0], y_dev)

    def ig_y2(g):
        return remote(crecv.at[yo, :, high, sets[g]], yr2.at[:, :, sets[g]],
                      igx_s.at[g, 2, 0], igx_r.at[g, 2, 0], y_dev)

    def ig_x2(g, k):
        return remote(crecv.at[y, x_at(k), high, sets[g]], xr2.at[k - 1, :, sets[g]],
                      igx_s.at[g, 3, k], igx_r.at[g, 3, k], at(z, y, x_at(k), c))

    def ig_first(g):
        for k in range(1, nx):
            go(ig_x1(g, k))
        go(ig_y2(g))

    def ig_second(g):
        for k in range(1, nx):
            ig_x1(g, k).wait_recv()
        for yy in range(ny):
            accumulate(crecv.at[yy, x, low, sets[g]],
                       [xr1.at[k, yy, :, sets[g]] for k in range(nx - 1)])
        go(ig_y1(g))
        ig_y2(g).wait_recv()
        for xx in range(nx):
            accumulate(crecv.at[y, xx, high, sets[g]], [yr2.at[xx, :, sets[g]]])
        for k in range(1, nx):
            go(ig_x2(g, k))

    ig_local = [
        pltpu.make_async_copy(crecv.at[y, x, :, sets[g]], ig_out.at[:, sets[g]], loc.at[5 + g])
        for g in range(2)
    ]

    def ig_last(g):
        ig_y1(g).wait_recv()
        accumulate(crecv.at[y, x, low, sets[g]], [yr1.at[:, sets[g]]])
        for k in range(1, nx):
            ig_x2(g, k).wait_recv()
        accumulate(crecv.at[y, x, high, sets[g]],
                   [xr2.at[k, :, sets[g]] for k in range(nx - 1)])
        ig_local[g].start()

    def acts_in(index):
        act_copy(index, True).wait_recv()

    def start():
        ag_step(DN, 0, 0, 0)
        for p in order[:2]:
            og_rows.start_y(p)
            og_rows.start_x(p)
        go(act_copy(0))
        go(weight_y(DN))
        for p in order[2:]:
            og_rows.start_y(p)
        go(act_copy(1))
        go(weight_y(UP))
        go(act_copy(2))
        in_rows.start_y(0)
        go(act_copy(3))
        ag_step(UP, 0, 0, 0, "edge")
        ag_step(UP, 0, 1, 0, "edge")
        for copy in local:
            copy.start()

    def first_rows():
        for p in order[:2]:
            og_rows.relay_y(p)
            og_rows.relay_x(p, 0)
        for p in order[2:]:
            og_rows.start_x(p)

    def first_rows_in():
        for p in order[:2]:
            og_rows.relay_x(p, 1)
        for p in order[:2]:
            og_rows.finish(p)

    def more_rows(p):
        og_rows.relay_y(p)
        og_rows.relay_x(p, 0)

    def more_rows_in(p):
        og_rows.relay_x(p, 1)
        og_rows.finish(p)

    def local_wait():
        for copy in local:
            copy.wait()

    def weight_in(w):
        weight_y(w, True).wait_recv()

    def ig_drain():
        for g in range(2):
            @pl.loop(0, ny * nx)
            def _(j):
                ig_c(g, j).wait_send()
            ig_local[g].wait()

    def gather_on(w, u, h):
        near_steps = [(ag_step, w, u, h, k, "near") for k in range(2, nz // 2)]
        return near_steps + [(ag_step, w, u, h, k, "far") for k in range(2, nz - 1)]

    plan = [
        (start,),
        (first_rows,),
        (ag_step, DN, 0, 0, 1),
        (first_rows_in,),
        (local_wait,),
        (acts_in, 0),
        (squares, 0),
        (dot_dn, 0, 0, 2),
        *gather_on(DN, 0, 0),
        (weight_in, DN),
        (ag_step, DN, 1, 0, 0),
        (near, DN, 0, 0, 1),
        *[(more_rows, p) for p in order[2:]],
        (in_rows.start_x, 0),
        *[call for i, p in enumerate(order[2:])
          for call in ((more_rows_in, p), (dot_dn, 0, i + 2, i + 3))],
        (ag_step, DN, 1, 0, 1),
        (acts_in, 1),
        (squares, 1),
        (dot_dn, 1),
        (near, DN, 0, 1, nz - 2),
        *gather_on(DN, 1, 0),
        (weight_in, UP),
        (ag_step, UP, 1, 0, 0, "edge"),
        (ag_step, UP, 1, 1, 0, "edge"),
        (ag_step, UP, 0, 0, 0, "inner"),
        (ag_step, UP, 1, 0, 0, "inner"),
        (ag_step, UP, 0, 0, 1, "near"),
        (acts_in, 2),
        (squares, 2),
        (dot_dn, 2),
        (near, DN, 1),
        (ag_step, UP, 0, 0, 1, "far"),
        (ag_step, UP, 1, 0, 1, "near"),
        (ag_finish, DN, 0, 0),
        (ag_finish, DN, 1, 0),
        (dot_hg, 0),
        (dot_hg, 1),
        (dot_hg, 2),
        (ag_step, UP, 1, 0, 1, "far"),
        (ag_step, UP, 0, 1, 0, "inner"),
        (ag_step, UP, 1, 1, 0, "inner"),
        (ag_step, UP, 0, 1, 1, "near"),
        (ag_step, UP, 1, 1, 1, "near"),
        (in_rows.relay_y, 0),
        (in_rows.relay_x, 0, 0),
        *gather_on(UP, 0, 0),
        *gather_on(UP, 1, 0),
        (acts_in, 3),
        (squares, 3),
        (dot_dn, 3),
        (dot_hg, 3),
        (near, DN, 2),
        (in_rows.relay_x, 0, 1),
        (in_rows.finish, 0),
        (dot_up, 0),
        (ag_step, UP, 0, 1, 1, "far"),
        (dot_up, 1),
        (near, DN, 3),
        (ag_step, UP, 1, 1, 1, "far"),
        (ag_finish, UP, 0, 0),
        (ag_finish, UP, 1, 0),
        (og_rows.drain,),
        (dot_in, 0, True),
        *gather_on(UP, 0, 1),
        (dot_in, 0, False),
        (dot_up, 2),
        *gather_on(UP, 1, 1),
        (ig_sum, 0),
        (ig_first, 0),
        (dot_up, 3),
        (far, DN, 0),
        (far, DN, 1),
        (near, UP, 0),
        (ig_second, 0),
        (ag_finish, UP, 0, 1),
        (ag_finish, UP, 1, 1),
        (dot_in, 1, True),
        (dot_in, 1, False),
        (far, DN, 2),
        (far, DN, 3),
        (ig_sum, 1),
        (ig_first, 1),
        (far, UP, 0),
        (near, UP, 1),
        (ig_last, 0),
        (rs_finish, DN, 0),
        (rs_finish, DN, 1),
        (far, UP, 1),
        (ig_second, 1),
        (rs_finish, DN, 2),
        (rs_finish, DN, 3),
        (near, UP, 2),
        (ig_last, 1),
        (far, UP, 2),
        (rs_finish, UP, 0),
        (near, UP, 3, 0, 1),
        (rs_finish, UP, 1),
        (near, UP, 3, 1, nz - 2),
        (far, UP, 3),
        (rs_finish, UP, 2),
        (rs_finish, UP, 3),
        (in_rows.drain,),
        (drain, sends),
        (ig_drain,),
        (rs_drain, DN),
        (rs_drain, UP),
        (fin_wait, DN),
        (fin_wait, UP),
    ]
    for index, (function, *args) in enumerate(plan):
        tags = [str(arg) for arg in args if not isinstance(arg, list)]
        label = "_".join([str(index), function.__name__, *tags])
        with jax.named_scope(label):
            function(*args)


def local_step(fs, tp, inp, act, og, upw, dnw):
    m = Dims(fs, tp, og.shape[0], og.shape[1], act.shape[1])
    dma = pltpu.SemaphoreType.DMA
    vm = pltpu.VMEM
    any_space = pl.BlockSpec(memory_space=pl.ANY)
    rows_events = 1 + 2 * (m.nx - 1) + m.ny * m.nx
    flops = 8 * m.all_rows * m.hh * m.d
    ig, ug, dg = pl.pallas_call(
        functools.partial(kernel, m),
        name="ffn_backward",
        out_shape=(
            jax.ShapeDtypeStruct((m.t, m.d), BF16),
            jax.ShapeDtypeStruct((m.df, m.h), BF16),
            jax.ShapeDtypeStruct((m.h, m.df), BF16),
        ),
        in_specs=[any_space] * 5,
        out_specs=(any_space,) * 3,
        scratch_shapes=[
            vm((m.all_rows, m.d), BF16),
            vm((m.all_rows, m.d), BF16),
            vm((m.all_rows, m.hh), BF16),
            vm((m.all_rows, m.hh), BF16),
            vm((m.all_rows, m.hh), BF16),
            vm((m.hh, m.d), BF16),
            vm((m.d, m.hh), BF16),
            vm((m.nz, CHUNKS, m.hc, m.dz), BF16),
            vm((m.nz, CHUNKS, m.dz, m.hc), BF16),
            vm((m.nz + 1, CHUNKS, m.hc, m.dz), BF16),
            vm((m.nz + 1, CHUNKS, m.dz, m.hc), BF16),
            vm((m.ny, m.nx, m.t, m.d), BF16),
            vm((m.nx - 1, m.ny, m.half, m.d), BF16),
            vm((m.half, m.d), BF16),
            vm((m.nx, m.half, m.d), BF16),
            vm((m.nx - 1, m.half, m.d), BF16),
            dma((7,)),
            dma((2, m.ny, 2, 2, m.nz - 1)),
            dma((2, m.ny, 2, 2, m.nz - 1)),
            dma((2,)),
            dma((2,)),
            dma((2, rows_events * m.nz)),
            dma((2, rows_events * m.nz)),
            dma((ACT_PARTS,)),
            dma((ACT_PARTS,)),
            dma((2, 2, m.nz, CHUNKS)),
            dma((2, 2, m.nz, CHUNKS)),
            dma((2, CHUNKS)),
            dma((2, CHUNKS)),
            dma((2, CHUNKS)),
            dma((2, m.ny * m.nx)),
            dma((2, m.ny * m.nx)),
            dma((2, 4, m.nx)),
            dma((2, 4, m.nx)),
        ],
        cost_estimate=pl.CostEstimate(flops=flops, bytes_accessed=2**25, transcendentals=0),
        compiler_params=pltpu.CompilerParams(
            collective_id=0, has_side_effects=True, vmem_limit_bytes=67043328
        ),
    )(inp, act, og, upw, dnw)
    ig = ig.reshape(m.t, 2, m.fs, m.df // 2).transpose(0, 2, 1, 3).reshape(m.t, m.d)
    return ig, ug.astype(F32), dg.astype(F32)


def solution(mesh):
    placed = (
        P(("fs", "tp"), None),
        P("fs", "tp"),
        P(("fs", "tp"), None),
        P("fs", "tp"),
        P("tp", "fs"),
    )
    return jax.shard_map(
        functools.partial(local_step, mesh.shape["fs"], mesh.shape["tp"]),
        mesh=mesh,
        in_specs=placed,
        out_specs=(P(("fs", "tp"), None), P("fs", "tp"), P("tp", "fs")),
        check_vma=False,
    )
```

```python
import functools

import jax
import jax.numpy as jnp
from jax import lax
from jax.experimental import pallas as pl
from jax.experimental.pallas import tpu as pltpu
from jax.sharding import PartitionSpec as P

MESH = pl.DeviceIdType.MESH
BF16, F32 = jnp.bfloat16, jnp.float32
CHUNKS = 4
ACT_PARTS = 4
DN, UP = 0, 1
RIGHT, LEFT = 0, 1


def aligned(value, unit):
    return pl.multiple_of(value, unit)


class Dims:
    def __init__(self, fs, tp, tokens, d, hidden):
        self.fs, self.tp = fs, tp
        self.ny, self.nc = 2, 2
        self.nz, self.nx = fs // 2, tp // 2
        self.t, self.d, self.h = tokens, d, hidden
        self.rows = tokens * tp
        self.all_rows = self.rows * self.ny
        self.hh = hidden // self.ny
        self.df = d // fs
        self.dz = self.df * self.ny
        self.half = tokens // 2
        self.hc = self.hh // CHUNKS
        self.ha = self.hh // ACT_PARTS
        self.direct = (self.df // 2) % 128 == 0


def kernel(
    m, inp, act, og, upw, dnw, ig_out, ug_out, dg_out,
    og_all, in_all, acts, hid, pre, dn_all, up_all,
    part_dn, part_up, slot_dn, slot_up, crecv, xr1, yr1, yr2, xr2,
    loc, ag_s, ag_r, wy_s, wy_r, tok_s, tok_r, act_s, act_r,
    rs_s, rs_r, fin_s, fin_r, fin_l, igc_s, igc_r, igx_s, igx_r,
):
    f, tt = lax.axis_index("fs"), lax.axis_index("tp")
    ny, nx, nz = m.ny, m.nx, m.nz
    z, y = f // ny, f % ny
    x, c = tt // 2, tt % 2
    yo, co = 1 - y, 1 - c
    sends = []

    def at(zz, yy, xx, cc):
        return (zz * ny + yy, xx * 2 + cc)

    y_dev, c_dev = at(z, yo, x, c), at(z, y, x, co)
    z_dev = (at(z + 1, y, x, c), at(z - 1, y, x, c))
    has_z = (z < nz - 1, z > 0)

    def x_at(k):
        return lax.rem(x + k, nx)

    def mirror(target):
        return jnp.where(z < nz // 2, target, nz - 1 - target)

    order = [mirror(nz - 1 - i // 2 if i % 2 == 0 else i // 2) for i in range(nz)]

    def remote(src, dst, ss, rs, dev):
        return pltpu.make_async_remote_copy(
            src_ref=src, dst_ref=dst, send_sem=ss, recv_sem=rs,
            device_id=dev, device_id_type=MESH,
        )

    def go(copy, cond=None, group=sends):
        if cond is None:
            copy.start()
        else:
            pl.when(cond)(copy.start)
        group.append((cond, copy))

    def drain(group):
        for cond, copy in group:
            if cond is None:
                copy.wait_send()
            else:
                pl.when(cond)(copy.wait_send)
        group.clear()

    barrier = pltpu.get_barrier_semaphore()
    peers = [(None, y_dev), (None, c_dev)]
    peers += [(None, at(z, y, x_at(k), c)) for k in range(1, nx)]
    peers += [(has_z[RIGHT], z_dev[RIGHT]), (has_z[LEFT], z_dev[LEFT])]
    for cond, dev in peers:
        def hello(dev=dev):
            pl.semaphore_signal(barrier, inc=1, device_id=dev, device_id_type=MESH)
        hello() if cond is None else pl.when(cond)(hello)
    lines = jnp.where(z > 0, 1, 0) + jnp.where(z < nz - 1, 1, 0)
    pl.semaphore_wait(barrier, 1 + nx + lines)

    def slot(buf, yy, xx, cc):
        start = aligned(((yy * nx + xx) * 2 + cc) * m.t, m.t)
        return buf.at[pl.ds(start, m.t), :]

    parts_of = (1, 2)

    def weight_view(w, ff, h=None):
        start, size = ff * m.df, m.df
        if w == DN:
            return dn_all.at[:, pl.ds(aligned(start, m.df), m.df)]
        if h is not None:
            size = m.df // parts_of[w]
            start = start + h * size
        return up_all.at[pl.ds(aligned(start, size), size), :]

    def weight_own(w, yy, h=None):
        start = aligned(yy * m.hh, m.hh)
        if w == DN:
            return dnw.at[pl.ds(start, m.hh), :]
        first, size = 0, m.df
        if h is not None:
            size = m.df // parts_of[w]
            first = h * size
        return upw.at[pl.ds(first, size), pl.ds(start, m.hh)]

    def ag(w, u, h, side, k, receive=False):
        back = k + 1 if receive else k
        origin = jnp.clip(z - back if side == RIGHT else z + back, 0, nz - 1)
        view = weight_view(w, origin * ny + (y if u == 0 else yo), h)
        src = weight_own(w, y, h) if (u == 0 and k == 0) else view
        return remote(src, view, ag_s.at[w, u, h, side, k], ag_r.at[w, u, h, side, k],
                      z_dev[side])

    def ag_sends(side, k):
        if side == RIGHT:
            return jnp.logical_and(z >= k, z < nz - 1)
        return jnp.logical_and(z <= nz - 1 - k, z > 0)

    def ag_step(w, u, h, k, where="all"):
        outer = (z == 0, z == nz - 1)
        inner = jnp.logical_and(z > 0, z < nz - 1)
        close = (z < nz // 2, z >= nz // 2)
        for side in (RIGHT, LEFT):
            cond = ag_sends(side, k)
            if where == "edge":
                cond = outer[side]
            if where == "inner":
                cond = inner
            if where == "near":
                cond = jnp.logical_and(cond, close[side])
            if where == "far":
                cond = jnp.logical_and(cond, close[1 - side])
            if k > 0:
                pl.when(cond)(ag(w, u, h, side, k - 1, True).wait_recv)
            go(ag(w, u, h, side, k), cond)

    def ag_finish(w, u, h):
        for k in range(nz - 1):
            pl.when(jnp.logical_and(z == nz - 1, z >= k + 1))(
                ag(w, u, h, RIGHT, k, True).wait_recv)
            pl.when(jnp.logical_and(z == 0, z <= nz - 2 - k))(
                ag(w, u, h, LEFT, k, True).wait_recv)

    def weight_y(w, receive=False):
        ff = z * ny + (yo if receive else y)
        return remote(weight_own(w, yo), weight_view(w, ff), wy_s.at[w], wy_r.at[w], y_dev)

    class Rows:
        def __init__(self, a, src, buf, pieces):
            self.a, self.buf, self.sends = a, buf, []
            self.pieces, self.width, self.source = pieces, m.d // pieces, src

        def go(self, copy):
            go(copy, None, self.sends)

        def drain(self):
            drain(self.sends)

        def cols(self, p):
            return pl.ds(aligned(p * self.width, self.width), self.width)

        def src(self, p):
            return self.source.at[:, self.cols(p)]

        def place(self, p, yy, xx, cc):
            start = aligned(((yy * nx + xx) * 2 + cc) * m.t, m.t)
            return self.buf.at[pl.ds(start, m.t), self.cols(p)]

        def copy(self, p, index, src, where, dev):
            index = index * self.pieces + p
            return remote(src, self.place(p, *where), tok_s.at[self.a, index],
                          tok_r.at[self.a, index], dev)

        def over_y(self, p, receive=False):
            return self.copy(p, 0, self.src(p), (yo if receive else y, x, c), y_dev)

        def over_x(self, p, j, k, receive=False):
            yy = y if j == 0 else yo
            xx = x_at(nx - k) if receive else x
            src = self.src(p) if j == 0 else self.place(p, yy, x, c)
            index = 1 + j * (nx - 1) + k - 1
            return self.copy(p, index, src, (yy, xx, c), at(z, y, x_at(k), c))

        def over_c(self, p, j, k, receive=False):
            yy = y if j == 0 else yo
            xx = x_at(nx - k) if k else x
            src = self.src(p) if j == 0 and k == 0 else self.place(p, yy, xx, c)
            index = 1 + 2 * (nx - 1) + j * nx + k
            return self.copy(p, index, src, (yy, xx, co if receive else c), c_dev)

        def start_y(self, p):
            self.go(self.over_y(p))

        def start_x(self, p):
            for k in range(1, nx):
                self.go(self.over_x(p, 0, k))
            self.go(self.over_c(p, 0, 0))

        def relay_y(self, p):
            self.over_y(p, True).wait_recv()
            for k in range(1, nx):
                self.go(self.over_x(p, 1, k))
            self.go(self.over_c(p, 1, 0))

        def relay_x(self, p, j):
            for k in range(1, nx):
                self.over_x(p, j, k, True).wait_recv()
                self.go(self.over_c(p, j, k))

        def finish(self, p):
            for j in range(ny):
                for k in range(nx):
                    self.over_c(p, j, k, True).wait_recv()

    og_rows = Rows(0, og, og_all, nz)
    in_rows = Rows(1, inp, in_all, 1)

    def act_copy(part, receive=False):
        col = part * m.ha
        src = act.at[:, pl.ds(aligned(yo * m.hh + col, m.ha), m.ha)]
        row = aligned((yo if receive else y) * m.rows, m.rows)
        dst = acts.at[pl.ds(row, m.rows), pl.ds(col, m.ha)]
        return remote(src, dst, act_s.at[part], act_r.at[part], y_dev)

    local = [
        pltpu.make_async_copy(weight_own(DN, y), weight_view(DN, f), loc.at[0, 0]),
        pltpu.make_async_copy(weight_own(UP, y), weight_view(UP, f), loc.at[1, 0]),
        pltpu.make_async_copy(og, slot(og_all, y, x, c), loc.at[2, 0]),
        pltpu.make_async_copy(inp, slot(in_all, y, x, c), loc.at[3, 0]),
        pltpu.make_async_copy(
            act.at[:, pl.ds(aligned(y * m.hh, m.hh), m.hh)],
            acts.at[pl.ds(aligned(y * m.rows, m.rows), m.rows), :], loc.at[4, 0]),
    ]

    parts, slots = (part_dn, part_up), (slot_dn, slot_up)

    def rs(w, side, target, ch, own):
        src = (parts if own else slots)[w].at[target, ch]
        if side == RIGHT:
            place = target
        else:
            place = jnp.where(target == z - 1, nz, target)
        return remote(src, slots[w].at[place, ch], rs_s.at[w, side, target, ch],
                      rs_r.at[w, side, target, ch], z_dev[side])

    def rs_waits(w, side, target, ch, place):
        return remote(parts[w].at[0, ch], slots[w].at[place, ch],
                      rs_s.at[w, side, target, ch], rs_r.at[w, side, target, ch],
                      z_dev[side])

    def by_rows(count, step, body):
        @pl.loop(0, count // step)
        def _(i):
            body(pl.ds(aligned(i * step, step), step))

    def rs_edge(w, target, ch):
        @pl.when(jnp.logical_and(z == 0, target > 0))
        def _():
            rs(w, RIGHT, target, ch, True).start()

        @pl.when(jnp.logical_and(z == nz - 1, target < nz - 1))
        def _():
            rs(w, LEFT, target, ch, True).start()

    def rs_pass(w, side, step, ch):
        target = nz - 1 - step if side == RIGHT else step
        if side == RIGHT:
            cond = jnp.logical_and(z > 0, z < target)
        else:
            cond = jnp.logical_and(z < nz - 1, z > target)

        @pl.when(cond)
        def _():
            rs_waits(w, side, target, ch, target).wait_recv()
            buf, own = slots[w].at[target, ch], parts[w].at[target, ch]

            def add(rows):
                buf[rows, :] = (buf[rows, :].astype(F32)
                                + own[rows, :].astype(F32)).astype(BF16)
            by_rows(buf.shape[0], 64, add)
            rs(w, side, target, ch, False).start()

    def near(w, ch, first=0, last=nz - 2):
        @pl.when(z < nz // 2)
        def _():
            for step in range(first, last):
                rs_pass(w, RIGHT, step, ch)

        @pl.when(z >= nz // 2)
        def _():
            for step in range(first, last):
                rs_pass(w, LEFT, step, ch)

    def far(w, ch):
        @pl.when(z < nz // 2)
        def _():
            for step in range(nz - 2):
                rs_pass(w, LEFT, step, ch)

        @pl.when(z >= nz // 2)
        def _():
            for step in range(nz - 2):
                rs_pass(w, RIGHT, step, ch)

    def rs_drain(w):
        for target in range(nz):
            @pl.loop(0, CHUNKS)
            def _(ch):
                pl.when(z < target)(rs(w, RIGHT, target, ch, False).wait_send)
                pl.when(z > target)(rs(w, LEFT, target, ch, False).wait_send)

    def fin_copy(w, ch, yy, receive=False):
        src = parts[w].at[z, ch]
        if w == DN:
            src = src.at[:, pl.ds(aligned(yy * m.df, m.df), m.df)]
            row = aligned((yo if receive else y) * m.hh + ch * m.hc, m.hc)
            return src, dg_out.at[pl.ds(row, m.hc), :]
        src = src.at[pl.ds(aligned(yy * m.df, m.df), m.df), :]
        col = aligned((yo if receive else y) * m.hh + ch * m.hc, m.hc)
        return src, ug_out.at[:, pl.ds(col, m.hc)]

    def fin_remote(w, ch, receive=False):
        src, dst = fin_copy(w, ch, yo, receive)
        return remote(src, dst, fin_s.at[w, ch], fin_r.at[w, ch], y_dev)

    def fin_local(w, ch):
        src, dst = fin_copy(w, ch, y)
        return pltpu.make_async_copy(src, dst, fin_l.at[w, ch])

    def rs_finish(w, ch):
        own = parts[w].at[z, ch]
        right, left = slots[w].at[z, ch], slots[w].at[nz, ch]
        pl.when(z > 0)(rs_waits(w, RIGHT, z, ch, z).wait_recv)
        pl.when(z < nz - 1)(rs_waits(w, LEFT, z, ch, nz).wait_recv)

        def total(*others):
            def add(rows):
                value = own[rows, :].astype(F32)
                for other in others:
                    value = value + other[rows, :].astype(F32)
                own[rows, :] = value.astype(BF16)
            by_rows(own.shape[0], 64, add)

        pl.when(z == 0)(lambda: total(left))
        pl.when(z == nz - 1)(lambda: total(right))
        pl.when(jnp.logical_and(z > 0, z < nz - 1))(lambda: total(right, left))
        fin_remote(w, ch).start()
        fin_local(w, ch).start()

    def fin_wait(w):
        @pl.loop(0, CHUNKS)
        def _(ch):
            fin_remote(w, ch).wait_send()
            fin_remote(w, ch, True).wait_recv()
            fin_local(w, ch).wait()

    def targets(i):
        turn = i // 2
        return mirror(jnp.where(i % 2 == 0, nz - 1 - turn, turn))

    def squares(ch):
        cols = pl.ds(ch * m.hc, m.hc)

        def body(rows):
            active = jnp.maximum(acts[rows, cols].astype(F32), 0.0)
            hid[rows, cols] = (active * active).astype(BF16)
        by_rows(m.all_rows, 64, body)

    def dot_rows(a, b):
        return lax.dot_general(a, b, (((0,), (0,)), ((), ())), preferred_element_type=F32)

    def dot_cols(a, b):
        return lax.dot_general(a, b, (((1,), (1,)), ((), ())), preferred_element_type=F32)

    def dot_dn(ch, first=0, last=nz):
        @pl.loop(first, last)
        def _(i):
            target = targets(i)
            a = hid[:, pl.ds(ch * m.hc, m.hc)]
            b = og_all[:, pl.ds(aligned(target * m.dz, m.dz), m.dz)]
            part_dn[target, ch] = dot_rows(a, b).astype(BF16)
            rs_edge(DN, target, ch)

    def dot_hg(ch):
        cols = pl.ds(ch * m.hc, m.hc)

        @pl.loop(0, m.all_rows // 512)
        def _(i):
            rows = pl.ds(aligned(i * 512, 512), 512)
            active = jnp.maximum(acts[rows, cols].astype(F32), 0.0)
            grad = dot_cols(og_all[rows, :], dn_all[cols, :])
            pre[rows, cols] = (2.0 * active * grad).astype(BF16)

    def dot_up(ch, send=True):
        @pl.loop(0, nz)
        def _(i):
            target = targets(i)
            a = in_all[:, pl.ds(aligned(target * m.dz, m.dz), m.dz)]
            b = pre[:, pl.ds(ch * m.hc, m.hc)]
            part_up[target, ch] = dot_rows(a, b).astype(BF16)
            if send:
                rs_edge(UP, target, ch)

    def up_sends(first):
        @pl.loop(0, nz * (CHUNKS - first))
        def _(i):
            count = CHUNKS - first
            rs_edge(UP, targets(i // count), first + i % count)

    part = og_all
    width = m.d // 2
    sets = [pl.ds(0, width), pl.ds(width, width)]

    def ig_c(g, j):
        yy, xx = j // nx, j % nx
        return remote(slot(part, yy, xx, co).at[:, sets[g]], crecv.at[yy, xx, :, sets[g]],
                      igc_s.at[g, j], igc_r.at[g, j], c_dev)

    def dot_in(g, remote_half):
        piece = m.df // 2
        group = 4
        tile = piece * group
        cc = co if remote_half else c
        count = m.fs // group

        @pl.loop(0, ny * count)
        def _(i):
            yy, n = i // count, i % count
            cols = pl.ds(aligned(g * width + n * tile, tile), tile)
            blocks = [pl.ds(aligned(((yy * nx + xx) * 2 + cc) * m.t, m.t), m.t)
                      for xx in range(nx)]
            rows_of = [pl.ds(aligned((n * group + q) * m.df + g * piece, piece), piece)
                       for q in range(group)]
            a = jnp.concatenate([pre[rows, :] for rows in blocks], 0)
            b = jnp.concatenate([up_all[rows, :] for rows in rows_of], 0)
            value = dot_cols(a, b).astype(BF16)
            for xx, rows in enumerate(blocks):
                part[rows, cols] = value[xx * m.t:(xx + 1) * m.t]
            if remote_half:
                @pl.when(n == count - 1)
                def _():
                    for xx in range(nx):
                        ig_c(g, yy * nx + xx).start()

    def ig_sum(g):
        @pl.loop(0, ny * nx)
        def _(j):
            ig_c(g, j).wait_recv()
            buf = crecv.at[j // nx, j % nx, :, sets[g]]
            own = slot(part, j // nx, j % nx, c).at[:, sets[g]]

            def add(rows):
                buf[rows, :] = (buf[rows, :].astype(F32) + own[rows, :].astype(F32)).astype(BF16)
            by_rows(m.t, 32, add)

    low, high = pl.ds(0, m.half), pl.ds(m.half, m.half)

    def accumulate(dst, others):
        def add(rows):
            value = dst[rows, :].astype(F32)
            for other in others:
                value = value + other[rows, :].astype(F32)
            dst[rows, :] = value.astype(BF16)
        by_rows(m.half, 32, add)

    def ig_x1(g, k):
        return remote(crecv.at[:, x_at(k), low, sets[g]], xr1.at[k - 1, :, :, sets[g]],
                      igx_s.at[g, 0, k], igx_r.at[g, 0, k], at(z, y, x_at(k), c))

    def ig_y1(g):
        return remote(crecv.at[yo, x, low, sets[g]], yr1.at[:, sets[g]],
                      igx_s.at[g, 1, 0], igx_r.at[g, 1, 0], y_dev)

    def ig_y2(g):
        return remote(crecv.at[yo, :, high, sets[g]], yr2.at[:, :, sets[g]],
                      igx_s.at[g, 2, 0], igx_r.at[g, 2, 0], y_dev)

    def ig_x2(g, k):
        return remote(crecv.at[y, x_at(k), high, sets[g]], xr2.at[k - 1, :, sets[g]],
                      igx_s.at[g, 3, k], igx_r.at[g, 3, k], at(z, y, x_at(k), c))

    def ig_first(g):
        for k in range(1, nx):
            go(ig_x1(g, k))
        go(ig_y2(g))

    def ig_second(g):
        for k in range(1, nx):
            ig_x1(g, k).wait_recv()
        for yy in range(ny):
            accumulate(crecv.at[yy, x, low, sets[g]],
                       [xr1.at[k, yy, :, sets[g]] for k in range(nx - 1)])
        go(ig_y1(g))
        ig_y2(g).wait_recv()
        for xx in range(nx):
            accumulate(crecv.at[y, xx, high, sets[g]], [yr2.at[xx, :, sets[g]]])
        for k in range(1, nx):
            go(ig_x2(g, k))

    piece = m.df // 2

    def ig_local(g):
        mine = crecv.at[y, x]
        if not m.direct:
            return [pltpu.make_async_copy(mine.at[:, sets[g]], ig_out.at[:, sets[g]],
                                          loc.at[5 + g, 0])]
        return [
            pltpu.make_async_copy(
                mine.at[:, pl.ds(g * width + n * piece, piece)],
                ig_out.at[:, pl.ds(n * m.df + g * piece, piece)], loc.at[5 + g, n])
            for n in range(m.fs)
        ]

    def ig_last(g):
        ig_y1(g).wait_recv()
        accumulate(crecv.at[y, x, low, sets[g]], [yr1.at[:, sets[g]]])
        for k in range(1, nx):
            ig_x2(g, k).wait_recv()
        accumulate(crecv.at[y, x, high, sets[g]],
                   [xr2.at[k, :, sets[g]] for k in range(nx - 1)])
        for copy in ig_local(g):
            copy.start()

    def acts_in(index):
        act_copy(index, True).wait_recv()

    def start():
        ag_step(DN, 0, 0, 0)
        for p in order[:2]:
            og_rows.start_y(p)
            og_rows.start_x(p)
        go(act_copy(0))
        go(weight_y(DN))
        for p in order[2:]:
            og_rows.start_y(p)
        go(act_copy(1))
        go(weight_y(UP))
        go(act_copy(2))
        in_rows.start_y(0)
        go(act_copy(3))
        ag_step(UP, 0, 0, 0)
        ag_step(UP, 0, 1, 0)
        for copy in local:
            copy.start()

    def first_rows():
        for p in order[:2]:
            og_rows.relay_y(p)
            og_rows.relay_x(p, 0)
        for p in order[2:]:
            og_rows.start_x(p)

    def first_rows_in():
        for p in order[:2]:
            og_rows.relay_x(p, 1)
        for p in order[:2]:
            og_rows.finish(p)

    def more_rows(p):
        og_rows.relay_y(p)
        og_rows.relay_x(p, 0)

    def more_rows_in(p):
        og_rows.relay_x(p, 1)
        og_rows.finish(p)

    def local_wait():
        for copy in local:
            copy.wait()

    def weight_in(w):
        weight_y(w, True).wait_recv()

    def ig_drain():
        for g in range(2):
            @pl.loop(0, ny * nx)
            def _(j):
                ig_c(g, j).wait_send()
            for copy in ig_local(g):
                copy.wait()

    def gather_on(w, u, h):
        near_steps = [(ag_step, w, u, h, k, "near") for k in range(2, nz // 2)]
        return near_steps + [(ag_step, w, u, h, k, "far") for k in range(2, nz - 1)]

    plan = [
        (start,),
        (first_rows,),
        (ag_step, DN, 0, 0, 1),
        (first_rows_in,),
        (local_wait,),
        (acts_in, 0),
        (squares, 0),
        (dot_dn, 0, 0, 2),
        *gather_on(DN, 0, 0),
        (weight_in, DN),
        (ag_step, DN, 1, 0, 0),
        (near, DN, 0, 0, 1),
        *[(more_rows, p) for p in order[2:]],
        (in_rows.start_x, 0),
        *[call for i, p in enumerate(order[2:])
          for call in ((more_rows_in, p), (dot_dn, 0, i + 2, i + 3))],
        (ag_step, DN, 1, 0, 1),
        (acts_in, 1),
        (squares, 1),
        (dot_dn, 1),
        (near, DN, 0, 1, nz - 2),
        *gather_on(DN, 1, 0),
        (weight_in, UP),
        (ag_step, UP, 1, 0, 0, "edge"),
        (ag_step, UP, 1, 1, 0, "edge"),
        (ag_step, UP, 1, 0, 0, "inner"),
        (ag_step, UP, 0, 0, 1, "near"),
        (acts_in, 2),
        (squares, 2),
        (dot_dn, 2),
        (near, DN, 1),
        (ag_step, UP, 0, 0, 1, "far"),
        (ag_step, UP, 1, 0, 1, "near"),
        (ag_finish, DN, 0, 0),
        (ag_finish, DN, 1, 0),
        (dot_hg, 0),
        (dot_hg, 1),
        (dot_hg, 2),
        (ag_step, UP, 1, 0, 1, "far"),
        (ag_step, UP, 1, 1, 0, "inner"),
        (ag_step, UP, 0, 1, 1, "near"),
        (ag_step, UP, 1, 1, 1, "near"),
        (in_rows.relay_y, 0),
        (in_rows.relay_x, 0, 0),
        *gather_on(UP, 0, 0),
        *gather_on(UP, 1, 0),
        (acts_in, 3),
        (squares, 3),
        (dot_dn, 3),
        (dot_hg, 3),
        (near, DN, 2),
        (in_rows.relay_x, 0, 1),
        (in_rows.finish, 0),
        (dot_up, 0),
        (ag_step, UP, 0, 1, 1, "far"),
        (dot_up, 1),
        (near, DN, 3),
        (ag_step, UP, 1, 1, 1, "far"),
        (ag_finish, UP, 0, 0),
        (ag_finish, UP, 1, 0),
        (og_rows.drain,),
        (dot_in, 0, True),
        *gather_on(UP, 0, 1),
        (dot_in, 0, False),
        (dot_up, 2, False),
        *gather_on(UP, 1, 1),
        (ig_sum, 0),
        (ig_first, 0),
        (dot_up, 3, False),
        (up_sends, 2),
        (far, DN, 0),
        (far, DN, 1),
        (near, UP, 0),
        (ig_second, 0),
        (ag_finish, UP, 0, 1),
        (ag_finish, UP, 1, 1),
        (dot_in, 1, True),
        (dot_in, 1, False),
        (far, DN, 2),
        (far, DN, 3),
        (ig_sum, 1),
        (ig_first, 1),
        (far, UP, 0),
        (near, UP, 1),
        (ig_last, 0),
        (rs_finish, DN, 0),
        (rs_finish, DN, 1),
        (far, UP, 1),
        (ig_second, 1),
        (rs_finish, DN, 2),
        (rs_finish, DN, 3),
        (near, UP, 2, 0, 1),
        (ig_last, 1),
        (near, UP, 3, 0, 1),
        (rs_finish, UP, 0),
        (near, UP, 2, 1, nz - 2),
        (far, UP, 2),
        (rs_finish, UP, 1),
        (near, UP, 3, 1, nz - 2),
        (far, UP, 3),
        (rs_finish, UP, 2),
        (rs_finish, UP, 3),
        (in_rows.drain,),
        (drain, sends),
        (ig_drain,),
        (rs_drain, DN),
        (rs_drain, UP),
        (fin_wait, DN),
        (fin_wait, UP),
    ]
    for index, (function, *args) in enumerate(plan):
        tags = [str(arg) for arg in args if isinstance(arg, (int, str))]
        label = "_".join([str(index), function.__name__, *tags])
        with jax.named_scope(label):
            function(*args)


def local_step(fs, tp, inp, act, og, upw, dnw):
    m = Dims(fs, tp, og.shape[0], og.shape[1], act.shape[1])
    dma = pltpu.SemaphoreType.DMA
    vm = pltpu.VMEM
    any_space = pl.BlockSpec(memory_space=pl.ANY)
    rows_events = 1 + 2 * (m.nx - 1) + m.ny * m.nx
    flops = 8 * m.all_rows * m.hh * m.d
    ig, ug, dg = pl.pallas_call(
        functools.partial(kernel, m),
        name="ffn_backward",
        out_shape=(
            jax.ShapeDtypeStruct((m.t, m.d), BF16),
            jax.ShapeDtypeStruct((m.df, m.h), BF16),
            jax.ShapeDtypeStruct((m.h, m.df), BF16),
        ),
        in_specs=[any_space] * 5,
        out_specs=(any_space,) * 3,
        scratch_shapes=[
            vm((m.all_rows, m.d), BF16),
            vm((m.all_rows, m.d), BF16),
            vm((m.all_rows, m.hh), BF16),
            vm((m.all_rows, m.hh), BF16),
            vm((m.all_rows, m.hh), BF16),
            vm((m.hh, m.d), BF16),
            vm((m.d, m.hh), BF16),
            vm((m.nz, CHUNKS, m.hc, m.dz), BF16),
            vm((m.nz, CHUNKS, m.dz, m.hc), BF16),
            vm((m.nz + 1, CHUNKS, m.hc, m.dz), BF16),
            vm((m.nz + 1, CHUNKS, m.dz, m.hc), BF16),
            vm((m.ny, m.nx, m.t, m.d), BF16),
            vm((m.nx - 1, m.ny, m.half, m.d), BF16),
            vm((m.half, m.d), BF16),
            vm((m.nx, m.half, m.d), BF16),
            vm((m.nx - 1, m.half, m.d), BF16),
            dma((7, m.fs)),
            dma((2, m.ny, 2, 2, m.nz - 1)),
            dma((2, m.ny, 2, 2, m.nz - 1)),
            dma((2,)),
            dma((2,)),
            dma((2, rows_events * m.nz)),
            dma((2, rows_events * m.nz)),
            dma((ACT_PARTS,)),
            dma((ACT_PARTS,)),
            dma((2, 2, m.nz, CHUNKS)),
            dma((2, 2, m.nz, CHUNKS)),
            dma((2, CHUNKS)),
            dma((2, CHUNKS)),
            dma((2, CHUNKS)),
            dma((2, m.ny * m.nx)),
            dma((2, m.ny * m.nx)),
            dma((2, 4, m.nx)),
            dma((2, 4, m.nx)),
        ],
        cost_estimate=pl.CostEstimate(flops=flops, bytes_accessed=2**25, transcendentals=0),
        compiler_params=pltpu.CompilerParams(
            collective_id=0, has_side_effects=True, vmem_limit_bytes=67043328
        ),
    )(inp, act, og, upw, dnw)
    if not m.direct:
        ig = ig.reshape(m.t, 2, m.fs, m.df // 2).transpose(0, 2, 1, 3)
        ig = ig.reshape(m.t, m.d)
    return ig, ug.astype(F32), dg.astype(F32)


def solution(mesh):
    placed = (
        P(("fs", "tp"), None),
        P("fs", "tp"),
        P(("fs", "tp"), None),
        P("fs", "tp"),
        P("tp", "fs"),
    )
    return jax.shard_map(
        functools.partial(local_step, mesh.shape["fs"], mesh.shape["tp"]),
        mesh=mesh,
        in_specs=placed,
        out_specs=(P(("fs", "tp"), None), P("fs", "tp"), P("tp", "fs")),
        check_vma=False,
    )
```

```python
import functools

import jax
import jax.numpy as jnp
from jax import lax
from jax.experimental import pallas as pl
from jax.experimental.pallas import tpu as pltpu
from jax.sharding import PartitionSpec as P

MESH = pl.DeviceIdType.MESH
BF16, F32 = jnp.bfloat16, jnp.float32
CHUNKS = 4
ACT_PARTS = 4
DN, UP = 0, 1
RIGHT, LEFT = 0, 1


def aligned(value, unit):
    return pl.multiple_of(value, unit)


class Dims:
    def __init__(self, fs, tp, tokens, d, hidden):
        self.fs, self.tp = fs, tp
        self.ny, self.nc = 2, 2
        self.nz, self.nx = fs // 2, tp // 2
        self.t, self.d, self.h = tokens, d, hidden
        self.rows = tokens * tp
        self.all_rows = self.rows * self.ny
        self.hh = hidden // self.ny
        self.df = d // fs
        self.dz = self.df * self.ny
        self.half = tokens // 2
        self.hc = self.hh // CHUNKS
        self.ha = self.hh // ACT_PARTS
        self.direct = (self.df // 2) % 128 == 0


def kernel(
    m, inp, act, og, upw, dnw, ig_out, ug_out, dg_out,
    og_all, in_all, acts, hid, pre, dn_all, up_all,
    part_dn, part_up, slot_dn, slot_up, crecv, xr1, yr1, yr2, xr2,
    loc, ag_s, ag_r, wy_s, wy_r, tok_s, tok_r, act_s, act_r,
    rs_s, rs_r, fin_s, fin_r, igc_s, igc_r, igx_s, igx_r,
):
    f, tt = lax.axis_index("fs"), lax.axis_index("tp")
    ny, nx, nz = m.ny, m.nx, m.nz
    z, y = f // ny, f % ny
    x, c = tt // 2, tt % 2
    yo, co = 1 - y, 1 - c
    sends = []

    def at(zz, yy, xx, cc):
        return (zz * ny + yy, xx * 2 + cc)

    y_dev, c_dev = at(z, yo, x, c), at(z, y, x, co)
    z_dev = (at(z + 1, y, x, c), at(z - 1, y, x, c))
    has_z = (z < nz - 1, z > 0)

    def x_at(k):
        return lax.rem(x + k, nx)

    def mirror(target):
        return jnp.where(z < nz // 2, target, nz - 1 - target)

    order = [mirror(nz - 1 - i // 2 if i % 2 == 0 else i // 2) for i in range(nz)]

    def remote(src, dst, ss, rs, dev):
        return pltpu.make_async_remote_copy(
            src_ref=src, dst_ref=dst, send_sem=ss, recv_sem=rs,
            device_id=dev, device_id_type=MESH,
        )

    def go(copy, cond=None, group=sends):
        if cond is None:
            copy.start()
        else:
            pl.when(cond)(copy.start)
        group.append((cond, copy))

    def drain(group):
        for cond, copy in group:
            if cond is None:
                copy.wait_send()
            else:
                pl.when(cond)(copy.wait_send)
        group.clear()

    barrier = pltpu.get_barrier_semaphore()
    peers = [(None, y_dev), (None, c_dev)]
    peers += [(None, at(z, y, x_at(k), c)) for k in range(1, nx)]
    peers += [(has_z[RIGHT], z_dev[RIGHT]), (has_z[LEFT], z_dev[LEFT])]
    for cond, dev in peers:
        def hello(dev=dev):
            pl.semaphore_signal(barrier, inc=1, device_id=dev, device_id_type=MESH)
        hello() if cond is None else pl.when(cond)(hello)
    lines = jnp.where(z > 0, 1, 0) + jnp.where(z < nz - 1, 1, 0)
    pl.semaphore_wait(barrier, 1 + nx + lines)

    def slot(buf, yy, xx, cc):
        start = aligned(((yy * nx + xx) * 2 + cc) * m.t, m.t)
        return buf.at[pl.ds(start, m.t), :]

    parts_of = (1, 2)

    def weight_view(w, ff, h=None):
        start, size = ff * m.df, m.df
        if w == DN:
            return dn_all.at[:, pl.ds(aligned(start, m.df), m.df)]
        if h is not None:
            size = m.df // parts_of[w]
            start = start + h * size
        return up_all.at[pl.ds(aligned(start, size), size), :]

    def weight_own(w, yy, h=None):
        start = aligned(yy * m.hh, m.hh)
        if w == DN:
            return dnw.at[pl.ds(start, m.hh), :]
        first, size = 0, m.df
        if h is not None:
            size = m.df // parts_of[w]
            first = h * size
        return upw.at[pl.ds(first, size), pl.ds(start, m.hh)]

    def ag(w, u, h, side, k, receive=False):
        back = k + 1 if receive else k
        origin = jnp.clip(z - back if side == RIGHT else z + back, 0, nz - 1)
        view = weight_view(w, origin * ny + (y if u == 0 else yo), h)
        src = weight_own(w, y, h) if (u == 0 and k == 0) else view
        unit = u if w == DN else ny + 2 * u + h
        return remote(src, view, ag_s.at[unit, side, k], ag_r.at[unit, origin], z_dev[side])

    def ag_sends(side, k):
        if side == RIGHT:
            return jnp.logical_and(z >= k, z < nz - 1)
        return jnp.logical_and(z <= nz - 1 - k, z > 0)

    def ag_step(w, u, h, k, where="all"):
        outer = (z == 0, z == nz - 1)
        inner = jnp.logical_and(z > 0, z < nz - 1)
        close = (z < nz // 2, z >= nz // 2)
        for side in (RIGHT, LEFT):
            cond = ag_sends(side, k)
            if where == "edge":
                cond = outer[side]
            if where == "inner":
                cond = inner
            if where == "near":
                cond = jnp.logical_and(cond, close[side])
            if where == "far":
                cond = jnp.logical_and(cond, close[1 - side])
            if k > 0:
                pl.when(cond)(ag(w, u, h, side, k - 1, True).wait_recv)
            go(ag(w, u, h, side, k), cond)

    def ag_finish(w, u, h):
        for k in range(nz - 1):
            pl.when(jnp.logical_and(z == nz - 1, z >= k + 1))(
                ag(w, u, h, RIGHT, k, True).wait_recv)
            pl.when(jnp.logical_and(z == 0, z <= nz - 2 - k))(
                ag(w, u, h, LEFT, k, True).wait_recv)

    def weight_y(w, receive=False):
        ff = z * ny + (yo if receive else y)
        return remote(weight_own(w, yo), weight_view(w, ff), wy_s.at[w], wy_r.at[w], y_dev)

    class Rows:
        def __init__(self, a, src, buf, pieces):
            self.a, self.buf = a, buf
            self.pieces, self.width, self.source = pieces, m.d // pieces, src

        def drain(self):
            count = 4 * nx - 1
            every = self.buf.at[pl.ds(0, count * m.t), :]
            remote(every, every, tok_s.at[self.a], tok_r.at[nz, 0], y_dev).wait_send()

        def cols(self, p):
            return pl.ds(aligned(p * self.width, self.width), self.width)

        def src(self, p):
            return self.source.at[:, self.cols(p)]

        def place(self, p, yy, xx, cc):
            start = aligned(((yy * nx + xx) * 2 + cc) * m.t, m.t)
            return self.buf.at[pl.ds(start, m.t), self.cols(p)]

        def copy(self, p, index, src, where, dev):
            row = p if self.a == 0 else nz
            return remote(src, self.place(p, *where), tok_s.at[self.a],
                          tok_r.at[row, index], dev)

        def over_y(self, p, receive=False):
            return self.copy(p, 0, self.src(p), (yo if receive else y, x, c), y_dev)

        def over_x(self, p, j, k, receive=False):
            yy = y if j == 0 else yo
            xx = x_at(nx - k) if receive else x
            src = self.src(p) if j == 0 else self.place(p, yy, x, c)
            index = 1 + j * (nx - 1) + k - 1
            return self.copy(p, index, src, (yy, xx, c), at(z, y, x_at(k), c))

        def over_c(self, p, j, k):
            yy = y if j == 0 else yo
            xx = x_at(nx - k) if k else x
            src = self.src(p) if j == 0 and k == 0 else self.place(p, yy, xx, c)
            return self.copy(p, 2 * nx - 1, src, (yy, xx, c), c_dev)

        def start_y(self, p):
            self.over_y(p).start()

        def start_x(self, p):
            for k in range(1, nx):
                self.over_x(p, 0, k).start()
            self.over_c(p, 0, 0).start()

        def relay_y(self, p):
            self.over_y(p, True).wait_recv()
            for k in range(1, nx):
                self.over_x(p, 1, k).start()
            self.over_c(p, 1, 0).start()

        def relay_x(self, p, j):
            for k in range(1, nx):
                self.over_x(p, j, k, True).wait_recv()
                self.over_c(p, j, k).start()

        def finish(self, p):
            row = p if self.a == 0 else nz
            half = self.buf.at[pl.ds(0, 2 * nx * m.t), self.cols(p)]
            remote(half, half, tok_s.at[self.a], tok_r.at[row, 2 * nx - 1], c_dev).wait_recv()

    og_rows = Rows(0, og, og_all, nz)
    in_rows = Rows(1, inp, in_all, 1)

    def act_copy(part, receive=False):
        col = part * m.ha
        src = act.at[:, pl.ds(aligned(yo * m.hh + col, m.ha), m.ha)]
        row = aligned((yo if receive else y) * m.rows, m.rows)
        dst = acts.at[pl.ds(row, m.rows), pl.ds(col, m.ha)]
        return remote(src, dst, act_s, act_r.at[part], y_dev)

    local = [
        pltpu.make_async_copy(weight_own(DN, y), weight_view(DN, f), loc.at[0]),
        pltpu.make_async_copy(weight_own(UP, y), weight_view(UP, f), loc.at[1]),
        pltpu.make_async_copy(og, slot(og_all, y, x, c), loc.at[2]),
        pltpu.make_async_copy(inp, slot(in_all, y, x, c), loc.at[3]),
        pltpu.make_async_copy(
            act.at[:, pl.ds(aligned(y * m.hh, m.hh), m.hh)],
            acts.at[pl.ds(aligned(y * m.rows, m.rows), m.rows), :], loc.at[4]),
    ]

    parts, slots = (part_dn, part_up), (slot_dn, slot_up)

    def rs(w, side, target, ch, own):
        src = (parts if own else slots)[w].at[target, ch]
        if side == RIGHT:
            place = target
        else:
            place = jnp.where(target == z - 1, nz, target)
        return remote(src, slots[w].at[place, ch], rs_s.at[w, target],
                      rs_r.at[w, place, ch], z_dev[side])

    def rs_waits(w, side, ch, place):
        return remote(parts[w].at[0, ch], slots[w].at[place, ch], rs_s.at[w, 0],
                      rs_r.at[w, place, ch], z_dev[side])

    def by_rows(count, step, body):
        @pl.loop(0, count // step)
        def _(i):
            body(pl.ds(aligned(i * step, step), step))

    def rs_edge(w, target, ch):
        @pl.when(jnp.logical_and(z == 0, target > 0))
        def _():
            rs(w, RIGHT, target, ch, True).start()

        @pl.when(jnp.logical_and(z == nz - 1, target < nz - 1))
        def _():
            rs(w, LEFT, target, ch, True).start()

    def rs_pass(w, side, step, ch):
        target = nz - 1 - step if side == RIGHT else step
        if side == RIGHT:
            cond = jnp.logical_and(z > 0, z < target)
        else:
            cond = jnp.logical_and(z < nz - 1, z > target)

        @pl.when(cond)
        def _():
            rs_waits(w, side, ch, target).wait_recv()
            buf, own = slots[w].at[target, ch], parts[w].at[target, ch]

            def add(rows):
                buf[rows, :] = (buf[rows, :].astype(F32)
                                + own[rows, :].astype(F32)).astype(BF16)
            by_rows(buf.shape[0], 64, add)
            rs(w, side, target, ch, False).start()

    def near(w, ch, first=0, last=nz - 2):
        @pl.when(z < nz // 2)
        def _():
            for step in range(first, last):
                rs_pass(w, RIGHT, step, ch)

        @pl.when(z >= nz // 2)
        def _():
            for step in range(first, last):
                rs_pass(w, LEFT, step, ch)

    def far(w, ch):
        @pl.when(z < nz // 2)
        def _():
            for step in range(nz - 2):
                rs_pass(w, LEFT, step, ch)

        @pl.when(z >= nz // 2)
        def _():
            for step in range(nz - 2):
                rs_pass(w, RIGHT, step, ch)

    def rs_drain(w):
        for target in range(nz):
            every = slots[w].at[target]
            pl.when(z != target)(
                remote(every, every, rs_s.at[w, target], rs_r.at[w, 0, 0], y_dev).wait_send)

    def fin_cut(w, buf, yy):
        cut = pl.ds(aligned(yy * m.df, m.df), m.df)
        return buf.at[:, cut] if w == DN else buf.at[cut, :]

    def fin_place(w, ch, yy):
        start = aligned(yy * m.hh + ch * m.hc, m.hc)
        if w == DN:
            return dg_out.at[pl.ds(start, m.hc), :]
        return ug_out.at[:, pl.ds(start, m.hc)]

    def fin_remote(w, ch):
        return remote(fin_cut(w, parts[w].at[z, ch], yo), fin_place(w, ch, y),
                      fin_s.at[w], fin_r.at[w], y_dev)

    def rs_finish(w, ch):
        own = parts[w].at[z, ch]
        right, left = slots[w].at[z, ch], slots[w].at[nz, ch]
        pl.when(z > 0)(rs_waits(w, RIGHT, ch, z).wait_recv)
        pl.when(z < nz - 1)(rs_waits(w, LEFT, ch, nz).wait_recv)

        def total(yy, dst, others):
            terms = [fin_cut(w, buf, yy) for buf in others]

            def add(rows):
                value = terms[0][rows, :].astype(F32)
                for term in terms[1:]:
                    value = value + term[rows, :].astype(F32)
                dst[rows, :] = value.astype(BF16)
            by_rows(terms[0].shape[0], 64, add)

        def both(yy, dst):
            pl.when(z == 0)(lambda: total(yy, dst, (own, left)))
            pl.when(z == nz - 1)(lambda: total(yy, dst, (own, right)))
            pl.when(jnp.logical_and(z > 0, z < nz - 1))(
                lambda: total(yy, dst, (own, right, left)))

        both(yo, fin_cut(w, own, yo))
        fin_remote(w, ch).start()
        both(y, fin_place(w, ch, y))

    def fin_wait(w):
        def half(yy):
            cut = pl.ds(aligned(yy * m.hh, m.hh), m.hh)
            return dg_out.at[cut, :] if w == DN else ug_out.at[:, cut]

        mine, other = half(y), half(yo)
        remote(mine, mine, fin_s.at[w], fin_r.at[w], y_dev).wait_send()
        remote(other, other, fin_s.at[w], fin_r.at[w], y_dev).wait_recv()

    def targets(i):
        turn = i // 2
        return mirror(jnp.where(i % 2 == 0, nz - 1 - turn, turn))

    def squares(ch):
        cols = pl.ds(ch * m.hc, m.hc)

        def body(rows):
            active = jnp.maximum(acts[rows, cols].astype(F32), 0.0)
            hid[rows, cols] = (active * active).astype(BF16)
        by_rows(m.all_rows, 64, body)

    def dot_rows(a, b):
        return lax.dot_general(a, b, (((0,), (0,)), ((), ())), preferred_element_type=F32)

    def dot_cols(a, b):
        return lax.dot_general(a, b, (((1,), (1,)), ((), ())), preferred_element_type=F32)

    def dot_dn(ch, first=0, last=nz):
        @pl.loop(first, last)
        def _(i):
            target = targets(i)
            a = hid[:, pl.ds(ch * m.hc, m.hc)]
            b = og_all[:, pl.ds(aligned(target * m.dz, m.dz), m.dz)]
            part_dn[target, ch] = dot_rows(a, b).astype(BF16)
            rs_edge(DN, target, ch)

    def dot_hg(ch):
        cols = pl.ds(ch * m.hc, m.hc)

        @pl.loop(0, m.all_rows // 512)
        def _(i):
            rows = pl.ds(aligned(i * 512, 512), 512)
            active = jnp.maximum(acts[rows, cols].astype(F32), 0.0)
            grad = dot_cols(og_all[rows, :], dn_all[cols, :])
            pre[rows, cols] = (2.0 * active * grad).astype(BF16)

    def dot_up(ch, send=True):
        @pl.loop(0, nz)
        def _(i):
            target = targets(i)
            a = in_all[:, pl.ds(aligned(target * m.dz, m.dz), m.dz)]
            b = pre[:, pl.ds(ch * m.hc, m.hc)]
            part_up[target, ch] = dot_rows(a, b).astype(BF16)
            if send:
                rs_edge(UP, target, ch)

    def up_sends(first):
        @pl.loop(0, nz * (CHUNKS - first))
        def _(i):
            count = CHUNKS - first
            rs_edge(UP, targets(i // count), first + i % count)

    part = og_all
    width = m.d // 2
    sets = [pl.ds(0, width), pl.ds(width, width)]

    def ig_c(g, j):
        yy, xx = j // nx, j % nx
        return remote(slot(part, yy, xx, co).at[:, sets[g]], crecv.at[yy, xx, :, sets[g]],
                      igc_s.at[g], igc_r.at[g], c_dev)

    def dot_in(g, remote_half):
        piece = m.df // 2
        group = 4
        tile = piece * group
        cc = co if remote_half else c
        count = m.fs // group

        @pl.loop(0, ny * count)
        def _(i):
            yy, n = i // count, i % count
            cols = pl.ds(aligned(g * width + n * tile, tile), tile)
            blocks = [pl.ds(aligned(((yy * nx + xx) * 2 + cc) * m.t, m.t), m.t)
                      for xx in range(nx)]
            rows_of = [pl.ds(aligned((n * group + q) * m.df + g * piece, piece), piece)
                       for q in range(group)]
            a = jnp.concatenate([pre[rows, :] for rows in blocks], 0)
            b = jnp.concatenate([up_all[rows, :] for rows in rows_of], 0)
            value = dot_cols(a, b).astype(BF16)
            for xx, rows in enumerate(blocks):
                part[rows, cols] = value[xx * m.t:(xx + 1) * m.t]
            if remote_half:
                @pl.when(n == count - 1)
                def _():
                    for xx in range(nx):
                        ig_c(g, yy * nx + xx).start()

    def ig_all(g):
        every = crecv.at[:, :, :, sets[g]]
        return remote(every, every, igc_s.at[g], igc_r.at[g], c_dev)

    def ig_sum(g):
        ig_all(g).wait_recv()

        @pl.loop(0, ny * nx)
        def _(j):
            buf = crecv.at[j // nx, j % nx, :, sets[g]]
            own = slot(part, j // nx, j % nx, c).at[:, sets[g]]

            def add(rows):
                buf[rows, :] = (buf[rows, :].astype(F32) + own[rows, :].astype(F32)).astype(BF16)
            by_rows(m.t, 32, add)

    low, high = pl.ds(0, m.half), pl.ds(m.half, m.half)

    def accumulate(dst, others):
        def add(rows):
            value = dst[rows, :].astype(F32)
            for other in others:
                value = value + other[rows, :].astype(F32)
            dst[rows, :] = value.astype(BF16)
        by_rows(m.half, 32, add)

    def ig_x1(g, k):
        return remote(crecv.at[:, x_at(k), low, sets[g]], xr1.at[k - 1, :, :, sets[g]],
                      igx_s.at[g, k - 1], igx_r.at[g, k - 1], at(z, y, x_at(k), c))

    def ig_y1(g):
        return remote(crecv.at[yo, x, low, sets[g]], yr1.at[:, sets[g]],
                      igx_s.at[g, nx - 1], igx_r.at[g, nx - 1], y_dev)

    def ig_y2(g):
        return remote(crecv.at[yo, :, high, sets[g]], yr2.at[:, :, sets[g]],
                      igx_s.at[g, nx], igx_r.at[g, nx], y_dev)

    def ig_x2(g, k):
        return remote(crecv.at[y, x_at(k), high, sets[g]], xr2.at[k - 1, :, sets[g]],
                      igx_s.at[g, nx + k], igx_r.at[g, nx + k], at(z, y, x_at(k), c))

    def ig_first(g):
        for k in range(1, nx):
            go(ig_x1(g, k))
        go(ig_y2(g))

    def ig_second(g):
        for k in range(1, nx):
            ig_x1(g, k).wait_recv()
        for yy in range(ny):
            accumulate(crecv.at[yy, x, low, sets[g]],
                       [xr1.at[k, yy, :, sets[g]] for k in range(nx - 1)])
        go(ig_y1(g))
        ig_y2(g).wait_recv()
        for xx in range(nx):
            accumulate(crecv.at[y, xx, high, sets[g]], [yr2.at[xx, :, sets[g]]])
        for k in range(1, nx):
            go(ig_x2(g, k))

    piece = m.df // 2

    def ig_store(rows, g, value):
        value = value.astype(BF16)
        if not m.direct:
            ig_out[rows, sets[g]] = value
            return
        for n in range(m.fs):
            ig_out[rows, pl.ds(n * m.df + g * piece, piece)] = value[:, n * piece:(n + 1) * piece]

    def ig_final(first, g, terms):
        def add(rows):
            value = terms[0][rows, :].astype(F32)
            for term in terms[1:]:
                value = value + term[rows, :].astype(F32)
            ig_store(pl.ds(aligned(first + rows.start, 32), rows.size), g, value)
        by_rows(m.half, 32, add)

    def ig_last(g):
        ig_y1(g).wait_recv()
        ig_final(0, g, [crecv.at[y, x, low, sets[g]], yr1.at[:, sets[g]]])
        for k in range(1, nx):
            ig_x2(g, k).wait_recv()
        ig_final(m.half, g, [crecv.at[y, x, high, sets[g]]]
                 + [xr2.at[k, :, sets[g]] for k in range(nx - 1)])

    def acts_in(index):
        act_copy(index, True).wait_recv()

    def start():
        ag_step(DN, 0, 0, 0)
        for p in order[:2]:
            og_rows.start_y(p)
            og_rows.start_x(p)
        act_copy(0).start()
        go(weight_y(DN))
        for p in order[2:]:
            og_rows.start_y(p)
        act_copy(1).start()
        go(weight_y(UP))
        act_copy(2).start()
        in_rows.start_y(0)
        act_copy(3).start()
        ag_step(UP, 0, 0, 0)
        ag_step(UP, 0, 1, 0)
        for copy in local:
            copy.start()

    def first_rows():
        for p in order[:2]:
            og_rows.relay_y(p)
            og_rows.relay_x(p, 0)
        for p in order[2:]:
            og_rows.start_x(p)

    def first_rows_in():
        for p in order[:2]:
            og_rows.relay_x(p, 1)
        for p in order[:2]:
            og_rows.finish(p)

    def more_rows(p):
        og_rows.relay_y(p)
        og_rows.relay_x(p, 0)

    def more_rows_in(p):
        og_rows.relay_x(p, 1)
        og_rows.finish(p)

    def local_wait():
        for copy in local:
            copy.wait()

    def weight_in(w):
        weight_y(w, True).wait_recv()

    def act_drain():
        every = acts.at[pl.ds(0, m.rows), :]
        remote(every, every, act_s, act_r.at[0], y_dev).wait_send()

    def ig_drain():
        for g in range(2):
            ig_all(g).wait_send()

    def gather_on(w, u, h):
        near_steps = [(ag_step, w, u, h, k, "near") for k in range(2, nz // 2)]
        return near_steps + [(ag_step, w, u, h, k, "far") for k in range(2, nz - 1)]

    plan = [
        (start,),
        (first_rows,),
        (ag_step, DN, 0, 0, 1),
        (first_rows_in,),
        (local_wait,),
        (acts_in, 0),
        (squares, 0),
        (dot_dn, 0, 0, 2),
        *gather_on(DN, 0, 0),
        (weight_in, DN),
        (ag_step, DN, 1, 0, 0),
        (near, DN, 0, 0, 1),
        *[(more_rows, p) for p in order[2:]],
        (in_rows.start_x, 0),
        *[call for i, p in enumerate(order[2:])
          for call in ((more_rows_in, p), (dot_dn, 0, i + 2, i + 3))],
        (ag_step, DN, 1, 0, 1),
        (acts_in, 1),
        (squares, 1),
        (dot_dn, 1),
        (near, DN, 0, 1, nz - 2),
        *gather_on(DN, 1, 0),
        (weight_in, UP),
        (ag_step, UP, 1, 0, 0, "edge"),
        (ag_step, UP, 1, 1, 0, "edge"),
        (ag_step, UP, 1, 0, 0, "inner"),
        (ag_step, UP, 0, 0, 1, "near"),
        (acts_in, 2),
        (squares, 2),
        (dot_dn, 2),
        (near, DN, 1),
        (ag_step, UP, 0, 0, 1, "far"),
        (ag_step, UP, 1, 0, 1, "near"),
        (ag_finish, DN, 0, 0),
        (ag_finish, DN, 1, 0),
        (dot_hg, 0),
        (dot_hg, 1),
        (dot_hg, 2),
        (ag_step, UP, 1, 0, 1, "far"),
        (ag_step, UP, 1, 1, 0, "inner"),
        (ag_step, UP, 0, 1, 1, "near"),
        (ag_step, UP, 1, 1, 1, "near"),
        (in_rows.relay_y, 0),
        (in_rows.relay_x, 0, 0),
        *gather_on(UP, 0, 0),
        *gather_on(UP, 1, 0),
        (acts_in, 3),
        (squares, 3),
        (dot_dn, 3),
        (dot_hg, 3),
        (near, DN, 2),
        (in_rows.relay_x, 0, 1),
        (in_rows.finish, 0),
        (dot_up, 0),
        (ag_step, UP, 0, 1, 1, "far"),
        (dot_up, 1),
        (near, DN, 3),
        (ag_step, UP, 1, 1, 1, "far"),
        (ag_finish, UP, 0, 0),
        (ag_finish, UP, 1, 0),
        (og_rows.drain,),
        (dot_in, 0, True),
        *gather_on(UP, 0, 1),
        (dot_in, 0, False),
        (dot_up, 2, False),
        *gather_on(UP, 1, 1),
        (ig_sum, 0),
        (ig_first, 0),
        (dot_up, 3, False),
        (up_sends, 2),
        (far, DN, 0),
        (far, DN, 1),
        (near, UP, 0),
        (ig_second, 0),
        (ag_finish, UP, 0, 1),
        (ag_finish, UP, 1, 1),
        (dot_in, 1, True),
        (dot_in, 1, False),
        (far, DN, 2),
        (far, DN, 3),
        (ig_sum, 1),
        (ig_first, 1),
        (far, UP, 0),
        (near, UP, 1),
        (ig_last, 0),
        (rs_finish, DN, 0),
        (rs_finish, DN, 1),
        (far, UP, 1),
        (ig_second, 1),
        (rs_finish, DN, 2),
        (rs_finish, DN, 3),
        (near, UP, 2, 0, 1),
        (ig_last, 1),
        (near, UP, 3, 0, 1),
        (rs_finish, UP, 0),
        (near, UP, 2, 1, nz - 2),
        (far, UP, 2),
        (rs_finish, UP, 1),
        (near, UP, 3, 1, nz - 2),
        (far, UP, 3),
        (rs_finish, UP, 2),
        (rs_finish, UP, 3),
        (in_rows.drain,),
        (drain, sends),
        (act_drain,),
        (ig_drain,),
        (rs_drain, DN),
        (rs_drain, UP),
        (fin_wait, DN),
        (fin_wait, UP),
    ]
    for index, (function, *args) in enumerate(plan):
        tags = [str(arg) for arg in args if isinstance(arg, (int, str))]
        label = "_".join([str(index), function.__name__, *tags])
        with jax.named_scope(label):
            function(*args)


def local_step(fs, tp, inp, act, og, upw, dnw):
    m = Dims(fs, tp, og.shape[0], og.shape[1], act.shape[1])
    dma = pltpu.SemaphoreType.DMA
    vm = pltpu.VMEM
    any_space = pl.BlockSpec(memory_space=pl.ANY)
    flops = 8 * m.all_rows * m.hh * m.d
    ig, ug, dg = pl.pallas_call(
        functools.partial(kernel, m),
        name="ffn_backward",
        out_shape=(
            vm((m.t, m.d), BF16),
            vm((m.df, m.h), BF16),
            vm((m.h, m.df), BF16),
        ),
        in_specs=[any_space] * 5,
        out_specs=(pl.BlockSpec(memory_space=pltpu.VMEM),) * 3,
        scratch_shapes=[
            vm((m.all_rows, m.d), BF16),
            vm((m.all_rows, m.d), BF16),
            vm((m.all_rows, m.hh), BF16),
            vm((m.all_rows, m.hh), BF16),
            vm((m.all_rows, m.hh), BF16),
            vm((m.hh, m.d), BF16),
            vm((m.d, m.hh), BF16),
            vm((m.nz, CHUNKS, m.hc, m.dz), BF16),
            vm((m.nz, CHUNKS, m.dz, m.hc), BF16),
            vm((m.nz + 1, CHUNKS, m.hc, m.dz), BF16),
            vm((m.nz + 1, CHUNKS, m.dz, m.hc), BF16),
            vm((m.ny, m.nx, m.t, m.d), BF16),
            vm((m.nx - 1, m.ny, m.half, m.d), BF16),
            vm((m.half, m.d), BF16),
            vm((m.nx, m.half, m.d), BF16),
            vm((m.nx - 1, m.half, m.d), BF16),
            dma((5,)),
            dma((3 * m.ny, 2, m.nz - 1)),
            dma((3 * m.ny, m.nz)),
            dma((2,)),
            dma((2,)),
            dma((2,)),
            dma((m.nz + 1, 2 * m.nx)),
            dma,
            dma((ACT_PARTS,)),
            dma((2, m.nz)),
            dma((2, m.nz + 1, CHUNKS)),
            dma((2,)),
            dma((2,)),
            dma((2,)),
            dma((2,)),
            dma((2, 2 * m.nx)),
            dma((2, 2 * m.nx)),
        ],
        cost_estimate=pl.CostEstimate(flops=flops, bytes_accessed=2**25, transcendentals=0),
        compiler_params=pltpu.CompilerParams(
            collective_id=0, has_side_effects=True, vmem_limit_bytes=62914560
        ),
    )(inp, act, og, upw, dnw)
    if not m.direct:
        ig = ig.reshape(m.t, 2, m.fs, m.df // 2).transpose(0, 2, 1, 3)
        ig = ig.reshape(m.t, m.d)
    return widen(ig, ug, dg)


def widen(ig, ug, dg):
    steps = 2

    def body(ig_in, ug_in, dg_in, ig_out, ug_out, dg_out, wide_ug, wide_dg, sems):
        copies = [pltpu.make_async_copy(ig_in, ig_out, sems.at[0])]
        copies[0].start()
        pairs = ((ug_in, wide_ug, ug_out), (dg_in, wide_dg, dg_out))
        for which, (src, wide, out) in enumerate(pairs):
            count = src.shape[0] // steps
            for i in range(steps):
                first = i * count
                rows = pl.ds(first, count)

                @pl.loop(0, count // 32)
                def _(j):
                    part = pl.ds(aligned(first + j * 32, 32), 32)
                    wide[part, :] = src[part, :].astype(F32)

                copies.append(pltpu.make_async_copy(
                    wide.at[rows, :], out.at[rows, :], sems.at[1 + which * steps + i]))
                copies[-1].start()
        for copy in copies:
            copy.wait()

    vmem = pl.BlockSpec(memory_space=pltpu.VMEM)
    outside = pl.BlockSpec(memory_space=pl.ANY)
    return pl.pallas_call(
        body,
        name="widen",
        out_shape=(
            jax.ShapeDtypeStruct(ig.shape, BF16),
            jax.ShapeDtypeStruct(ug.shape, F32),
            jax.ShapeDtypeStruct(dg.shape, F32),
        ),
        in_specs=[vmem] * 3,
        out_specs=(outside,) * 3,
        scratch_shapes=[
            pltpu.VMEM(ug.shape, F32),
            pltpu.VMEM(dg.shape, F32),
            pltpu.SemaphoreType.DMA((1 + 2 * steps,)),
        ],
        cost_estimate=pl.CostEstimate(flops=ug.size, bytes_accessed=16 * ug.size, transcendentals=0),
        compiler_params=pltpu.CompilerParams(vmem_limit_bytes=16 * ug.size),
    )(*(pltpu.with_memory_space_constraint(v, pltpu.VMEM) for v in (ig, ug, dg)))


def solution(mesh):
    placed = (
        P(("fs", "tp"), None),
        P("fs", "tp"),
        P(("fs", "tp"), None),
        P("fs", "tp"),
        P("tp", "fs"),
    )
    return jax.shard_map(
        functools.partial(local_step, mesh.shape["fs"], mesh.shape["tp"]),
        mesh=mesh,
        in_specs=placed,
        out_specs=(P(("fs", "tp"), None), P("fs", "tp"), P("tp", "fs")),
        check_vma=False,
    )
```

```python
import functools

import jax
import jax.numpy as jnp
from jax import lax
from jax.experimental import pallas as pl
from jax.experimental.pallas import tpu as pltpu
from jax.sharding import PartitionSpec as P

MESH = pl.DeviceIdType.MESH
BF16, F32 = jnp.bfloat16, jnp.float32
CHUNKS = 4
ACT_PARTS = 4
DN, UP = 0, 1
RIGHT, LEFT = 0, 1


def aligned(value, unit):
    return pl.multiple_of(value, unit)


class Dims:
    def __init__(self, fs, tp, tokens, d, hidden):
        self.fs, self.tp = fs, tp
        self.ny, self.nc = 2, 2
        self.nz, self.nx = fs // 2, tp // 2
        self.t, self.d, self.h = tokens, d, hidden
        self.rows = tokens * tp
        self.all_rows = self.rows * self.ny
        self.hh = hidden // self.ny
        self.df = d // fs
        self.dz = self.df * self.ny
        self.half = tokens // 2
        self.hc = self.hh // CHUNKS
        self.ha = self.hh // ACT_PARTS
        self.direct = (self.df // 2) % 128 == 0


def kernel(
    m, inp, act, og, upw, dnw, ig_out, ug_out, dg_out,
    og_all, in_all, acts, hid, pre, dn_all, up_all,
    part_dn, part_up, slot_dn, slot_up, crecv, xr1, yr1, yr2, xr2,
    loc, ag_s, ag_r, wy_s, wy_r, tok_s, tok_r, act_s, act_r,
    rs_s, rs_r, rs_h, fin_s, fin_r, igc_s, igc_r, igx_s, igx_r,
):
    f, tt = lax.axis_index("fs"), lax.axis_index("tp")
    ny, nx, nz = m.ny, m.nx, m.nz
    z, y = f // ny, f % ny
    x, c = tt // 2, tt % 2
    yo, co = 1 - y, 1 - c
    sends = []

    def at(zz, yy, xx, cc):
        return (zz * ny + yy, xx * 2 + cc)

    y_dev, c_dev = at(z, yo, x, c), at(z, y, x, co)
    z_dev = (at(z + 1, y, x, c), at(z - 1, y, x, c))
    has_z = (z < nz - 1, z > 0)

    def x_at(k):
        return lax.rem(x + k, nx)

    def mirror(target):
        return jnp.where(z < nz // 2, target, nz - 1 - target)

    order = [mirror(nz - 1 - i // 2 if i % 2 == 0 else i // 2) for i in range(nz)]

    def remote(src, dst, ss, rs, dev):
        return pltpu.make_async_remote_copy(
            src_ref=src, dst_ref=dst, send_sem=ss, recv_sem=rs,
            device_id=dev, device_id_type=MESH,
        )

    def go(copy, cond=None, group=sends):
        if cond is None:
            copy.start()
        else:
            pl.when(cond)(copy.start)
        group.append((cond, copy))

    def drain(group):
        for cond, copy in group:
            if cond is None:
                copy.wait_send()
            else:
                pl.when(cond)(copy.wait_send)
        group.clear()

    barrier = pltpu.get_barrier_semaphore()
    peers = [(None, y_dev), (None, c_dev)]
    peers += [(None, at(z, y, x_at(k), c)) for k in range(1, nx)]
    peers += [(has_z[RIGHT], z_dev[RIGHT]), (has_z[LEFT], z_dev[LEFT])]
    for cond, dev in peers:
        def hello(dev=dev):
            pl.semaphore_signal(barrier, inc=1, device_id=dev, device_id_type=MESH)
        hello() if cond is None else pl.when(cond)(hello)
    lines = jnp.where(z > 0, 1, 0) + jnp.where(z < nz - 1, 1, 0)
    pl.semaphore_wait(barrier, 1 + nx + lines)

    def slot(buf, yy, xx, cc):
        start = aligned(((yy * nx + xx) * 2 + cc) * m.t, m.t)
        return buf.at[pl.ds(start, m.t), :]

    parts_of = (1, 2)

    def weight_view(w, ff, h=None):
        start, size = ff * m.df, m.df
        if w == DN:
            return dn_all.at[:, pl.ds(aligned(start, m.df), m.df)]
        if h is not None:
            size = m.df // parts_of[w]
            start = start + h * size
        return up_all.at[pl.ds(aligned(start, size), size), :]

    def weight_own(w, yy, h=None):
        start = aligned(yy * m.hh, m.hh)
        if w == DN:
            return dnw.at[pl.ds(start, m.hh), :]
        first, size = 0, m.df
        if h is not None:
            size = m.df // parts_of[w]
            first = h * size
        return upw.at[pl.ds(first, size), pl.ds(start, m.hh)]

    def ag(w, u, h, side, k, receive=False):
        back = k + 1 if receive else k
        origin = jnp.clip(z - back if side == RIGHT else z + back, 0, nz - 1)
        view = weight_view(w, origin * ny + (y if u == 0 else yo), h)
        src = weight_own(w, y, h) if (u == 0 and k == 0) else view
        unit = u if w == DN else ny + 2 * u + h
        return remote(src, view, ag_s.at[unit, side, k], ag_r.at[unit, origin], z_dev[side])

    def ag_sends(side, k):
        if side == RIGHT:
            return jnp.logical_and(z >= k, z < nz - 1)
        return jnp.logical_and(z <= nz - 1 - k, z > 0)

    def ag_step(w, u, h, k, where="all"):
        outer = (z == 0, z == nz - 1)
        inner = jnp.logical_and(z > 0, z < nz - 1)
        close = (z < nz // 2, z >= nz // 2)
        for side in (RIGHT, LEFT):
            cond = ag_sends(side, k)
            if where == "edge":
                cond = outer[side]
            if where == "inner":
                cond = inner
            if where == "near":
                cond = jnp.logical_and(cond, close[side])
            if where == "far":
                cond = jnp.logical_and(cond, close[1 - side])
            if k > 0:
                pl.when(cond)(ag(w, u, h, side, k - 1, True).wait_recv)
            go(ag(w, u, h, side, k), cond)

    def ag_finish(w, u, h):
        for k in range(nz - 1):
            pl.when(jnp.logical_and(z == nz - 1, z >= k + 1))(
                ag(w, u, h, RIGHT, k, True).wait_recv)
            pl.when(jnp.logical_and(z == 0, z <= nz - 2 - k))(
                ag(w, u, h, LEFT, k, True).wait_recv)

    def weight_y(w, receive=False):
        ff = z * ny + (yo if receive else y)
        return remote(weight_own(w, yo), weight_view(w, ff), wy_s.at[w], wy_r.at[w], y_dev)

    class Rows:
        def __init__(self, a, src, buf, pieces):
            self.a, self.buf = a, buf
            self.pieces, self.width, self.source = pieces, m.d // pieces, src

        def drain(self):
            count = 4 * nx - 1
            every = self.buf.at[pl.ds(0, count * m.t), :]
            remote(every, every, tok_s.at[self.a], tok_r.at[nz, 0], y_dev).wait_send()

        def cols(self, p):
            return pl.ds(aligned(p * self.width, self.width), self.width)

        def src(self, p):
            return self.source.at[:, self.cols(p)]

        def place(self, p, yy, xx, cc):
            start = aligned(((yy * nx + xx) * 2 + cc) * m.t, m.t)
            return self.buf.at[pl.ds(start, m.t), self.cols(p)]

        def copy(self, p, index, src, where, dev):
            row = p if self.a == 0 else nz
            return remote(src, self.place(p, *where), tok_s.at[self.a],
                          tok_r.at[row, index], dev)

        def over_y(self, p, receive=False):
            return self.copy(p, 0, self.src(p), (yo if receive else y, x, c), y_dev)

        def over_x(self, p, j, k, receive=False):
            yy = y if j == 0 else yo
            xx = x_at(nx - k) if receive else x
            src = self.src(p) if j == 0 else self.place(p, yy, x, c)
            index = 1 + j * (nx - 1) + k - 1
            return self.copy(p, index, src, (yy, xx, c), at(z, y, x_at(k), c))

        def over_c(self, p, j, k):
            yy = y if j == 0 else yo
            xx = x_at(nx - k) if k else x
            src = self.src(p) if j == 0 and k == 0 else self.place(p, yy, xx, c)
            return self.copy(p, 2 * nx - 1, src, (yy, xx, c), c_dev)

        def start_y(self, p):
            self.over_y(p).start()

        def start_x(self, p):
            for k in range(1, nx):
                self.over_x(p, 0, k).start()
            self.over_c(p, 0, 0).start()

        def relay_y(self, p):
            self.over_y(p, True).wait_recv()
            for k in range(1, nx):
                self.over_x(p, 1, k).start()
            self.over_c(p, 1, 0).start()

        def relay_x(self, p, j):
            for k in range(1, nx):
                self.over_x(p, j, k, True).wait_recv()
                self.over_c(p, j, k).start()

        def finish(self, p):
            row = p if self.a == 0 else nz
            half = self.buf.at[pl.ds(0, 2 * nx * m.t), self.cols(p)]
            remote(half, half, tok_s.at[self.a], tok_r.at[row, 2 * nx - 1], c_dev).wait_recv()

    og_rows = Rows(0, og, og_all, nz)
    in_rows = Rows(1, inp, in_all, 1)

    def act_copy(part, receive=False):
        col = part * m.ha
        src = act.at[:, pl.ds(aligned(yo * m.hh + col, m.ha), m.ha)]
        row = aligned((yo if receive else y) * m.rows, m.rows)
        dst = acts.at[pl.ds(row, m.rows), pl.ds(col, m.ha)]
        return remote(src, dst, act_s, act_r.at[part], y_dev)

    local = [
        pltpu.make_async_copy(weight_own(DN, y), weight_view(DN, f), loc.at[0]),
        pltpu.make_async_copy(weight_own(UP, y), weight_view(UP, f), loc.at[1]),
        pltpu.make_async_copy(og, slot(og_all, y, x, c), loc.at[2]),
        pltpu.make_async_copy(inp, slot(in_all, y, x, c), loc.at[3]),
        pltpu.make_async_copy(
            act.at[:, pl.ds(aligned(y * m.hh, m.hh), m.hh)],
            acts.at[pl.ds(aligned(y * m.rows, m.rows), m.rows), :], loc.at[4]),
    ]

    parts, slots = (part_dn, part_up), (slot_dn, slot_up)

    def half_of(ref, half):
        if half is None:
            return ref
        yy = yo if half == 0 else y
        return ref.at[pl.ds(aligned(yy * m.df, m.df), m.df), :]

    def rs_sem(w, place, ch, half):
        return rs_r.at[w, place, ch] if half != 1 else rs_h.at[place, ch]

    def rs(w, side, target, ch, own, half=None):
        src = (parts if own else slots)[w].at[target, ch]
        if side == RIGHT:
            place = target
        else:
            place = jnp.where(target == z - 1, nz, target)
        return remote(half_of(src, half), half_of(slots[w].at[place, ch], half),
                      rs_s.at[w, target], rs_sem(w, place, ch, half), z_dev[side])

    def rs_waits(w, side, ch, place, half=None):
        return remote(half_of(parts[w].at[0, ch], half), half_of(slots[w].at[place, ch], half),
                      rs_s.at[w, 0], rs_sem(w, place, ch, half), z_dev[side])

    def by_rows(count, step, body):
        @pl.loop(0, count // step)
        def _(i):
            body(pl.ds(aligned(i * step, step), step))

    def rs_edge(w, target, ch, half=None):
        @pl.when(jnp.logical_and(z == 0, target > 0))
        def _():
            rs(w, RIGHT, target, ch, True, half).start()

        @pl.when(jnp.logical_and(z == nz - 1, target < nz - 1))
        def _():
            rs(w, LEFT, target, ch, True, half).start()

    def rs_pass(w, side, step, ch, half=None):
        target = nz - 1 - step if side == RIGHT else step
        if side == RIGHT:
            cond = jnp.logical_and(z > 0, z < target)
        else:
            cond = jnp.logical_and(z < nz - 1, z > target)

        @pl.when(cond)
        def _():
            rs_waits(w, side, ch, target, half).wait_recv()
            buf = half_of(slots[w].at[target, ch], half)
            own = half_of(parts[w].at[target, ch], half)

            def add(rows):
                buf[rows, :] = (buf[rows, :].astype(F32)
                                + own[rows, :].astype(F32)).astype(BF16)
            by_rows(buf.shape[0], 64, add)
            rs(w, side, target, ch, False, half).start()

    def passes(w, sides, chunks, first, last, half):
        for low_side in (True, False):
            @pl.when(z < nz // 2 if low_side else z >= nz // 2)
            def _():
                for step in range(first, last):
                    for ch in chunks:
                        rs_pass(w, sides[0] if low_side else sides[1], step, ch, half)

    def near(w, ch, first=0, last=nz - 2):
        passes(w, (RIGHT, LEFT), [ch], first, last, None)

    def far(w, ch):
        passes(w, (LEFT, RIGHT), [ch], 0, nz - 2, None)

    tail = (CHUNKS - 2, CHUNKS - 1)

    def near_tail(first, last, half):
        passes(UP, (RIGHT, LEFT), tail, first, last, half)

    def far_tail(half):
        passes(UP, (LEFT, RIGHT), tail, 0, nz - 2, half)

    def rs_drain(w):
        for target in range(nz):
            every = slots[w].at[target]
            pl.when(z != target)(
                remote(every, every, rs_s.at[w, target], rs_r.at[w, 0, 0], y_dev).wait_send)

    def fin_cut(w, buf, yy):
        cut = pl.ds(aligned(yy * m.df, m.df), m.df)
        return buf.at[:, cut] if w == DN else buf.at[cut, :]

    def fin_place(w, ch, yy):
        start = aligned(yy * m.hh + ch * m.hc, m.hc)
        if w == DN:
            return dg_out.at[pl.ds(start, m.hc), :]
        return ug_out.at[:, pl.ds(start, m.hc)]

    def fin_remote(w, ch):
        return remote(fin_cut(w, parts[w].at[z, ch], yo), fin_place(w, ch, y),
                      fin_s.at[w], fin_r.at[w], y_dev)

    def rs_finish(w, ch, half=None):
        own = parts[w].at[z, ch]
        right, left = slots[w].at[z, ch], slots[w].at[nz, ch]
        pl.when(z > 0)(rs_waits(w, RIGHT, ch, z, half).wait_recv)
        pl.when(z < nz - 1)(rs_waits(w, LEFT, ch, nz, half).wait_recv)

        def total(yy, dst, others):
            terms = [fin_cut(w, buf, yy) for buf in others]

            def add(rows):
                value = terms[0][rows, :].astype(F32)
                for term in terms[1:]:
                    value = value + term[rows, :].astype(F32)
                dst[rows, :] = value.astype(BF16)
            by_rows(terms[0].shape[0], 64, add)

        def both(yy, dst):
            pl.when(z == 0)(lambda: total(yy, dst, (own, left)))
            pl.when(z == nz - 1)(lambda: total(yy, dst, (own, right)))
            pl.when(jnp.logical_and(z > 0, z < nz - 1))(
                lambda: total(yy, dst, (own, right, left)))

        if half != 1:
            both(yo, fin_cut(w, own, yo))
            fin_remote(w, ch).start()
        if half != 0:
            both(y, fin_place(w, ch, y))

    def finish_tail(half):
        for ch in tail:
            rs_finish(UP, ch, half)

    def fin_wait(w):
        def half(yy):
            cut = pl.ds(aligned(yy * m.hh, m.hh), m.hh)
            return dg_out.at[cut, :] if w == DN else ug_out.at[:, cut]

        mine, other = half(y), half(yo)
        remote(mine, mine, fin_s.at[w], fin_r.at[w], y_dev).wait_send()
        remote(other, other, fin_s.at[w], fin_r.at[w], y_dev).wait_recv()

    def targets(i):
        turn = i // 2
        return mirror(jnp.where(i % 2 == 0, nz - 1 - turn, turn))

    def squares(ch):
        cols = pl.ds(ch * m.hc, m.hc)

        def body(rows):
            active = jnp.maximum(acts[rows, cols].astype(F32), 0.0)
            hid[rows, cols] = (active * active).astype(BF16)
        by_rows(m.all_rows, 64, body)

    def dot_rows(a, b):
        return lax.dot_general(a, b, (((0,), (0,)), ((), ())), preferred_element_type=F32)

    def dot_cols(a, b):
        return lax.dot_general(a, b, (((1,), (1,)), ((), ())), preferred_element_type=F32)

    def dot_dn(ch, first=0, last=nz):
        @pl.loop(first, last)
        def _(i):
            target = targets(i)
            a = hid[:, pl.ds(ch * m.hc, m.hc)]
            b = og_all[:, pl.ds(aligned(target * m.dz, m.dz), m.dz)]
            part_dn[target, ch] = dot_rows(a, b).astype(BF16)
            rs_edge(DN, target, ch)

    def dot_hg(ch):
        cols = pl.ds(ch * m.hc, m.hc)

        @pl.loop(0, m.all_rows // 512)
        def _(i):
            rows = pl.ds(aligned(i * 512, 512), 512)
            active = jnp.maximum(acts[rows, cols].astype(F32), 0.0)
            grad = dot_cols(og_all[rows, :], dn_all[cols, :])
            pre[rows, cols] = (2.0 * active * grad).astype(BF16)

    def dot_up(ch, send=True):
        @pl.loop(0, nz)
        def _(i):
            target = targets(i)
            a = in_all[:, pl.ds(aligned(target * m.dz, m.dz), m.dz)]
            b = pre[:, pl.ds(ch * m.hc, m.hc)]
            part_up[target, ch] = dot_rows(a, b).astype(BF16)
            if send:
                rs_edge(UP, target, ch)

    def up_sends():
        @pl.loop(0, nz)
        def _(i):
            for half in range(2):
                for ch in tail:
                    rs_edge(UP, targets(i), ch, half)

    part = og_all
    width = m.d // 2
    sets = [pl.ds(0, width), pl.ds(width, width)]

    def ig_c(g, j):
        yy, xx = j // nx, j % nx
        return remote(slot(part, yy, xx, co).at[:, sets[g]], crecv.at[yy, xx, :, sets[g]],
                      igc_s.at[g], igc_r.at[g], c_dev)

    def dot_in(g, remote_half):
        piece = m.df // 2
        group = 4
        tile = piece * group
        cc = co if remote_half else c
        count = m.fs // group

        @pl.loop(0, ny * count)
        def _(i):
            yy, n = i // count, i % count
            cols = pl.ds(aligned(g * width + n * tile, tile), tile)
            blocks = [pl.ds(aligned(((yy * nx + xx) * 2 + cc) * m.t, m.t), m.t)
                      for xx in range(nx)]
            rows_of = [pl.ds(aligned((n * group + q) * m.df + g * piece, piece), piece)
                       for q in range(group)]
            a = jnp.concatenate([pre[rows, :] for rows in blocks], 0)
            b = jnp.concatenate([up_all[rows, :] for rows in rows_of], 0)
            value = dot_cols(a, b).astype(BF16)
            for xx, rows in enumerate(blocks):
                part[rows, cols] = value[xx * m.t:(xx + 1) * m.t]
            if remote_half:
                @pl.when(n == count - 1)
                def _():
                    for xx in range(nx):
                        ig_c(g, yy * nx + xx).start()

    def ig_all(g):
        every = crecv.at[:, :, :, sets[g]]
        return remote(every, every, igc_s.at[g], igc_r.at[g], c_dev)

    def ig_sum(g):
        ig_all(g).wait_recv()

        @pl.loop(0, ny * nx)
        def _(j):
            buf = crecv.at[j // nx, j % nx, :, sets[g]]
            own = slot(part, j // nx, j % nx, c).at[:, sets[g]]

            def add(rows):
                buf[rows, :] = (buf[rows, :].astype(F32) + own[rows, :].astype(F32)).astype(BF16)
            by_rows(m.t, 32, add)

    low, high = pl.ds(0, m.half), pl.ds(m.half, m.half)

    def accumulate(dst, others):
        def add(rows):
            value = dst[rows, :].astype(F32)
            for other in others:
                value = value + other[rows, :].astype(F32)
            dst[rows, :] = value.astype(BF16)
        by_rows(m.half, 32, add)

    def ig_x1(g, k):
        return remote(crecv.at[:, x_at(k), low, sets[g]], xr1.at[k - 1, :, :, sets[g]],
                      igx_s.at[g, k - 1], igx_r.at[g, k - 1], at(z, y, x_at(k), c))

    def ig_y1(g):
        return remote(crecv.at[yo, x, low, sets[g]], yr1.at[:, sets[g]],
                      igx_s.at[g, nx - 1], igx_r.at[g, nx - 1], y_dev)

    def ig_y2(g):
        return remote(crecv.at[yo, :, high, sets[g]], yr2.at[:, :, sets[g]],
                      igx_s.at[g, nx], igx_r.at[g, nx], y_dev)

    def ig_x2(g, k):
        return remote(crecv.at[y, x_at(k), high, sets[g]], xr2.at[k - 1, :, sets[g]],
                      igx_s.at[g, nx + k], igx_r.at[g, nx + k], at(z, y, x_at(k), c))

    def ig_first(g):
        for k in range(1, nx):
            go(ig_x1(g, k))
        go(ig_y2(g))

    def ig_second(g):
        for k in range(1, nx):
            ig_x1(g, k).wait_recv()
        for yy in range(ny):
            accumulate(crecv.at[yy, x, low, sets[g]],
                       [xr1.at[k, yy, :, sets[g]] for k in range(nx - 1)])
        go(ig_y1(g))
        ig_y2(g).wait_recv()
        for xx in range(nx):
            accumulate(crecv.at[y, xx, high, sets[g]], [yr2.at[xx, :, sets[g]]])
        for k in range(1, nx):
            go(ig_x2(g, k))

    piece = m.df // 2

    def ig_store(rows, g, value):
        value = value.astype(BF16)
        if not m.direct:
            ig_out[rows, sets[g]] = value
            return
        for n in range(m.fs):
            ig_out[rows, pl.ds(n * m.df + g * piece, piece)] = value[:, n * piece:(n + 1) * piece]

    def ig_final(first, g, terms):
        def add(rows):
            value = terms[0][rows, :].astype(F32)
            for term in terms[1:]:
                value = value + term[rows, :].astype(F32)
            ig_store(pl.ds(aligned(first + rows.start, 32), rows.size), g, value)
        by_rows(m.half, 32, add)

    def ig_last(g):
        ig_y1(g).wait_recv()
        ig_final(0, g, [crecv.at[y, x, low, sets[g]], yr1.at[:, sets[g]]])
        for k in range(1, nx):
            ig_x2(g, k).wait_recv()
        ig_final(m.half, g, [crecv.at[y, x, high, sets[g]]]
                 + [xr2.at[k, :, sets[g]] for k in range(nx - 1)])

    def acts_in(index):
        act_copy(index, True).wait_recv()

    def start():
        ag_step(DN, 0, 0, 0)
        for p in order[:2]:
            og_rows.start_y(p)
            og_rows.start_x(p)
        act_copy(0).start()
        go(weight_y(DN))
        for p in order[2:]:
            og_rows.start_y(p)
        act_copy(1).start()
        go(weight_y(UP))
        act_copy(2).start()
        in_rows.start_y(0)
        act_copy(3).start()
        ag_step(UP, 0, 0, 0)
        ag_step(UP, 0, 1, 0)
        for copy in local:
            copy.start()

    def first_rows():
        for p in order[:2]:
            og_rows.relay_y(p)
            og_rows.relay_x(p, 0)
        for p in order[2:]:
            og_rows.start_x(p)

    def first_rows_in():
        for p in order[:2]:
            og_rows.relay_x(p, 1)
        for p in order[:2]:
            og_rows.finish(p)

    def more_rows(p):
        og_rows.relay_y(p)
        og_rows.relay_x(p, 0)

    def more_rows_in(p):
        og_rows.relay_x(p, 1)
        og_rows.finish(p)

    def local_wait():
        for copy in local:
            copy.wait()

    def weight_in(w):
        weight_y(w, True).wait_recv()

    def act_drain():
        every = acts.at[pl.ds(0, m.rows), :]
        remote(every, every, act_s, act_r.at[0], y_dev).wait_send()

    def ig_drain():
        for g in range(2):
            ig_all(g).wait_send()

    def gather_on(w, u, h):
        near_steps = [(ag_step, w, u, h, k, "near") for k in range(2, nz // 2)]
        return near_steps + [(ag_step, w, u, h, k, "far") for k in range(2, nz - 1)]

    plan = [
        (start,),
        (first_rows,),
        (ag_step, DN, 0, 0, 1),
        (first_rows_in,),
        (local_wait,),
        (acts_in, 0),
        (squares, 0),
        (dot_dn, 0, 0, 2),
        *gather_on(DN, 0, 0),
        (weight_in, DN),
        (ag_step, DN, 1, 0, 0),
        (near, DN, 0, 0, 1),
        *[(more_rows, p) for p in order[2:]],
        (in_rows.start_x, 0),
        *[call for i, p in enumerate(order[2:])
          for call in ((more_rows_in, p), (dot_dn, 0, i + 2, i + 3))],
        (ag_step, DN, 1, 0, 1),
        (acts_in, 1),
        (squares, 1),
        (dot_dn, 1),
        (near, DN, 0, 1, nz - 2),
        *gather_on(DN, 1, 0),
        (weight_in, UP),
        (ag_step, UP, 1, 0, 0, "edge"),
        (ag_step, UP, 1, 1, 0, "edge"),
        (ag_step, UP, 1, 0, 0, "inner"),
        (ag_step, UP, 0, 0, 1, "near"),
        (acts_in, 2),
        (squares, 2),
        (dot_dn, 2),
        (near, DN, 1),
        (ag_step, UP, 0, 0, 1, "far"),
        (ag_step, UP, 1, 0, 1, "near"),
        (ag_finish, DN, 0, 0),
        (ag_finish, DN, 1, 0),
        (dot_hg, 0),
        (dot_hg, 1),
        (dot_hg, 2),
        (ag_step, UP, 1, 0, 1, "far"),
        (ag_step, UP, 1, 1, 0, "inner"),
        (ag_step, UP, 0, 1, 1, "near"),
        (ag_step, UP, 1, 1, 1, "near"),
        (in_rows.relay_y, 0),
        (in_rows.relay_x, 0, 0),
        *gather_on(UP, 0, 0),
        *gather_on(UP, 1, 0),
        (acts_in, 3),
        (squares, 3),
        (dot_dn, 3),
        (dot_hg, 3),
        (near, DN, 2),
        (in_rows.relay_x, 0, 1),
        (in_rows.finish, 0),
        (dot_up, 0),
        (ag_step, UP, 0, 1, 1, "far"),
        (dot_up, 1),
        (near, DN, 3),
        (ag_step, UP, 1, 1, 1, "far"),
        (ag_finish, UP, 0, 0),
        (ag_finish, UP, 1, 0),
        (og_rows.drain,),
        (dot_in, 0, True),
        *gather_on(UP, 0, 1),
        (dot_in, 0, False),
        (dot_up, 2, False),
        *gather_on(UP, 1, 1),
        (ig_sum, 0),
        (ig_first, 0),
        (dot_up, 3, False),
        (up_sends,),
        (far, DN, 0),
        (far, DN, 1),
        (near, UP, 0),
        (ig_second, 0),
        (ag_finish, UP, 0, 1),
        (ag_finish, UP, 1, 1),
        (dot_in, 1, True),
        (dot_in, 1, False),
        (far, DN, 2),
        (far, DN, 3),
        (ig_sum, 1),
        (ig_first, 1),
        (far, UP, 0),
        (near, UP, 1),
        (ig_last, 0),
        (rs_finish, DN, 0),
        (rs_finish, DN, 1),
        (far, UP, 1),
        (ig_second, 1),
        (rs_finish, DN, 2),
        (rs_finish, DN, 3),
        (near_tail, 0, 1, 0),
        (ig_last, 1),
        (near_tail, 0, 1, 1),
        (rs_finish, UP, 0),
        (near_tail, 1, nz - 2, 0),
        (far_tail, 0),
        (rs_finish, UP, 1),
        (near_tail, 1, nz - 2, 1),
        (far_tail, 1),
        (finish_tail, 0),
        (finish_tail, 1),
        (in_rows.drain,),
        (drain, sends),
        (act_drain,),
        (ig_drain,),
        (rs_drain, DN),
        (rs_drain, UP),
        (fin_wait, DN),
        (fin_wait, UP),
    ]
    for index, (function, *args) in enumerate(plan):
        tags = [str(arg) for arg in args if isinstance(arg, (int, str))]
        label = "_".join([str(index), function.__name__, *tags])
        with jax.named_scope(label):
            function(*args)


def local_step(fs, tp, inp, act, og, upw, dnw):
    m = Dims(fs, tp, og.shape[0], og.shape[1], act.shape[1])
    dma = pltpu.SemaphoreType.DMA
    vm = pltpu.VMEM
    any_space = pl.BlockSpec(memory_space=pl.ANY)
    flops = 8 * m.all_rows * m.hh * m.d
    ig, ug, dg = pl.pallas_call(
        functools.partial(kernel, m),
        name="ffn_backward",
        out_shape=(
            vm((m.t, m.d), BF16),
            vm((m.df, m.h), BF16),
            vm((m.h, m.df), BF16),
        ),
        in_specs=[any_space] * 5,
        out_specs=(pl.BlockSpec(memory_space=pltpu.VMEM),) * 3,
        scratch_shapes=[
            vm((m.all_rows, m.d), BF16),
            vm((m.all_rows, m.d), BF16),
            vm((m.all_rows, m.hh), BF16),
            vm((m.all_rows, m.hh), BF16),
            vm((m.all_rows, m.hh), BF16),
            vm((m.hh, m.d), BF16),
            vm((m.d, m.hh), BF16),
            vm((m.nz, CHUNKS, m.hc, m.dz), BF16),
            vm((m.nz, CHUNKS, m.dz, m.hc), BF16),
            vm((m.nz + 1, CHUNKS, m.hc, m.dz), BF16),
            vm((m.nz + 1, CHUNKS, m.dz, m.hc), BF16),
            vm((m.ny, m.nx, m.t, m.d), BF16),
            vm((m.nx - 1, m.ny, m.half, m.d), BF16),
            vm((m.half, m.d), BF16),
            vm((m.nx, m.half, m.d), BF16),
            vm((m.nx - 1, m.half, m.d), BF16),
            dma((5,)),
            dma((3 * m.ny, 2, m.nz - 1)),
            dma((3 * m.ny, m.nz)),
            dma((2,)),
            dma((2,)),
            dma((2,)),
            dma((m.nz + 1, 2 * m.nx)),
            dma,
            dma((ACT_PARTS,)),
            dma((2, m.nz)),
            dma((2, m.nz + 1, CHUNKS)),
            dma((m.nz + 1, CHUNKS)),
            dma((2,)),
            dma((2,)),
            dma((2,)),
            dma((2,)),
            dma((2, 2 * m.nx)),
            dma((2, 2 * m.nx)),
        ],
        cost_estimate=pl.CostEstimate(flops=flops, bytes_accessed=2**25, transcendentals=0),
        compiler_params=pltpu.CompilerParams(
            collective_id=0, has_side_effects=True, vmem_limit_bytes=62914560
        ),
    )(inp, act, og, upw, dnw)
    if not m.direct:
        ig = ig.reshape(m.t, 2, m.fs, m.df // 2).transpose(0, 2, 1, 3)
        ig = ig.reshape(m.t, m.d)
    return widen(ig, ug, dg)


def widen(ig, ug, dg):
    steps = 2

    def body(ig_in, ug_in, dg_in, ig_out, ug_out, dg_out, wide_ug, wide_dg, sems):
        copies = [pltpu.make_async_copy(ig_in, ig_out, sems.at[0])]
        copies[0].start()
        pairs = ((ug_in, wide_ug, ug_out), (dg_in, wide_dg, dg_out))
        for which, (src, wide, out) in enumerate(pairs):
            count = src.shape[0] // steps
            for i in range(steps):
                first = i * count
                rows = pl.ds(first, count)

                @pl.loop(0, count // 32)
                def _(j):
                    part = pl.ds(aligned(first + j * 32, 32), 32)
                    wide[part, :] = src[part, :].astype(F32)

                copies.append(pltpu.make_async_copy(
                    wide.at[rows, :], out.at[rows, :], sems.at[1 + which * steps + i]))
                copies[-1].start()
        for copy in copies:
            copy.wait()

    vmem = pl.BlockSpec(memory_space=pltpu.VMEM)
    outside = pl.BlockSpec(memory_space=pl.ANY)
    return pl.pallas_call(
        body,
        name="widen",
        out_shape=(
            jax.ShapeDtypeStruct(ig.shape, BF16),
            jax.ShapeDtypeStruct(ug.shape, F32),
            jax.ShapeDtypeStruct(dg.shape, F32),
        ),
        in_specs=[vmem] * 3,
        out_specs=(outside,) * 3,
        scratch_shapes=[
            pltpu.VMEM(ug.shape, F32),
            pltpu.VMEM(dg.shape, F32),
            pltpu.SemaphoreType.DMA((1 + 2 * steps,)),
        ],
        cost_estimate=pl.CostEstimate(flops=ug.size, bytes_accessed=16 * ug.size, transcendentals=0),
        compiler_params=pltpu.CompilerParams(vmem_limit_bytes=16 * ug.size),
    )(*(pltpu.with_memory_space_constraint(v, pltpu.VMEM) for v in (ig, ug, dg)))


def solution(mesh):
    placed = (
        P(("fs", "tp"), None),
        P("fs", "tp"),
        P(("fs", "tp"), None),
        P("fs", "tp"),
        P("tp", "fs"),
    )
    return jax.shard_map(
        functools.partial(local_step, mesh.shape["fs"], mesh.shape["tp"]),
        mesh=mesh,
        in_specs=placed,
        out_specs=(P(("fs", "tp"), None), P("fs", "tp"), P("tp", "fs")),
        check_vma=False,
    )
```

```python
import functools

import jax
import jax.numpy as jnp
from jax import lax
from jax.experimental import pallas as pl
from jax.experimental.pallas import tpu as pltpu
from jax.sharding import PartitionSpec as P

MESH = pl.DeviceIdType.MESH
BF16, F32 = jnp.bfloat16, jnp.float32
CHUNKS = 4
ACT_PARTS = 4
DN, UP = 0, 1
RIGHT, LEFT = 0, 1


def aligned(value, unit):
    return pl.multiple_of(value, unit)


class Dims:
    def __init__(self, fs, tp, tokens, d, hidden):
        self.fs, self.tp = fs, tp
        self.ny, self.nc = 2, 2
        self.nz, self.nx = fs // 2, tp // 2
        self.t, self.d, self.h = tokens, d, hidden
        self.rows = tokens * tp
        self.all_rows = self.rows * self.ny
        self.hh = hidden // self.ny
        self.df = d // fs
        self.dz = self.df * self.ny
        self.half = tokens // 2
        self.hc = self.hh // CHUNKS
        self.ha = self.hh // ACT_PARTS
        self.direct = (self.df // 2) % 128 == 0


def kernel(
    m, inp, act, og, upw, dnw, ig_out, ug_out, dg_out,
    og_all, in_all, acts, hid, pre, dn_all, up_all,
    part_dn, part_up, slot_dn, slot_up, crecv, xr1, yr1, yr2, xr2,
    loc, ag_s, ag_r, wy_s, wy_r, tok_s, tok_r, act_s, act_r,
    rs_s, rs_r, rs_h, fin_s, fin_r, igc_s, igc_r, igx_s, igx_r,
):
    f, tt = lax.axis_index("fs"), lax.axis_index("tp")
    ny, nx, nz = m.ny, m.nx, m.nz
    z, y = f // ny, f % ny
    x, c = tt // 2, tt % 2
    yo, co = 1 - y, 1 - c
    sends = []

    def at(zz, yy, xx, cc):
        return (zz * ny + yy, xx * 2 + cc)

    y_dev, c_dev = at(z, yo, x, c), at(z, y, x, co)
    z_dev = (at(z + 1, y, x, c), at(z - 1, y, x, c))
    has_z = (z < nz - 1, z > 0)

    def x_at(k):
        return lax.rem(x + k, nx)

    def mirror(target):
        return jnp.where(z < nz // 2, target, nz - 1 - target)

    order = [mirror(nz - 1 - i) for i in range(nz)]

    def remote(src, dst, ss, rs, dev):
        return pltpu.make_async_remote_copy(
            src_ref=src, dst_ref=dst, send_sem=ss, recv_sem=rs,
            device_id=dev, device_id_type=MESH,
        )

    def go(copy, cond=None, group=sends):
        if cond is None:
            copy.start()
        else:
            pl.when(cond)(copy.start)
        group.append((cond, copy))

    def drain(group):
        for cond, copy in group:
            if cond is None:
                copy.wait_send()
            else:
                pl.when(cond)(copy.wait_send)
        group.clear()

    barrier = pltpu.get_barrier_semaphore()
    peers = [(None, y_dev), (None, c_dev)]
    peers += [(None, at(z, y, x_at(k), c)) for k in range(1, nx)]
    peers += [(has_z[RIGHT], z_dev[RIGHT]), (has_z[LEFT], z_dev[LEFT])]
    for cond, dev in peers:
        def hello(dev=dev):
            pl.semaphore_signal(barrier, inc=1, device_id=dev, device_id_type=MESH)
        hello() if cond is None else pl.when(cond)(hello)
    lines = jnp.where(z > 0, 1, 0) + jnp.where(z < nz - 1, 1, 0)
    pl.semaphore_wait(barrier, 1 + nx + lines)

    def slot(buf, yy, xx, cc):
        start = aligned(((yy * nx + xx) * 2 + cc) * m.t, m.t)
        return buf.at[pl.ds(start, m.t), :]

    parts_of = (1, 2)

    def weight_view(w, ff, h=None):
        start, size = ff * m.df, m.df
        if w == DN:
            return dn_all.at[:, pl.ds(aligned(start, m.df), m.df)]
        if h is not None:
            size = m.df // parts_of[w]
            start = start + h * size
        return up_all.at[pl.ds(aligned(start, size), size), :]

    def weight_own(w, yy, h=None):
        start = aligned(yy * m.hh, m.hh)
        if w == DN:
            return dnw.at[pl.ds(start, m.hh), :]
        first, size = 0, m.df
        if h is not None:
            size = m.df // parts_of[w]
            first = h * size
        return upw.at[pl.ds(first, size), pl.ds(start, m.hh)]

    def ag(w, u, h, side, k, receive=False):
        back = k + 1 if receive else k
        origin = jnp.clip(z - back if side == RIGHT else z + back, 0, nz - 1)
        view = weight_view(w, origin * ny + (y if u == 0 else yo), h)
        src = weight_own(w, y, h) if (u == 0 and k == 0) else view
        unit = u if w == DN else ny + 2 * u + h
        return remote(src, view, ag_s.at[side, k], ag_r.at[unit, origin], z_dev[side])

    def ag_sends(side, k):
        if side == RIGHT:
            return jnp.logical_and(z >= k, z < nz - 1)
        return jnp.logical_and(z <= nz - 1 - k, z > 0)

    def ag_step(w, u, h, k, where="all"):
        outer = (z == 0, z == nz - 1)
        inner = jnp.logical_and(z > 0, z < nz - 1)
        close = (z < nz // 2, z >= nz // 2)
        for side in (RIGHT, LEFT):
            cond = ag_sends(side, k)
            if where == "edge":
                cond = outer[side]
            if where == "inner":
                cond = inner
            if where == "near":
                cond = jnp.logical_and(cond, close[side])
            if where == "far":
                cond = jnp.logical_and(cond, close[1 - side])
            if k > 0:
                pl.when(cond)(ag(w, u, h, side, k - 1, True).wait_recv)
            pl.when(cond)(ag(w, u, h, side, k).start)

    def ag_drain():
        every = up_all.at[pl.ds(0, 4 * m.df), :]
        for side in (RIGHT, LEFT):
            for k in range(nz - 1):
                pl.when(ag_sends(side, k))(
                    remote(every, every, ag_s.at[side, k], ag_r.at[0, 0], y_dev).wait_send)

    def ag_finish(w, u, h):
        for k in range(nz - 1):
            pl.when(jnp.logical_and(z == nz - 1, z >= k + 1))(
                ag(w, u, h, RIGHT, k, True).wait_recv)
            pl.when(jnp.logical_and(z == 0, z <= nz - 2 - k))(
                ag(w, u, h, LEFT, k, True).wait_recv)

    def weight_y(w, receive=False):
        ff = z * ny + (yo if receive else y)
        return remote(weight_own(w, yo), weight_view(w, ff), wy_s.at[w], wy_r.at[w], y_dev)

    class Rows:
        def __init__(self, a, src, buf, pieces):
            self.a, self.buf = a, buf
            self.pieces, self.width, self.source = pieces, m.d // pieces, src

        def drain(self):
            count = 4 * nx - 1
            every = self.buf.at[pl.ds(0, count * m.t), :]
            remote(every, every, tok_s.at[self.a], tok_r.at[nz, 0], y_dev).wait_send()

        def cols(self, p):
            return pl.ds(aligned(p * self.width, self.width), self.width)

        def src(self, p):
            return self.source.at[:, self.cols(p)]

        def place(self, p, yy, xx, cc):
            start = aligned(((yy * nx + xx) * 2 + cc) * m.t, m.t)
            return self.buf.at[pl.ds(start, m.t), self.cols(p)]

        def copy(self, p, index, src, where, dev):
            row = p if self.a == 0 else nz
            return remote(src, self.place(p, *where), tok_s.at[self.a],
                          tok_r.at[row, index], dev)

        def over_y(self, p, receive=False):
            return self.copy(p, 0, self.src(p), (yo if receive else y, x, c), y_dev)

        def over_x(self, p, j, k, receive=False):
            yy = y if j == 0 else yo
            xx = x_at(nx - k) if receive else x
            src = self.src(p) if j == 0 else self.place(p, yy, x, c)
            index = 1 + j * (nx - 1) + k - 1
            return self.copy(p, index, src, (yy, xx, c), at(z, y, x_at(k), c))

        def over_c(self, p, j, k):
            yy = y if j == 0 else yo
            xx = x_at(nx - k) if k else x
            src = self.src(p) if j == 0 and k == 0 else self.place(p, yy, xx, c)
            return self.copy(p, 2 * nx - 1, src, (yy, xx, c), c_dev)

        def start_y(self, p):
            self.over_y(p).start()

        def start_x(self, p):
            for k in range(1, nx):
                self.over_x(p, 0, k).start()
            self.over_c(p, 0, 0).start()

        def relay_y(self, p):
            self.over_y(p, True).wait_recv()
            for k in range(1, nx):
                self.over_x(p, 1, k).start()
            self.over_c(p, 1, 0).start()

        def relay_x(self, p, j):
            for k in range(1, nx):
                self.over_x(p, j, k, True).wait_recv()
                self.over_c(p, j, k).start()

        def finish(self, p):
            row = p if self.a == 0 else nz
            half = self.buf.at[pl.ds(0, 2 * nx * m.t), self.cols(p)]
            remote(half, half, tok_s.at[self.a], tok_r.at[row, 2 * nx - 1], c_dev).wait_recv()

    og_rows = Rows(0, og, og_all, nz)
    in_rows = Rows(1, inp, in_all, 1)

    def act_copy(part, receive=False):
        col = part * m.ha
        src = act.at[:, pl.ds(aligned(yo * m.hh + col, m.ha), m.ha)]
        row = aligned((yo if receive else y) * m.rows, m.rows)
        dst = acts.at[pl.ds(row, m.rows), pl.ds(col, m.ha)]
        return remote(src, dst, act_s, act_r.at[part], y_dev)

    local = [
        pltpu.make_async_copy(weight_own(DN, y), weight_view(DN, f), loc.at[0]),
        pltpu.make_async_copy(weight_own(UP, y), weight_view(UP, f), loc.at[1]),
        pltpu.make_async_copy(og, slot(og_all, y, x, c), loc.at[2]),
        pltpu.make_async_copy(inp, slot(in_all, y, x, c), loc.at[3]),
        pltpu.make_async_copy(
            act.at[:, pl.ds(aligned(y * m.hh, m.hh), m.hh)],
            acts.at[pl.ds(aligned(y * m.rows, m.rows), m.rows), :], loc.at[4]),
    ]

    parts, slots = (part_dn, part_up), (slot_dn, slot_up)

    def half_of(ref, half):
        if half is None:
            return ref
        yy = yo if half == 0 else y
        return ref.at[pl.ds(aligned(yy * m.df, m.df), m.df), :]

    def rs_sem(w, place, ch, half):
        return rs_r.at[w, place, ch] if half != 1 else rs_h.at[place, ch - tail[0]]

    def rs(w, side, target, ch, own, half=None):
        src = (parts if own else slots)[w].at[target, ch]
        if side == RIGHT:
            place = target
        else:
            place = jnp.where(target == z - 1, nz, target)
        return remote(half_of(src, half), half_of(slots[w].at[place, ch], half),
                      rs_s.at[w, target], rs_sem(w, place, ch, half), z_dev[side])

    def rs_waits(w, side, ch, place, half=None):
        return remote(half_of(parts[w].at[0, ch], half), half_of(slots[w].at[place, ch], half),
                      rs_s.at[w, 0], rs_sem(w, place, ch, half), z_dev[side])

    def by_rows(count, step, body):
        @pl.loop(0, count // step)
        def _(i):
            body(pl.ds(aligned(i * step, step), step))

    def rs_edge(w, target, ch, half=None):
        @pl.when(jnp.logical_and(z == 0, target > 0))
        def _():
            rs(w, RIGHT, target, ch, True, half).start()

        @pl.when(jnp.logical_and(z == nz - 1, target < nz - 1))
        def _():
            rs(w, LEFT, target, ch, True, half).start()

    def rs_pass(w, side, step, ch, half=None):
        target = nz - 1 - step if side == RIGHT else step
        if side == RIGHT:
            cond = jnp.logical_and(z > 0, z < target)
        else:
            cond = jnp.logical_and(z < nz - 1, z > target)

        @pl.when(cond)
        def _():
            rs_waits(w, side, ch, target, half).wait_recv()
            buf = half_of(slots[w].at[target, ch], half)
            own = half_of(parts[w].at[target, ch], half)

            def add(rows):
                buf[rows, :] = (buf[rows, :].astype(F32)
                                + own[rows, :].astype(F32)).astype(BF16)
            by_rows(buf.shape[0], 64, add)
            rs(w, side, target, ch, False, half).start()

    def passes(w, sides, chunks, first, last, half):
        for low_side in (True, False):
            @pl.when(z < nz // 2 if low_side else z >= nz // 2)
            def _():
                for step in range(first, last):
                    for ch in chunks:
                        rs_pass(w, sides[0] if low_side else sides[1], step, ch, half)

    def near(w, ch, first=0, last=nz - 2):
        passes(w, (RIGHT, LEFT), [ch], first, last, None)

    def far(w, ch):
        passes(w, (LEFT, RIGHT), [ch], 0, nz - 2, None)

    tail = (CHUNKS - 2, CHUNKS - 1)

    def near_tail(first, last, half):
        passes(UP, (RIGHT, LEFT), tail, first, last, half)

    def far_tail(half):
        passes(UP, (LEFT, RIGHT), tail, 0, nz - 2, half)

    def rs_drain(w):
        for target in range(nz):
            every = slots[w].at[target]
            pl.when(z != target)(
                remote(every, every, rs_s.at[w, target], rs_r.at[w, 0, 0], y_dev).wait_send)

    def fin_cut(w, buf, yy):
        cut = pl.ds(aligned(yy * m.df, m.df), m.df)
        return buf.at[:, cut] if w == DN else buf.at[cut, :]

    def fin_place(w, ch, yy):
        start = aligned(yy * m.hh + ch * m.hc, m.hc)
        if w == DN:
            return dg_out.at[pl.ds(start, m.hc), :]
        return ug_out.at[:, pl.ds(start, m.hc)]

    def fin_remote(w, ch):
        return remote(fin_cut(w, parts[w].at[z, ch], yo), fin_place(w, ch, y),
                      fin_s.at[w], fin_r.at[w], y_dev)

    def rs_finish(w, ch, half=None):
        own = parts[w].at[z, ch]
        right, left = slots[w].at[z, ch], slots[w].at[nz, ch]
        pl.when(z > 0)(rs_waits(w, RIGHT, ch, z, half).wait_recv)
        pl.when(z < nz - 1)(rs_waits(w, LEFT, ch, nz, half).wait_recv)

        def total(yy, dst, others):
            terms = [fin_cut(w, buf, yy) for buf in others]

            def add(rows):
                value = terms[0][rows, :].astype(F32)
                for term in terms[1:]:
                    value = value + term[rows, :].astype(F32)
                dst[rows, :] = value.astype(BF16)
            by_rows(terms[0].shape[0], 64, add)

        def both(yy, dst):
            pl.when(z == 0)(lambda: total(yy, dst, (own, left)))
            pl.when(z == nz - 1)(lambda: total(yy, dst, (own, right)))
            pl.when(jnp.logical_and(z > 0, z < nz - 1))(
                lambda: total(yy, dst, (own, right, left)))

        if half != 1:
            both(yo, fin_cut(w, own, yo))
            fin_remote(w, ch).start()
        if half != 0:
            both(y, fin_place(w, ch, y))

    def finish_tail(half):
        for ch in tail:
            rs_finish(UP, ch, half)

    def fin_wait(w):
        def half(yy):
            cut = pl.ds(aligned(yy * m.hh, m.hh), m.hh)
            return dg_out.at[cut, :] if w == DN else ug_out.at[:, cut]

        mine, other = half(y), half(yo)
        remote(mine, mine, fin_s.at[w], fin_r.at[w], y_dev).wait_send()
        remote(other, other, fin_s.at[w], fin_r.at[w], y_dev).wait_recv()

    def targets(i):
        return mirror(nz - 1 - i)

    def squares(ch):
        cols = pl.ds(ch * m.hc, m.hc)

        def body(rows):
            active = jnp.maximum(acts[rows, cols].astype(F32), 0.0)
            hid[rows, cols] = (active * active).astype(BF16)
        by_rows(m.all_rows, 64, body)

    def dot_rows(a, b):
        return lax.dot_general(a, b, (((0,), (0,)), ((), ())), preferred_element_type=F32)

    def dot_cols(a, b):
        return lax.dot_general(a, b, (((1,), (1,)), ((), ())), preferred_element_type=F32)

    def dot_dn(ch, first=0, last=nz):
        @pl.loop(first, last)
        def _(i):
            target = targets(i)
            a = hid[:, pl.ds(ch * m.hc, m.hc)]
            b = og_all[:, pl.ds(aligned(target * m.dz, m.dz), m.dz)]
            part_dn[target, ch] = dot_rows(a, b).astype(BF16)
            rs_edge(DN, target, ch)

    def dot_hg(ch):
        cols = pl.ds(ch * m.hc, m.hc)

        @pl.loop(0, m.all_rows // 512)
        def _(i):
            rows = pl.ds(aligned(i * 512, 512), 512)
            active = jnp.maximum(acts[rows, cols].astype(F32), 0.0)
            grad = dot_cols(og_all[rows, :], dn_all[cols, :])
            pre[rows, cols] = (2.0 * active * grad).astype(BF16)

    def dot_up(ch, send=True):
        @pl.loop(0, nz)
        def _(i):
            target = targets(i)
            a = in_all[:, pl.ds(aligned(target * m.dz, m.dz), m.dz)]
            b = pre[:, pl.ds(ch * m.hc, m.hc)]
            part_up[target, ch] = dot_rows(a, b).astype(BF16)
            if send:
                rs_edge(UP, target, ch)

    def up_sends():
        @pl.loop(0, nz)
        def _(i):
            for half in range(2):
                for ch in tail:
                    rs_edge(UP, targets(i), ch, half)

    part = og_all
    width = m.d // 2
    sets = [pl.ds(0, width), pl.ds(width, width)]

    def ig_c(g, j):
        yy, xx = j // nx, j % nx
        return remote(slot(part, yy, xx, co).at[:, sets[g]], crecv.at[yy, xx, :, sets[g]],
                      igc_s.at[g], igc_r.at[g], c_dev)

    def dot_in(g, remote_half):
        piece = m.df // 2
        group = 4
        tile = piece * group
        cc = co if remote_half else c
        count = m.fs // group

        @pl.loop(0, ny * count)
        def _(i):
            yy, n = i // count, i % count
            cols = pl.ds(aligned(g * width + n * tile, tile), tile)
            blocks = [pl.ds(aligned(((yy * nx + xx) * 2 + cc) * m.t, m.t), m.t)
                      for xx in range(nx)]
            rows_of = [pl.ds(aligned((n * group + q) * m.df + g * piece, piece), piece)
                       for q in range(group)]
            a = jnp.concatenate([pre[rows, :] for rows in blocks], 0)
            b = jnp.concatenate([up_all[rows, :] for rows in rows_of], 0)
            value = dot_cols(a, b).astype(BF16)
            for xx, rows in enumerate(blocks):
                part[rows, cols] = value[xx * m.t:(xx + 1) * m.t]
            if remote_half:
                @pl.when(n == count - 1)
                def _():
                    for xx in range(nx):
                        ig_c(g, yy * nx + xx).start()

    def ig_all(g):
        every = crecv.at[:, :, :, sets[g]]
        return remote(every, every, igc_s.at[g], igc_r.at[g], c_dev)

    def ig_sum(g):
        ig_all(g).wait_recv()

        @pl.loop(0, ny * nx)
        def _(j):
            buf = crecv.at[j // nx, j % nx, :, sets[g]]
            own = slot(part, j // nx, j % nx, c).at[:, sets[g]]

            def add(rows):
                buf[rows, :] = (buf[rows, :].astype(F32) + own[rows, :].astype(F32)).astype(BF16)
            by_rows(m.t, 32, add)

    low, high = pl.ds(0, m.half), pl.ds(m.half, m.half)

    def accumulate(dst, others):
        def add(rows):
            value = dst[rows, :].astype(F32)
            for other in others:
                value = value + other[rows, :].astype(F32)
            dst[rows, :] = value.astype(BF16)
        by_rows(m.half, 32, add)

    def ig_x1(g, k):
        return remote(crecv.at[:, x_at(k), low, sets[g]], xr1.at[k - 1, :, :, sets[g]],
                      igx_s.at[g], igx_r.at[g, k - 1], at(z, y, x_at(k), c))

    def ig_y1(g):
        return remote(crecv.at[yo, x, low, sets[g]], yr1.at[:, sets[g]],
                      igx_s.at[g], igx_r.at[g, nx - 1], y_dev)

    def ig_y2(g):
        return remote(crecv.at[yo, :, high, sets[g]], yr2.at[:, :, sets[g]],
                      igx_s.at[g], igx_r.at[g, nx], y_dev)

    def ig_x2(g, k):
        return remote(crecv.at[y, x_at(k), high, sets[g]], xr2.at[k - 1, :, sets[g]],
                      igx_s.at[g], igx_r.at[g, nx + k], at(z, y, x_at(k), c))

    def ig_first(g):
        for k in range(1, nx):
            ig_x1(g, k).start()
        ig_y2(g).start()

    def ig_second(g):
        for k in range(1, nx):
            ig_x1(g, k).wait_recv()
        for yy in range(ny):
            accumulate(crecv.at[yy, x, low, sets[g]],
                       [xr1.at[k, yy, :, sets[g]] for k in range(nx - 1)])
        ig_y1(g).start()
        ig_y2(g).wait_recv()
        for xx in range(nx):
            accumulate(crecv.at[y, xx, high, sets[g]], [yr2.at[xx, :, sets[g]]])
        for k in range(1, nx):
            ig_x2(g, k).start()

    piece = m.df // 2

    def ig_store(rows, g, value):
        value = value.astype(BF16)
        if not m.direct:
            ig_out[rows, sets[g]] = value
            return
        for n in range(m.fs):
            ig_out[rows, pl.ds(n * m.df + g * piece, piece)] = value[:, n * piece:(n + 1) * piece]

    def ig_final(first, g, terms):
        def add(rows):
            value = terms[0][rows, :].astype(F32)
            for term in terms[1:]:
                value = value + term[rows, :].astype(F32)
            ig_store(pl.ds(aligned(first + rows.start, 32), rows.size), g, value)
        by_rows(m.half, 32, add)

    def ig_last(g):
        ig_y1(g).wait_recv()
        ig_final(0, g, [crecv.at[y, x, low, sets[g]], yr1.at[:, sets[g]]])
        for k in range(1, nx):
            ig_x2(g, k).wait_recv()
        ig_final(m.half, g, [crecv.at[y, x, high, sets[g]]]
                 + [xr2.at[k, :, sets[g]] for k in range(nx - 1)])

    def acts_in(index):
        act_copy(index, True).wait_recv()

    def start():
        ag_step(DN, 0, 0, 0)
        ag_step(UP, 0, 0, 0)
        ag_step(UP, 0, 1, 0)
        for p in order[:2]:
            og_rows.start_x(p)
        og_rows.start_y(order[0])
        act_copy(0).start()
        for p in order[1:-1]:
            og_rows.start_y(p)
        go(weight_y(DN))
        act_copy(1).start()
        og_rows.start_y(order[-1])
        go(weight_y(UP))
        act_copy(2).start()
        in_rows.start_y(0)
        act_copy(3).start()
        for copy in local:
            copy.start()

    def rows_on(i):
        og_rows.relay_y(order[i])
        og_rows.relay_x(order[i], 0)
        if i + 2 < nz:
            og_rows.start_x(order[i + 2])

    def rows_in(i):
        og_rows.relay_x(order[i], 1)
        og_rows.finish(order[i])

    def local_wait():
        for copy in local:
            copy.wait()

    def weight_in(w):
        weight_y(w, True).wait_recv()

    def in_relay(edge):
        outer = jnp.logical_or(z == 0, z == nz - 1)

        @pl.when(outer if edge else jnp.logical_not(outer))
        def _():
            in_rows.relay_y(0)
            in_rows.relay_x(0, 0)

    def act_drain():
        every = acts.at[pl.ds(0, m.rows), :]
        remote(every, every, act_s, act_r.at[0], y_dev).wait_send()

    def ig_drain():
        for g in range(2):
            ig_all(g).wait_send()
            every = part.at[pl.ds(0, (2 * nx - 1) * m.t), sets[g]]
            remote(every, every, igx_s.at[g], igx_r.at[g, 0], y_dev).wait_send()

    def gather_on(w, u, h):
        near_steps = [(ag_step, w, u, h, k, "near") for k in range(2, nz // 2)]
        return near_steps + [(ag_step, w, u, h, k, "far") for k in range(2, nz - 1)]

    plan = [
        (start,),
        (rows_on, 0),
        (ag_step, DN, 0, 0, 1),
        (rows_in, 0),
        (local_wait,),
        (acts_in, 0),
        (squares, 0),
        (dot_dn, 0, 0, 1),
        *[(rows_on, i) for i in range(1, nz - 1)],
        *[call for i in range(1, nz - 1)
          for call in ((rows_in, i), (dot_dn, 0, i, i + 1))],
        (near, DN, 0, 0, 1),
        (weight_in, DN),
        (ag_step, DN, 1, 0, 0),
        *gather_on(DN, 0, 0),
        (near, DN, 0, 1, nz - 2),
        (acts_in, 1),
        (squares, 1),
        (dot_dn, 1, 0, nz - 1),
        (rows_on, nz - 1),
        (in_rows.start_x, 0),
        (ag_step, DN, 1, 0, 1),
        (rows_in, nz - 1),
        (dot_dn, 0, nz - 1, nz),
        (dot_dn, 1, nz - 1, nz),
        (weight_in, UP),
        (ag_step, UP, 1, 0, 0, "edge"),
        (ag_step, UP, 1, 1, 0, "edge"),
        (ag_step, UP, 1, 0, 0, "inner"),
        (ag_step, UP, 0, 0, 1, "near"),
        (near, DN, 1),
        (acts_in, 2),
        (squares, 2),
        (dot_dn, 2),
        *gather_on(DN, 1, 0),
        (ag_step, UP, 0, 0, 1, "far"),
        (ag_step, UP, 1, 0, 1, "near"),
        (in_relay, True),
        (ag_finish, DN, 0, 0),
        (ag_finish, DN, 1, 0),
        (dot_hg, 0),
        (dot_hg, 1),
        (dot_hg, 2),
        (ag_step, UP, 1, 0, 1, "far"),
        (ag_step, UP, 1, 1, 0, "inner"),
        (ag_step, UP, 0, 1, 1, "near"),
        (ag_step, UP, 1, 1, 1, "near"),
        (in_relay, False),
        *gather_on(UP, 0, 0),
        *gather_on(UP, 1, 0),
        (acts_in, 3),
        (squares, 3),
        (dot_dn, 3),
        (dot_hg, 3),
        (near, DN, 2),
        (in_rows.relay_x, 0, 1),
        (in_rows.finish, 0),
        (dot_up, 0),
        (ag_step, UP, 0, 1, 1, "far"),
        (dot_up, 1),
        (near, DN, 3),
        (ag_step, UP, 1, 1, 1, "far"),
        (ag_finish, UP, 0, 0),
        (ag_finish, UP, 1, 0),
        (og_rows.drain,),
        (dot_in, 0, True),
        *gather_on(UP, 0, 1),
        (dot_in, 0, False),
        (dot_up, 2, False),
        *gather_on(UP, 1, 1),
        (ig_sum, 0),
        (ig_first, 0),
        (dot_up, 3, False),
        (up_sends,),
        (far, DN, 0),
        (far, DN, 1),
        (near, UP, 0),
        (ig_second, 0),
        (ag_finish, UP, 0, 1),
        (ag_finish, UP, 1, 1),
        (dot_in, 1, True),
        (dot_in, 1, False),
        (far, DN, 2),
        (far, DN, 3),
        (ig_sum, 1),
        (ig_first, 1),
        (far, UP, 0),
        (near, UP, 1),
        (ig_last, 0),
        (rs_finish, DN, 0),
        (rs_finish, DN, 1),
        (far, UP, 1),
        (ig_second, 1),
        (rs_finish, DN, 2),
        (rs_finish, DN, 3),
        (near_tail, 0, 1, 0),
        (ig_last, 1),
        (near_tail, 0, 1, 1),
        (rs_finish, UP, 0),
        (near_tail, 1, nz - 2, 0),
        (far_tail, 0),
        (rs_finish, UP, 1),
        (near_tail, 1, nz - 2, 1),
        (far_tail, 1),
        (finish_tail, 0),
        (finish_tail, 1),
        (in_rows.drain,),
        (drain, sends),
        (ag_drain,),
        (act_drain,),
        (ig_drain,),
        (rs_drain, DN),
        (rs_drain, UP),
        (fin_wait, DN),
        (fin_wait, UP),
    ]
    for index, (function, *args) in enumerate(plan):
        tags = [str(arg) for arg in args if isinstance(arg, (int, str))]
        label = "_".join([str(index), function.__name__, *tags])
        with jax.named_scope(label):
            function(*args)


def local_step(fs, tp, inp, act, og, upw, dnw):
    m = Dims(fs, tp, og.shape[0], og.shape[1], act.shape[1])
    dma = pltpu.SemaphoreType.DMA
    vm = pltpu.VMEM
    any_space = pl.BlockSpec(memory_space=pl.ANY)
    flops = 8 * m.all_rows * m.hh * m.d
    ig, ug, dg = pl.pallas_call(
        functools.partial(kernel, m),
        name="ffn_backward",
        out_shape=(
            vm((m.t, m.d), BF16),
            vm((m.df, m.h), BF16),
            vm((m.h, m.df), BF16),
        ),
        in_specs=[any_space] * 5,
        out_specs=(pl.BlockSpec(memory_space=pltpu.VMEM),) * 3,
        scratch_shapes=[
            vm((m.all_rows, m.d), BF16),
            vm((m.all_rows, m.d), BF16),
            vm((m.all_rows, m.hh), BF16),
            vm((m.all_rows, m.hh), BF16),
            vm((m.all_rows, m.hh), BF16),
            vm((m.hh, m.d), BF16),
            vm((m.d, m.hh), BF16),
            vm((m.nz, CHUNKS, m.hc, m.dz), BF16),
            vm((m.nz, CHUNKS, m.dz, m.hc), BF16),
            vm((m.nz + 1, CHUNKS, m.hc, m.dz), BF16),
            vm((m.nz + 1, CHUNKS, m.dz, m.hc), BF16),
            vm((m.ny, m.nx, m.t, m.d), BF16),
            vm((m.nx - 1, m.ny, m.half, m.d), BF16),
            vm((m.half, m.d), BF16),
            vm((m.nx, m.half, m.d), BF16),
            vm((m.nx - 1, m.half, m.d), BF16),
            dma((5,)),
            dma((2, m.nz - 1)),
            dma((3 * m.ny, m.nz)),
            dma((2,)),
            dma((2,)),
            dma((2,)),
            dma((m.nz + 1, 2 * m.nx)),
            dma,
            dma((ACT_PARTS,)),
            dma((2, m.nz)),
            dma((2, m.nz + 1, CHUNKS)),
            dma((m.nz + 1, 2)),
            dma((2,)),
            dma((2,)),
            dma((2,)),
            dma((2,)),
            dma((2,)),
            dma((2, 2 * m.nx)),
        ],
        cost_estimate=pl.CostEstimate(flops=flops, bytes_accessed=2**25, transcendentals=0),
        compiler_params=pltpu.CompilerParams(
            collective_id=0, has_side_effects=True, vmem_limit_bytes=62914560
        ),
    )(inp, act, og, upw, dnw)
    if not m.direct:
        ig = ig.reshape(m.t, 2, m.fs, m.df // 2).transpose(0, 2, 1, 3)
        ig = ig.reshape(m.t, m.d)
    return widen(ig, ug, dg)


def widen(ig, ug, dg):
    steps = 2

    def body(ig_in, ug_in, dg_in, ig_out, ug_out, dg_out, wide_ug, wide_dg, sems):
        copies = [pltpu.make_async_copy(ig_in, ig_out, sems.at[0])]
        copies[0].start()
        pairs = ((ug_in, wide_ug, ug_out), (dg_in, wide_dg, dg_out))
        for which, (src, wide, out) in enumerate(pairs):
            count = src.shape[0] // steps
            for i in range(steps):
                first = i * count
                rows = pl.ds(first, count)

                @pl.loop(0, count // 32)
                def _(j):
                    part = pl.ds(aligned(first + j * 32, 32), 32)
                    wide[part, :] = src[part, :].astype(F32)

                copies.append(pltpu.make_async_copy(
                    wide.at[rows, :], out.at[rows, :], sems.at[1 + which * steps + i]))
                copies[-1].start()
        for copy in copies:
            copy.wait()

    vmem = pl.BlockSpec(memory_space=pltpu.VMEM)
    outside = pl.BlockSpec(memory_space=pl.ANY)
    return pl.pallas_call(
        body,
        name="widen",
        out_shape=(
            jax.ShapeDtypeStruct(ig.shape, BF16),
            jax.ShapeDtypeStruct(ug.shape, F32),
            jax.ShapeDtypeStruct(dg.shape, F32),
        ),
        in_specs=[vmem] * 3,
        out_specs=(outside,) * 3,
        scratch_shapes=[
            pltpu.VMEM(ug.shape, F32),
            pltpu.VMEM(dg.shape, F32),
            pltpu.SemaphoreType.DMA((1 + 2 * steps,)),
        ],
        cost_estimate=pl.CostEstimate(flops=ug.size, bytes_accessed=16 * ug.size, transcendentals=0),
        compiler_params=pltpu.CompilerParams(vmem_limit_bytes=16 * ug.size),
    )(*(pltpu.with_memory_space_constraint(v, pltpu.VMEM) for v in (ig, ug, dg)))


def solution(mesh):
    placed = (
        P(("fs", "tp"), None),
        P("fs", "tp"),
        P(("fs", "tp"), None),
        P("fs", "tp"),
        P("tp", "fs"),
    )
    return jax.shard_map(
        functools.partial(local_step, mesh.shape["fs"], mesh.shape["tp"]),
        mesh=mesh,
        in_specs=placed,
        out_specs=(P(("fs", "tp"), None), P("fs", "tp"), P("tp", "fs")),
        check_vma=False,
    )
```

```python
import functools

import jax
import jax.numpy as jnp
from jax import lax
from jax.experimental import pallas as pl
from jax.experimental.pallas import tpu as pltpu
from jax.sharding import PartitionSpec as P

MESH = pl.DeviceIdType.MESH
BF16, F32 = jnp.bfloat16, jnp.float32
CHUNKS = 4
ACT_PARTS = 4
DN, UP = 0, 1
RIGHT, LEFT = 0, 1


def aligned(value, unit):
    return pl.multiple_of(value, unit)


class Dims:
    def __init__(self, fs, tp, tokens, d, hidden):
        self.fs, self.tp = fs, tp
        self.ny, self.nc = 2, 2
        self.nz, self.nx = fs // 2, tp // 2
        self.t, self.d, self.h = tokens, d, hidden
        self.rows = tokens * tp
        self.all_rows = self.rows * self.ny
        self.hh = hidden // self.ny
        self.df = d // fs
        self.dz = self.df * self.ny
        self.half = tokens // 2
        self.hc = self.hh // CHUNKS
        self.ha = self.hh // ACT_PARTS
        self.direct = (self.df // 2) % 128 == 0


def kernel(
    m, inp, act, og, upw, dnw, ig_out, ug_out, dg_out,
    og_all, in_all, acts, hid, pre, dn_all, up_all,
    part_dn, part_up, slot_dn, slot_up, crecv, xr1, yr1, yr2, xr2,
    loc, ag_s, ag_r, wy_s, wy_r, tok_s, tok_r, act_s, act_r,
    rs_s, rs_r, rs_h, fin_s, fin_r, igc_s, igc_r, igx_s, igx_r,
):
    f, tt = lax.axis_index("fs"), lax.axis_index("tp")
    ny, nx, nz = m.ny, m.nx, m.nz
    z, y = f // ny, f % ny
    x, c = tt // 2, tt % 2
    yo, co = 1 - y, 1 - c
    sends = []

    def at(zz, yy, xx, cc):
        return (zz * ny + yy, xx * 2 + cc)

    y_dev, c_dev = at(z, yo, x, c), at(z, y, x, co)
    z_dev = (at(z + 1, y, x, c), at(z - 1, y, x, c))
    has_z = (z < nz - 1, z > 0)

    def x_at(k):
        return lax.rem(x + k, nx)

    def mirror(target):
        return jnp.where(z < nz // 2, target, nz - 1 - target)

    order = [mirror(nz - 1 - i) for i in range(nz)]

    def remote(src, dst, ss, rs, dev):
        return pltpu.make_async_remote_copy(
            src_ref=src, dst_ref=dst, send_sem=ss, recv_sem=rs,
            device_id=dev, device_id_type=MESH,
        )

    def go(copy, cond=None, group=sends):
        if cond is None:
            copy.start()
        else:
            pl.when(cond)(copy.start)
        group.append((cond, copy))

    def drain(group):
        for cond, copy in group:
            if cond is None:
                copy.wait_send()
            else:
                pl.when(cond)(copy.wait_send)
        group.clear()

    barrier = pltpu.get_barrier_semaphore()
    peers = [(None, y_dev), (None, c_dev)]
    peers += [(None, at(z, y, x_at(k), c)) for k in range(1, nx)]
    peers += [(has_z[RIGHT], z_dev[RIGHT]), (has_z[LEFT], z_dev[LEFT])]
    for cond, dev in peers:
        def hello(dev=dev):
            pl.semaphore_signal(barrier, inc=1, device_id=dev, device_id_type=MESH)
        hello() if cond is None else pl.when(cond)(hello)
    lines = jnp.where(z > 0, 1, 0) + jnp.where(z < nz - 1, 1, 0)
    pl.semaphore_wait(barrier, 1 + nx + lines)

    def slot(buf, yy, xx, cc):
        start = aligned(((yy * nx + xx) * 2 + cc) * m.t, m.t)
        return buf.at[pl.ds(start, m.t), :]

    parts_of = (1, 2)

    def weight_view(w, ff, h=None):
        start, size = ff * m.df, m.df
        if w == DN:
            return dn_all.at[:, pl.ds(aligned(start, m.df), m.df)]
        if h is not None:
            size = m.df // parts_of[w]
            start = start + h * size
        return up_all.at[pl.ds(aligned(start, size), size), :]

    def weight_own(w, yy, h=None):
        start = aligned(yy * m.hh, m.hh)
        if w == DN:
            return dnw.at[pl.ds(start, m.hh), :]
        first, size = 0, m.df
        if h is not None:
            size = m.df // parts_of[w]
            first = h * size
        return upw.at[pl.ds(first, size), pl.ds(start, m.hh)]

    def ag(w, u, h, side, k, receive=False):
        back = k + 1 if receive else k
        origin = jnp.clip(z - back if side == RIGHT else z + back, 0, nz - 1)
        view = weight_view(w, origin * ny + (y if u == 0 else yo), h)
        src = weight_own(w, y, h) if (u == 0 and k == 0) else view
        unit = u if w == DN else ny + 2 * u + h
        return remote(src, view, ag_s.at[side, k], ag_r.at[unit, origin], z_dev[side])

    def ag_sends(side, k):
        if side == RIGHT:
            return jnp.logical_and(z >= k, z < nz - 1)
        return jnp.logical_and(z <= nz - 1 - k, z > 0)

    def ag_step(w, u, h, k, where="all"):
        outer = (z == 0, z == nz - 1)
        inner = jnp.logical_and(z > 0, z < nz - 1)
        close = (z < nz // 2, z >= nz // 2)
        for side in (RIGHT, LEFT):
            cond = ag_sends(side, k)
            if where == "edge":
                cond = outer[side]
            if where == "inner":
                cond = inner
            if where == "near":
                cond = jnp.logical_and(cond, close[side])
            if where == "far":
                cond = jnp.logical_and(cond, close[1 - side])
            if k > 0:
                pl.when(cond)(ag(w, u, h, side, k - 1, True).wait_recv)
            pl.when(cond)(ag(w, u, h, side, k).start)

    def ag_drain():
        every = up_all.at[pl.ds(0, 4 * m.df), :]
        for side in (RIGHT, LEFT):
            for k in range(nz - 1):
                pl.when(ag_sends(side, k))(
                    remote(every, every, ag_s.at[side, k], ag_r.at[0, 0], y_dev).wait_send)

    def ag_finish(w, u, h):
        for k in range(nz - 1):
            pl.when(jnp.logical_and(z == nz - 1, z >= k + 1))(
                ag(w, u, h, RIGHT, k, True).wait_recv)
            pl.when(jnp.logical_and(z == 0, z <= nz - 2 - k))(
                ag(w, u, h, LEFT, k, True).wait_recv)

    def weight_y(w, receive=False):
        ff = z * ny + (yo if receive else y)
        return remote(weight_own(w, yo), weight_view(w, ff), wy_s.at[w], wy_r.at[w], y_dev)

    class Rows:
        def __init__(self, a, src, buf, pieces):
            self.a, self.buf = a, buf
            self.pieces, self.width, self.source = pieces, m.d // pieces, src

        def drain(self):
            count = 4 * nx - 1
            every = self.buf.at[pl.ds(0, count * m.t), :]
            remote(every, every, tok_s.at[self.a], tok_r.at[nz, 0], y_dev).wait_send()

        def cols(self, p):
            return pl.ds(aligned(p * self.width, self.width), self.width)

        def src(self, p):
            return self.source.at[:, self.cols(p)]

        def place(self, p, yy, xx, cc):
            start = aligned(((yy * nx + xx) * 2 + cc) * m.t, m.t)
            return self.buf.at[pl.ds(start, m.t), self.cols(p)]

        def copy(self, p, index, src, where, dev):
            row = p if self.a == 0 else nz
            return remote(src, self.place(p, *where), tok_s.at[self.a],
                          tok_r.at[row, index], dev)

        def over_y(self, p, receive=False):
            return self.copy(p, 0, self.src(p), (yo if receive else y, x, c), y_dev)

        def over_x(self, p, j, k, receive=False):
            yy = y if j == 0 else yo
            xx = x_at(nx - k) if receive else x
            src = self.src(p) if j == 0 else self.place(p, yy, x, c)
            index = 1 + j * (nx - 1) + k - 1
            return self.copy(p, index, src, (yy, xx, c), at(z, y, x_at(k), c))

        def over_c(self, p, j, k):
            yy = y if j == 0 else yo
            xx = x_at(nx - k) if k else x
            src = self.src(p) if j == 0 and k == 0 else self.place(p, yy, xx, c)
            return self.copy(p, 2 * nx - 1, src, (yy, xx, c), c_dev)

        def start_y(self, p):
            self.over_y(p).start()

        def start_x(self, p):
            for k in range(1, nx):
                self.over_x(p, 0, k).start()
            self.over_c(p, 0, 0).start()

        def relay_y(self, p):
            self.over_y(p, True).wait_recv()
            for k in range(1, nx):
                self.over_x(p, 1, k).start()
            self.over_c(p, 1, 0).start()

        def relay_x(self, p, j):
            for k in range(1, nx):
                self.over_x(p, j, k, True).wait_recv()
                self.over_c(p, j, k).start()

        def finish(self, p):
            row = p if self.a == 0 else nz
            half = self.buf.at[pl.ds(0, 2 * nx * m.t), self.cols(p)]
            remote(half, half, tok_s.at[self.a], tok_r.at[row, 2 * nx - 1], c_dev).wait_recv()

    og_rows = Rows(0, og, og_all, nz)
    in_rows = Rows(1, inp, in_all, 1)

    def act_copy(part, receive=False):
        col = part * m.ha
        src = act.at[:, pl.ds(aligned(yo * m.hh + col, m.ha), m.ha)]
        row = aligned((yo if receive else y) * m.rows, m.rows)
        dst = acts.at[pl.ds(row, m.rows), pl.ds(col, m.ha)]
        return remote(src, dst, act_s, act_r.at[part], y_dev)

    local = [
        pltpu.make_async_copy(weight_own(DN, y), weight_view(DN, f), loc.at[0]),
        pltpu.make_async_copy(weight_own(UP, y), weight_view(UP, f), loc.at[1]),
        pltpu.make_async_copy(og, slot(og_all, y, x, c), loc.at[2]),
        pltpu.make_async_copy(inp, slot(in_all, y, x, c), loc.at[3]),
        pltpu.make_async_copy(
            act.at[:, pl.ds(aligned(y * m.hh, m.hh), m.hh)],
            acts.at[pl.ds(aligned(y * m.rows, m.rows), m.rows), :], loc.at[4]),
    ]

    parts, slots = (part_dn, part_up), (slot_dn, slot_up)

    def half_of(ref, half):
        if half is None:
            return ref
        yy = yo if half == 0 else y
        return ref.at[pl.ds(aligned(yy * m.df, m.df), m.df), :]

    def rs_sem(w, place, ch, half):
        return rs_r.at[w, place, ch] if half != 1 else rs_h.at[place, ch - tail[0]]

    def rs(w, side, target, ch, own, half=None):
        src = (parts if own else slots)[w].at[target, ch]
        if side == RIGHT:
            place = target
        else:
            place = jnp.where(target == z - 1, nz, target)
        return remote(half_of(src, half), half_of(slots[w].at[place, ch], half),
                      rs_s.at[w, target], rs_sem(w, place, ch, half), z_dev[side])

    def rs_waits(w, side, ch, place, half=None):
        return remote(half_of(parts[w].at[0, ch], half), half_of(slots[w].at[place, ch], half),
                      rs_s.at[w, 0], rs_sem(w, place, ch, half), z_dev[side])

    def by_rows(count, step, body):
        @pl.loop(0, count // step)
        def _(i):
            body(pl.ds(aligned(i * step, step), step))

    def rs_edge(w, target, ch, half=None):
        @pl.when(jnp.logical_and(z == 0, target > 0))
        def _():
            rs(w, RIGHT, target, ch, True, half).start()

        @pl.when(jnp.logical_and(z == nz - 1, target < nz - 1))
        def _():
            rs(w, LEFT, target, ch, True, half).start()

    def rs_pass(w, side, step, ch, half=None):
        target = nz - 1 - step if side == RIGHT else step
        if side == RIGHT:
            cond = jnp.logical_and(z > 0, z < target)
        else:
            cond = jnp.logical_and(z < nz - 1, z > target)

        @pl.when(cond)
        def _():
            rs_waits(w, side, ch, target, half).wait_recv()
            buf = half_of(slots[w].at[target, ch], half)
            own = half_of(parts[w].at[target, ch], half)

            def add(rows):
                buf[rows, :] = (buf[rows, :].astype(F32)
                                + own[rows, :].astype(F32)).astype(BF16)
            by_rows(buf.shape[0], 64, add)
            rs(w, side, target, ch, False, half).start()

    def passes(w, sides, chunks, first, last, half):
        for low_side in (True, False):
            @pl.when(z < nz // 2 if low_side else z >= nz // 2)
            def _():
                for step in range(first, last):
                    for ch in chunks:
                        rs_pass(w, sides[0] if low_side else sides[1], step, ch, half)

    def near(w, ch, first=0, last=nz - 2):
        passes(w, (RIGHT, LEFT), [ch], first, last, None)

    def far(w, ch):
        passes(w, (LEFT, RIGHT), [ch], 0, nz - 2, None)

    tail = (CHUNKS - 2, CHUNKS - 1)

    def near_tail(first, last, half):
        passes(UP, (RIGHT, LEFT), tail, first, last, half)

    def far_tail(half):
        passes(UP, (LEFT, RIGHT), tail, 0, nz - 2, half)

    def rs_drain(w):
        for target in range(nz):
            every = slots[w].at[target]
            pl.when(z != target)(
                remote(every, every, rs_s.at[w, target], rs_r.at[w, 0, 0], y_dev).wait_send)

    def fin_cut(w, buf, yy):
        cut = pl.ds(aligned(yy * m.df, m.df), m.df)
        return buf.at[:, cut] if w == DN else buf.at[cut, :]

    def fin_place(w, ch, yy):
        start = aligned(yy * m.hh + ch * m.hc, m.hc)
        if w == DN:
            return dg_out.at[pl.ds(start, m.hc), :]
        return ug_out.at[:, pl.ds(start, m.hc)]

    def fin_remote(w, ch):
        return remote(fin_cut(w, parts[w].at[z, ch], yo), fin_place(w, ch, y),
                      fin_s.at[w], fin_r.at[w], y_dev)

    def rs_finish(w, ch, half=None):
        own = parts[w].at[z, ch]
        right, left = slots[w].at[z, ch], slots[w].at[nz, ch]
        pl.when(z > 0)(rs_waits(w, RIGHT, ch, z, half).wait_recv)
        pl.when(z < nz - 1)(rs_waits(w, LEFT, ch, nz, half).wait_recv)

        def total(yy, dst, others):
            terms = [fin_cut(w, buf, yy) for buf in others]

            def add(rows):
                value = terms[0][rows, :].astype(F32)
                for term in terms[1:]:
                    value = value + term[rows, :].astype(F32)
                dst[rows, :] = value.astype(BF16)
            by_rows(terms[0].shape[0], 64, add)

        def both(yy, dst):
            pl.when(z == 0)(lambda: total(yy, dst, (own, left)))
            pl.when(z == nz - 1)(lambda: total(yy, dst, (own, right)))
            pl.when(jnp.logical_and(z > 0, z < nz - 1))(
                lambda: total(yy, dst, (own, right, left)))

        if half != 1:
            both(yo, fin_cut(w, own, yo))
            fin_remote(w, ch).start()
        if half != 0:
            both(y, fin_place(w, ch, y))

    def finish_tail(half):
        for ch in tail:
            rs_finish(UP, ch, half)

    def fin_wait(w):
        def half(yy):
            cut = pl.ds(aligned(yy * m.hh, m.hh), m.hh)
            return dg_out.at[cut, :] if w == DN else ug_out.at[:, cut]

        mine, other = half(y), half(yo)
        remote(mine, mine, fin_s.at[w], fin_r.at[w], y_dev).wait_send()
        remote(other, other, fin_s.at[w], fin_r.at[w], y_dev).wait_recv()

    def targets(i):
        return mirror(nz - 1 - i)

    def squares(ch):
        cols = pl.ds(ch * m.hc, m.hc)

        def body(rows):
            active = jnp.maximum(acts[rows, cols].astype(F32), 0.0)
            hid[rows, cols] = (active * active).astype(BF16)
        by_rows(m.all_rows, 64, body)

    def dot_rows(a, b):
        return lax.dot_general(a, b, (((0,), (0,)), ((), ())), preferred_element_type=F32)

    def dot_cols(a, b):
        return lax.dot_general(a, b, (((1,), (1,)), ((), ())), preferred_element_type=F32)

    def dot_dn(ch, first=0, last=nz):
        @pl.loop(first, last)
        def _(i):
            target = targets(i)
            a = hid[:, pl.ds(ch * m.hc, m.hc)]
            b = og_all[:, pl.ds(aligned(target * m.dz, m.dz), m.dz)]
            part_dn[target, ch] = dot_rows(a, b).astype(BF16)
            rs_edge(DN, target, ch)

    def dot_hg(ch):
        cols = pl.ds(ch * m.hc, m.hc)

        @pl.loop(0, m.all_rows // 512)
        def _(i):
            rows = pl.ds(aligned(i * 512, 512), 512)
            active = jnp.maximum(acts[rows, cols].astype(F32), 0.0)
            grad = dot_cols(og_all[rows, :], dn_all[cols, :])
            pre[rows, cols] = (2.0 * active * grad).astype(BF16)

    def dot_up(ch, send=True):
        @pl.loop(0, nz)
        def _(i):
            target = targets(i)
            a = in_all[:, pl.ds(aligned(target * m.dz, m.dz), m.dz)]
            b = pre[:, pl.ds(ch * m.hc, m.hc)]
            part_up[target, ch] = dot_rows(a, b).astype(BF16)
            if send:
                rs_edge(UP, target, ch)

    def up_sends():
        @pl.loop(0, nz)
        def _(i):
            for half in range(2):
                for ch in tail:
                    rs_edge(UP, targets(i), ch, half)

    part = og_all
    width = m.d // 2
    sets = [pl.ds(0, width), pl.ds(width, width)]

    def ig_c(g, j):
        yy, xx = j // nx, j % nx
        return remote(slot(part, yy, xx, co).at[:, sets[g]], crecv.at[yy, xx, :, sets[g]],
                      igc_s.at[g], igc_r.at[g], c_dev)

    def dot_in(g, remote_half):
        piece = m.df // 2
        group = 4
        tile = piece * group
        cc = co if remote_half else c
        count = m.fs // group

        @pl.loop(0, ny * count)
        def _(i):
            yy, n = i // count, i % count
            cols = pl.ds(aligned(g * width + n * tile, tile), tile)
            blocks = [pl.ds(aligned(((yy * nx + xx) * 2 + cc) * m.t, m.t), m.t)
                      for xx in range(nx)]
            rows_of = [pl.ds(aligned((n * group + q) * m.df + g * piece, piece), piece)
                       for q in range(group)]
            a = jnp.concatenate([pre[rows, :] for rows in blocks], 0)
            b = jnp.concatenate([up_all[rows, :] for rows in rows_of], 0)
            value = dot_cols(a, b).astype(BF16)
            for xx, rows in enumerate(blocks):
                part[rows, cols] = value[xx * m.t:(xx + 1) * m.t]
            if remote_half:
                @pl.when(n == count - 1)
                def _():
                    for xx in range(nx):
                        ig_c(g, yy * nx + xx).start()

    def ig_all(g):
        every = crecv.at[:, :, :, sets[g]]
        return remote(every, every, igc_s.at[g], igc_r.at[g], c_dev)

    def ig_sum(g):
        ig_all(g).wait_recv()

        @pl.loop(0, ny * nx)
        def _(j):
            buf = crecv.at[j // nx, j % nx, :, sets[g]]
            own = slot(part, j // nx, j % nx, c).at[:, sets[g]]

            def add(rows):
                buf[rows, :] = (buf[rows, :].astype(F32) + own[rows, :].astype(F32)).astype(BF16)
            by_rows(m.t, 32, add)

    low, high = pl.ds(0, m.half), pl.ds(m.half, m.half)

    def accumulate(dst, others):
        def add(rows):
            value = dst[rows, :].astype(F32)
            for other in others:
                value = value + other[rows, :].astype(F32)
            dst[rows, :] = value.astype(BF16)
        by_rows(m.half, 32, add)

    def ig_x1(g, k):
        return remote(crecv.at[:, x_at(k), low, sets[g]], xr1.at[k - 1, :, :, sets[g]],
                      igx_s.at[g], igx_r.at[g, k - 1], at(z, y, x_at(k), c))

    def ig_y1(g):
        return remote(crecv.at[yo, x, low, sets[g]], yr1.at[:, sets[g]],
                      igx_s.at[g], igx_r.at[g, nx - 1], y_dev)

    def ig_y2(g):
        return remote(crecv.at[yo, :, high, sets[g]], yr2.at[:, :, sets[g]],
                      igx_s.at[g], igx_r.at[g, nx], y_dev)

    def ig_x2(g, k):
        return remote(crecv.at[y, x_at(k), high, sets[g]], xr2.at[k - 1, :, sets[g]],
                      igx_s.at[g], igx_r.at[g, nx + k], at(z, y, x_at(k), c))

    def ig_first(g):
        for k in range(1, nx):
            ig_x1(g, k).start()
        ig_y2(g).start()

    def ig_second(g):
        for k in range(1, nx):
            ig_x1(g, k).wait_recv()
        for yy in range(ny):
            accumulate(crecv.at[yy, x, low, sets[g]],
                       [xr1.at[k, yy, :, sets[g]] for k in range(nx - 1)])
        ig_y1(g).start()
        ig_y2(g).wait_recv()
        for xx in range(nx):
            accumulate(crecv.at[y, xx, high, sets[g]], [yr2.at[xx, :, sets[g]]])
        for k in range(1, nx):
            ig_x2(g, k).start()

    piece = m.df // 2

    def ig_store(rows, g, value):
        value = value.astype(BF16)
        if not m.direct:
            ig_out[rows, sets[g]] = value
            return
        for n in range(m.fs):
            ig_out[rows, pl.ds(n * m.df + g * piece, piece)] = value[:, n * piece:(n + 1) * piece]

    def ig_final(first, g, terms):
        def add(rows):
            value = terms[0][rows, :].astype(F32)
            for term in terms[1:]:
                value = value + term[rows, :].astype(F32)
            ig_store(pl.ds(aligned(first + rows.start, 32), rows.size), g, value)
        by_rows(m.half, 32, add)

    def ig_last(g):
        ig_y1(g).wait_recv()
        ig_final(0, g, [crecv.at[y, x, low, sets[g]], yr1.at[:, sets[g]]])
        for k in range(1, nx):
            ig_x2(g, k).wait_recv()
        ig_final(m.half, g, [crecv.at[y, x, high, sets[g]]]
                 + [xr2.at[k, :, sets[g]] for k in range(nx - 1)])

    def acts_in(index):
        act_copy(index, True).wait_recv()

    def start():
        ag_step(DN, 0, 0, 0)
        ag_step(UP, 0, 0, 0)
        ag_step(UP, 0, 1, 0)
        for p in order[:2]:
            og_rows.start_x(p)
        og_rows.start_y(order[0])
        act_copy(0).start()
        for p in order[1:-1]:
            og_rows.start_y(p)
        go(weight_y(DN))
        act_copy(1).start()
        og_rows.start_y(order[-1])
        go(weight_y(UP))
        act_copy(2).start()
        in_rows.start_y(0)
        act_copy(3).start()
        for copy in local:
            copy.start()

    def rows_on(i):
        og_rows.relay_y(order[i])
        og_rows.relay_x(order[i], 0)
        if i + 2 < nz:
            og_rows.start_x(order[i + 2])

    def rows_in(i):
        og_rows.relay_x(order[i], 1)
        og_rows.finish(order[i])

    def local_wait():
        for copy in local:
            copy.wait()

    def weight_in(w):
        weight_y(w, True).wait_recv()

    def in_relay(edge):
        outer = jnp.logical_or(z == 0, z == nz - 1)

        @pl.when(outer if edge else jnp.logical_not(outer))
        def _():
            in_rows.relay_y(0)
            in_rows.relay_x(0, 0)

    def act_drain():
        every = acts.at[pl.ds(0, m.rows), :]
        remote(every, every, act_s, act_r.at[0], y_dev).wait_send()

    def ig_drain():
        for g in range(2):
            ig_all(g).wait_send()
            every = part.at[pl.ds(0, (2 * nx - 1) * m.t), sets[g]]
            remote(every, every, igx_s.at[g], igx_r.at[g, 0], y_dev).wait_send()

    def gather_on(w, u, h):
        near_steps = [(ag_step, w, u, h, k, "near") for k in range(2, nz // 2)]
        return near_steps + [(ag_step, w, u, h, k, "far") for k in range(2, nz - 1)]

    plan = [
        (start,),
        (rows_on, 0),
        (ag_step, DN, 0, 0, 1),
        (rows_in, 0),
        (local_wait,),
        (acts_in, 0),
        (squares, 0),
        (dot_dn, 0, 0, 1),
        *[(rows_on, i) for i in range(1, nz - 1)],
        *[call for i in range(1, nz - 1)
          for call in ((rows_in, i), (dot_dn, 0, i, i + 1))],
        (near, DN, 0, 0, 1),
        (weight_in, DN),
        (ag_step, DN, 1, 0, 0),
        *gather_on(DN, 0, 0),
        (near, DN, 0, 1, nz - 2),
        (acts_in, 1),
        (squares, 1),
        (dot_dn, 1, 0, nz - 1),
        (rows_on, nz - 1),
        (in_rows.start_x, 0),
        (ag_step, DN, 1, 0, 1),
        (rows_in, nz - 1),
        (dot_dn, 0, nz - 1, nz),
        (dot_dn, 1, nz - 1, nz),
        (weight_in, UP),
        (ag_step, UP, 1, 0, 0, "edge"),
        (ag_step, UP, 1, 1, 0, "edge"),
        (ag_step, UP, 1, 0, 0, "inner"),
        (ag_step, UP, 0, 0, 1, "near"),
        (near, DN, 1),
        (acts_in, 2),
        (squares, 2),
        (dot_dn, 2),
        *gather_on(DN, 1, 0),
        (ag_step, UP, 0, 0, 1, "far"),
        (ag_step, UP, 1, 0, 1, "near"),
        (in_relay, True),
        (ag_finish, DN, 0, 0),
        (ag_finish, DN, 1, 0),
        (dot_hg, 0),
        (dot_hg, 1),
        (dot_hg, 2),
        (ag_step, UP, 1, 0, 1, "far"),
        (ag_step, UP, 1, 1, 0, "inner"),
        (ag_step, UP, 0, 1, 1, "near"),
        (ag_step, UP, 1, 1, 1, "near"),
        (in_relay, False),
        *gather_on(UP, 0, 0),
        *gather_on(UP, 1, 0),
        (acts_in, 3),
        (squares, 3),
        (dot_dn, 3),
        (dot_hg, 3),
        (near, DN, 2),
        (in_rows.relay_x, 0, 1),
        (in_rows.finish, 0),
        (dot_up, 0),
        (ag_step, UP, 0, 1, 1, "far"),
        (dot_up, 1),
        (near, DN, 3),
        (ag_step, UP, 1, 1, 1, "far"),
        (ag_finish, UP, 0, 0),
        (ag_finish, UP, 1, 0),
        (og_rows.drain,),
        (dot_in, 0, True),
        *gather_on(UP, 0, 1),
        (dot_in, 0, False),
        (dot_up, 2, False),
        *gather_on(UP, 1, 1),
        (ig_sum, 0),
        (ig_first, 0),
        (dot_up, 3, False),
        (up_sends,),
        (far, DN, 0),
        (far, DN, 1),
        (near, UP, 0),
        (ig_second, 0),
        (ag_finish, UP, 0, 1),
        (ag_finish, UP, 1, 1),
        (dot_in, 1, True),
        (dot_in, 1, False),
        (far, DN, 2),
        (far, DN, 3),
        (ig_sum, 1),
        (ig_first, 1),
        (far, UP, 0),
        (near, UP, 1),
        (ig_last, 0),
        (rs_finish, DN, 0),
        (rs_finish, DN, 1),
        (far, UP, 1),
        (ig_second, 1),
        (rs_finish, DN, 2),
        (rs_finish, DN, 3),
        (near_tail, 0, 1, 0),
        (ig_last, 1),
        (near_tail, 0, 1, 1),
        (rs_finish, UP, 0),
        (near_tail, 1, nz - 2, 0),
        (far_tail, 0),
        (rs_finish, UP, 1),
        (near_tail, 1, nz - 2, 1),
        (far_tail, 1),
        (finish_tail, 0),
        (finish_tail, 1),
        (in_rows.drain,),
        (drain, sends),
        (ag_drain,),
        (act_drain,),
        (ig_drain,),
        (rs_drain, DN),
        (rs_drain, UP),
        (fin_wait, DN),
        (fin_wait, UP),
    ]
    for index, (function, *args) in enumerate(plan):
        tags = [str(arg) for arg in args if isinstance(arg, (int, str))]
        label = "_".join([str(index), function.__name__, *tags])
        with jax.named_scope(label):
            function(*args)


def local_step(fs, tp, inp, act, og, upw, dnw):
    m = Dims(fs, tp, og.shape[0], og.shape[1], act.shape[1])
    dma = pltpu.SemaphoreType.DMA
    vm = pltpu.VMEM
    any_space = pl.BlockSpec(memory_space=pl.ANY)
    flops = 8 * m.all_rows * m.hh * m.d
    ig, ug, dg = pl.pallas_call(
        functools.partial(kernel, m),
        name="ffn_backward",
        out_shape=(
            vm((m.t, m.d), BF16),
            vm((m.df, m.h), BF16),
            vm((m.h, m.df), BF16),
        ),
        in_specs=[any_space] * 5,
        out_specs=(pl.BlockSpec(memory_space=pltpu.VMEM),) * 3,
        scratch_shapes=[
            vm((m.all_rows, m.d), BF16),
            vm((m.all_rows, m.d), BF16),
            vm((m.all_rows, m.hh), BF16),
            vm((m.all_rows, m.hh), BF16),
            vm((m.all_rows, m.hh), BF16),
            vm((m.hh, m.d), BF16),
            vm((m.d, m.hh), BF16),
            vm((m.nz, CHUNKS, m.hc, m.dz), BF16),
            vm((m.nz, CHUNKS, m.dz, m.hc), BF16),
            vm((m.nz + 1, CHUNKS, m.hc, m.dz), BF16),
            vm((m.nz + 1, CHUNKS, m.dz, m.hc), BF16),
            vm((m.ny, m.nx, m.t, m.d), BF16),
            vm((m.nx - 1, m.ny, m.half, m.d), BF16),
            vm((m.half, m.d), BF16),
            vm((m.nx, m.half, m.d), BF16),
            vm((m.nx - 1, m.half, m.d), BF16),
            dma((5,)),
            dma((2, m.nz - 1)),
            dma((3 * m.ny, m.nz)),
            dma((2,)),
            dma((2,)),
            dma((2,)),
            dma((m.nz + 1, 2 * m.nx)),
            dma,
            dma((ACT_PARTS,)),
            dma((2, m.nz)),
            dma((2, m.nz + 1, CHUNKS)),
            dma((m.nz + 1, 2)),
            dma((2,)),
            dma((2,)),
            dma((2,)),
            dma((2,)),
            dma((2,)),
            dma((2, 2 * m.nx)),
        ],
        cost_estimate=pl.CostEstimate(flops=flops, bytes_accessed=2**25, transcendentals=0),
        compiler_params=pltpu.CompilerParams(
            collective_id=0, has_side_effects=True, vmem_limit_bytes=62914560
        ),
    )(inp, act, og, upw, dnw)
    if not m.direct:
        ig = ig.reshape(m.t, 2, m.fs, m.df // 2).transpose(0, 2, 1, 3)
        ig = ig.reshape(m.t, m.d)
    return widen(ig, ug, dg)


def widen(ig, ug, dg):
    steps = 4

    def body(ig_in, ug_in, dg_in, ig_out, ug_out, dg_out, wide_ug, wide_dg, sems):
        copies = [pltpu.make_async_copy(ig_in, ig_out, sems.at[0])]
        copies[0].start()
        pairs = ((ug_in, wide_ug, ug_out), (dg_in, wide_dg, dg_out))
        for which, (src, wide, out) in enumerate(pairs):
            count = src.shape[0] // steps
            for i in range(steps):
                first = i * count
                rows = pl.ds(first, count)

                @pl.loop(0, count // 32)
                def _(j):
                    part = pl.ds(aligned(first + j * 32, 32), 32)
                    wide[part, :] = src[part, :].astype(F32)

                copies.append(pltpu.make_async_copy(
                    wide.at[rows, :], out.at[rows, :], sems.at[1 + which * steps + i]))
                copies[-1].start()
        for copy in copies:
            copy.wait()

    vmem = pl.BlockSpec(memory_space=pltpu.VMEM)
    outside = pl.BlockSpec(memory_space=pl.ANY)
    return pl.pallas_call(
        body,
        name="widen",
        out_shape=(
            jax.ShapeDtypeStruct(ig.shape, BF16),
            jax.ShapeDtypeStruct(ug.shape, F32),
            jax.ShapeDtypeStruct(dg.shape, F32),
        ),
        in_specs=[vmem] * 3,
        out_specs=(outside,) * 3,
        scratch_shapes=[
            pltpu.VMEM(ug.shape, F32),
            pltpu.VMEM(dg.shape, F32),
            pltpu.SemaphoreType.DMA((1 + 2 * steps,)),
        ],
        cost_estimate=pl.CostEstimate(flops=ug.size, bytes_accessed=16 * ug.size, transcendentals=0),
        compiler_params=pltpu.CompilerParams(vmem_limit_bytes=16 * ug.size),
    )(*(pltpu.with_memory_space_constraint(v, pltpu.VMEM) for v in (ig, ug, dg)))


def solution(mesh):
    placed = (
        P(("fs", "tp"), None),
        P("fs", "tp"),
        P(("fs", "tp"), None),
        P("fs", "tp"),
        P("tp", "fs"),
    )
    return jax.shard_map(
        functools.partial(local_step, mesh.shape["fs"], mesh.shape["tp"]),
        mesh=mesh,
        in_specs=placed,
        out_specs=(P(("fs", "tp"), None), P("fs", "tp"), P("tp", "fs")),
        check_vma=False,
    )
```
